32 devices in a mesh: grp: 2 (over y), fs: 4 (over z), tp: 4 (over x, core).
Axes of the slice: x: 2, y: 2, z: 4, core: 2. Of those that a mesh axis runs over, the one named last changes fastest.
Arguments:
- layer_input_tokens: bfloat16 [4096, 2048], P(('grp', 'fs')), parts along dimension 0, may hold values from -6 to 6
- attention_norm_gain: float32 [2048], replicated, may hold values from 0.1 to 1.9
- query_projection: bfloat16 [2048, 1024], P('fs', 'tp'), may hold values from -0.125 to 0.125
- key_projection: bfloat16 [2048, 1024], P('fs', 'tp'), may hold values from -0.125 to 0.125
- value_projection: bfloat16 [2048, 2048], P('fs', 'tp'), may hold values from -0.125 to 0.125
- decay_first_factor: bfloat16 [2048, 16], replicated, may hold values from -0.125 to 0.125
- decay_second_factor: bfloat16 [16, 1024], P(None, 'tp'), may hold values from -1.5 to 1.5
- decay_logit_bias: float32 [1024], P('tp'), may hold values from -0.5 to 6
- extra_log_decay: float32 [4096, 8], P(('grp', 'fs'), 'tp'), parts along dimension 0, may hold values from -0.7 to 0
- head_output_gain: float32 [256], replicated, may hold values from 0.1 to 1.9
- attention_output_projection: bfloat16 [2048, 2048], P(('tp', 'fs')), may hold values from -0.125 to 0.125
- feedforward_norm_gain: float32 [2048], replicated, may hold values from 0.1 to 1.9
- gate_projection: bfloat16 [2048, 5632], P('fs', 'tp'), may hold values from -0.125 to 0.125
- up_projection: bfloat16 [2048, 5632], P('fs', 'tp'), may hold values from -0.125 to 0.125
- down_projection: bfloat16 [5632, 2048], P(('tp', 'fs')), may hold values from -0.078125 to 0.078125
Outputs:
- result: bfloat16 [4096, 2048], P(('grp', 'fs')), parts along dimension 0
The draws below stay inside these ranges and needn't reach their ends.
There are 2 independent parts, one for each index of `grp`. The reference program is written for one: setup_inputs(seed, part) draws one part's arguments, and reference() takes and returns one part's arrays. A program takes and returns all parts, laid end to end along the dimension named above; an argument that names none is the same for every part. Nothing has to cross between parts.
All inputs are finite; a program needn't handle non-finite values.
Results may differ from the reference program's by a relative error of at most 0.02.
Values may be sent and summed in bfloat16 or wider, within the bound.
A program may use at most 64 MiB of HBM per device.

```python
import jax
import jax.numpy as jnp
from jax import lax

D = 2048
HEADS = 8
KEY_CHANNELS = 128
DV = 256
RANK = 16
FF = 5632
BLOCK = 64
SEQ_LEN = 512
TOKENS = 2048
N_FS = 4
N_TP = 4


def draw_decay_logit_bias(key, part):
    pick = jax.random.randint(jax.random.fold_in(key, 11), (HEADS * KEY_CHANNELS,), 0, 10)
    fast = jax.random.uniform(jax.random.fold_in(key, 12), (HEADS * KEY_CHANNELS,), jnp.float32, -0.5, 1.0)
    slow = jax.random.uniform(jax.random.fold_in(key, 13), (HEADS * KEY_CHANNELS,), jnp.float32, 3.5, 5.5)
    return jnp.where(pick < 5, fast, slow).astype(jnp.float32)


def draw_extra_log_decay(key, part):
    hits = jax.random.randint(jax.random.fold_in(key, 21), (TOKENS, HEADS), 0, SEQ_LEN)
    depth = jnp.log(jax.random.uniform(jax.random.fold_in(key, 22), (TOKENS, HEADS), jnp.float32, 0.5, 0.8))
    return jnp.where(hits < 3, depth, 0.0).astype(jnp.float32)


def shard_levels(stream_key, extent, cuts, smallest, largest):
    def one(dim, parts):
        steps = jax.random.uniform(jax.random.fold_in(jax.random.fold_in(stream_key, 6), dim), (parts,), jnp.float32, smallest / len(cuts), largest / len(cuts))
        return jnp.repeat(jnp.exp(steps), extent[dim] // parts).reshape((-1,) + (1,) * (len(extent) - dim - 1))

    level = one(*cuts[0])
    for cut in cuts[1:]:
        level = level * one(*cut)
    return level


def noise(own_key, dims, deviation, most, cuts=(), held_as=jnp.bfloat16):
    entries = deviation * jax.random.normal(own_key, dims, jnp.float32)
    if cuts:
        entries = entries * shard_levels(own_key, dims, cuts, -0.22, 0.18)
    return jnp.clip(entries, -most, most).astype(held_as)


def setup_inputs(seed: int = 0, part: int = 0) -> dict:
    seeds = jax.random.split(jax.random.key(seed), 16)
    part_splits = jax.random.split(jax.random.fold_in(seeds[15], part), 16)
    layer_input_tokens = noise(part_splits[0], (TOKENS, D), 1.0, 6.0, ((0, 4),))
    attention_norm_gain = jnp.clip(1.0 + 0.18 * jax.random.normal(seeds[1], (D,), jnp.float32), 0.1, 1.9)
    query_projection = noise(seeds[2], (D, HEADS * KEY_CHANNELS), D ** -0.5, 0.125, ((0, 4), (1, 4)))
    key_projection = noise(seeds[3], (D, HEADS * KEY_CHANNELS), D ** -0.5, 0.125, ((0, 4), (1, 4)))
    value_projection = noise(seeds[4], (D, HEADS * DV), D ** -0.5, 0.125, ((0, 4), (1, 4)))
    decay_first_factor = noise(seeds[5], (D, RANK), D ** -0.5, 0.125)
    decay_second_factor = noise(seeds[6], (RANK, HEADS * KEY_CHANNELS), RANK ** -0.5, 1.5, ((1, 4),))
    decay_logit_bias = draw_decay_logit_bias(jax.random.fold_in(seeds[15], 71), part)
    extra_log_decay = draw_extra_log_decay(jax.random.fold_in(jax.random.fold_in(seeds[15], part), 71), part)
    head_output_gain = jnp.clip(1.0 + 0.18 * jax.random.normal(seeds[9], (DV,), jnp.float32), 0.1, 1.9)
    attention_output_projection = noise(seeds[10], (HEADS * DV, D), (HEADS * DV) ** -0.5, 0.125, ((0, 16),))
    feedforward_norm_gain = jnp.clip(1.0 + 0.18 * jax.random.normal(seeds[11], (D,), jnp.float32), 0.1, 1.9)
    gate_projection = noise(seeds[12], (D, FF), D ** -0.5, 0.125, ((0, 4), (1, 4)))
    up_projection = noise(seeds[13], (D, FF), D ** -0.5, 0.125, ((0, 4), (1, 4)))
    down_projection = noise(seeds[14], (FF, D), FF ** -0.5, 0.078125, ((0, 16),))
    return {"layer_input_tokens": layer_input_tokens, "attention_norm_gain": attention_norm_gain, "query_projection": query_projection, "key_projection": key_projection, "value_projection": value_projection, "decay_first_factor": decay_first_factor, "decay_second_factor": decay_second_factor, "decay_logit_bias": decay_logit_bias, "extra_log_decay": extra_log_decay, "head_output_gain": head_output_gain, "attention_output_projection": attention_output_projection, "feedforward_norm_gain": feedforward_norm_gain, "gate_projection": gate_projection, "up_projection": up_projection, "down_projection": down_projection}


normed_gate = 16.0

def norm_rows(values, gain):
    wide = values.astype(jnp.float32)
    scale = lax.rsqrt(lax.optimization_barrier(jnp.mean(wide * wide, axis=-1, keepdims=True)) + 1e-06)
    return wide * scale * gain

def block_scan(queries, keys, values, decays):
    length, key_channel_width = queries.shape
    value_width = values.shape[1]
    count = length // BLOCK
    lower_mask = jnp.arange(BLOCK)[:, None] >= jnp.arange(BLOCK)[None, :]

    def advance(carry, items):
        query_block, key_block, value_block, decay_block = items
        running = jnp.cumsum(decay_block, axis=0)
        middle = running[BLOCK // 2 - 1]
        closing = running[BLOCK - 1]
        carried = jnp.dot(query_block * jnp.exp(running), carry, precision=lax.Precision.HIGHEST)
        scores = jnp.dot(query_block * jnp.exp(running - middle), (key_block * jnp.exp(middle - running)).T, precision=lax.Precision.HIGHEST)
        scores = jnp.where(lower_mask, scores, 0.0)
        inside = jnp.dot(scores, value_block, precision=lax.Precision.HIGHEST)
        fresh = carry * jnp.exp(closing)[:, None] + jnp.dot((key_block * jnp.exp(closing - running)).T, value_block, precision=lax.Precision.HIGHEST)
        return (fresh, carried + inside)
    items = (queries.reshape(count, BLOCK, key_channel_width), keys.reshape(count, BLOCK, key_channel_width), values.reshape(count, BLOCK, value_width), decays.reshape(count, BLOCK, key_channel_width))
    _, outputs = lax.scan(advance, jnp.zeros((key_channel_width, value_width), jnp.float32), items)
    return outputs.reshape(length, value_width)

def both_ways(queries, keys, values, decays):
    ahead = block_scan(queries, keys, values, decays)
    behind = block_scan(jnp.flip(queries, 0), jnp.flip(keys, 0), jnp.flip(values, 0), jnp.flip(decays, 0))
    return ahead + jnp.flip(behind, 0)

def head_norm(mixed, gain):
    scale = lax.rsqrt(lax.optimization_barrier(jnp.mean(mixed * mixed, axis=-1, keepdims=True)) + 1e-06)
    return mixed * scale * gain

def group_sum(left, right):
    width = left.shape[1] // N_TP
    total = jnp.zeros((left.shape[0], right.shape[1]), jnp.float32)
    for group in range(N_TP):
        part = jnp.dot(left[:, group * width:(group + 1) * width], right[group * width:(group + 1) * width], preferred_element_type=jnp.float32)
        part = lax.optimization_barrier(part.astype(jnp.bfloat16))
        total = total + part.astype(jnp.float32)
    return total

def reference(layer_input_tokens, attention_norm_gain, query_projection, key_projection, value_projection, decay_first_factor, decay_second_factor, decay_logit_bias, extra_log_decay, head_output_gain, attention_output_projection, feedforward_norm_gain, gate_projection, up_projection, down_projection):
    normed = norm_rows(layer_input_tokens, attention_norm_gain).astype(jnp.bfloat16)
    query = jnp.dot(normed, query_projection, preferred_element_type=jnp.float32).astype(jnp.bfloat16)
    key = jnp.dot(normed, key_projection, preferred_element_type=jnp.float32).astype(jnp.bfloat16)
    value = jnp.dot(normed, value_projection, preferred_element_type=jnp.float32).astype(jnp.bfloat16)
    lowrank = jnp.dot(normed, decay_first_factor, preferred_element_type=jnp.float32).astype(jnp.bfloat16)
    decay_logit_values = jnp.dot(lowrank, decay_second_factor, preferred_element_type=jnp.float32) + decay_logit_bias
    decay_logarithm = jax.nn.log_sigmoid(decay_logit_values) / normed_gate + jnp.repeat(extra_log_decay, KEY_CHANNELS, axis=1)

    def sequences(array, width):
        return array.astype(jnp.float32).reshape(N_FS, SEQ_LEN, HEADS, width)
    mixed = jax.vmap(jax.vmap(both_ways, in_axes=1, out_axes=1))(sequences(query, KEY_CHANNELS), sequences(key, KEY_CHANNELS), sequences(value, DV), sequences(decay_logarithm, KEY_CHANNELS))
    headed = head_norm(mixed.reshape(TOKENS, HEADS, DV), head_output_gain)
    headed = headed.reshape(TOKENS, HEADS * DV).astype(jnp.bfloat16)
    mixer = group_sum(headed, attention_output_projection)
    residual = (layer_input_tokens.astype(jnp.float32) + mixer).astype(jnp.bfloat16)
    second = norm_rows(residual, feedforward_norm_gain).astype(jnp.bfloat16)
    gate = jnp.dot(second, gate_projection, preferred_element_type=jnp.float32)
    up = jnp.dot(second, up_projection, preferred_element_type=jnp.float32)
    hidden = (jax.nn.silu(gate) * up).astype(jnp.bfloat16)
    channel = group_sum(hidden, down_projection)
    return (residual.astype(jnp.float32) + channel).astype(jnp.bfloat16)
```

```python
import functools

import jax
import jax.numpy as jnp
from jax import lax
from jax.experimental import pallas as pl
from jax.experimental.pallas import tpu as pltpu
from jax.sharding import PartitionSpec as P

BLOCK = 64
DECAY_GATE = 16.0


def norm_rows(values, gain):
    wide = values.astype(jnp.float32)
    scale = lax.rsqrt(jnp.mean(wide * wide, axis=-1, keepdims=True) + 1e-06)
    return wide * scale * gain


def attention_kernel(heads, qkv_ref, lowrank_ref, second_ref, bias_ref, extra_ref, gain_ref, out_ref):
    rows = qkv_ref.shape[0]
    kc = second_ref.shape[1] // heads
    vc = out_ref.shape[1] // heads
    count = rows // BLOCK
    f32, bf16 = jnp.float32, jnp.bfloat16
    row_id = lax.broadcasted_iota(jnp.int32, (BLOCK, BLOCK), 0)
    col_id = lax.broadcasted_iota(jnp.int32, (BLOCK, BLOCK), 1)
    lower = row_id >= col_id
    upper = row_id <= col_id
    lower_ones = jnp.where(lower, 1.0, 0.0).astype(f32)
    half = BLOCK // 2
    for h in range(heads):
        kcols = slice(h * kc, (h + 1) * kc)
        logits = (
            jnp.dot(lowrank_ref[...], second_ref[:, kcols], preferred_element_type=f32)
            + bias_ref[:, kcols]
        )
        log_sig = jnp.minimum(logits, 0.0) - jnp.log1p(jnp.exp(-jnp.abs(logits)))
        decay = log_sig / DECAY_GATE + extra_ref[:, h : h + 1]
        queries_fb, updates, closings, scores = [], [], [], []
        for b in range(count):
            r = slice(b * BLOCK, (b + 1) * BLOCK)
            d = decay[r]
            q = qkv_ref[r, h * kc : (h + 1) * kc].astype(f32)
            k = qkv_ref[r, (heads + h) * kc : (heads + h + 1) * kc].astype(f32)
            v = qkv_ref[r, 2 * heads * kc + h * vc : 2 * heads * kc + (h + 1) * vc]
            run = jnp.dot(lower_ones, d, precision=lax.Precision.HIGHEST, preferred_element_type=f32)
            closing = run[BLOCK - 1 : BLOCK]
            back = closing - run + d
            mid_f = run[half - 1 : half]
            mid_b = back[half : half + 1]
            qf = (q * jnp.exp(run - mid_f)).astype(bf16)
            kf = (k * jnp.exp(mid_f - run)).astype(bf16)
            qb = (q * jnp.exp(back - mid_b)).astype(bf16)
            kb = (k * jnp.exp(mid_b - back)).astype(bf16)
            nt = (((1,), (1,)), ((), ()))
            sf = lax.dot_general(qf, kf, nt, preferred_element_type=f32)
            sb = lax.dot_general(qb, kb, nt, preferred_element_type=f32)
            scores.append(
                (jnp.where(lower, sf, 0.0) + jnp.where(upper, sb, 0.0)).astype(bf16)
            )
            queries_fb.append(
                jnp.concatenate([q * jnp.exp(run), q * jnp.exp(back)], axis=1).astype(bf16)
            )
            keys_fb = jnp.concatenate(
                [k * jnp.exp(closing - run), k * jnp.exp(closing - back)], axis=1
            ).astype(bf16)
            updates.append(
                lax.dot_general(v, keys_fb, (((0,), (0,)), ((), ())), preferred_element_type=f32)
            )
            closings.append(jnp.exp(closing))
        state = jnp.zeros((vc, kc), f32)
        ahead = []
        for b in range(count):
            ahead.append(state.astype(bf16))
            state = state * closings[b] + updates[b][:, :kc]
        state = jnp.zeros((vc, kc), f32)
        behind = [None] * count
        for b in reversed(range(count)):
            behind[b] = state.astype(bf16)
            state = state * closings[b] + updates[b][:, kc:]
        for b in range(count):
            r = slice(b * BLOCK, (b + 1) * BLOCK)
            v = qkv_ref[r, 2 * heads * kc + h * vc : 2 * heads * kc + (h + 1) * vc]
            states = jnp.concatenate([ahead[b], behind[b]], axis=1)
            mixed = lax.dot_general(
                queries_fb[b], states, (((1,), (1,)), ((), ())), preferred_element_type=f32
            ) + jnp.dot(scores[b], v, preferred_element_type=f32)
            scale = lax.rsqrt(jnp.mean(mixed * mixed, axis=-1, keepdims=True) + 1e-06)
            out_ref[r, h * vc : (h + 1) * vc] = (mixed * scale * gain_ref[...]).astype(bf16)


def attention(qkv, lowrank, second_factor, bias, extra, gain):
    rows = qkv.shape[0]
    heads = extra.shape[1]
    width = heads * gain.shape[0]
    kc = second_factor.shape[1] // heads
    return pl.pallas_call(
        functools.partial(attention_kernel, heads),
        out_shape=jax.ShapeDtypeStruct((rows, width), jnp.bfloat16),
        in_specs=[pl.BlockSpec(memory_space=pltpu.VMEM)] * 6,
        out_specs=pl.BlockSpec(memory_space=pltpu.VMEM),
        compiler_params=pltpu.CompilerParams(vmem_limit_bytes=32 * 1024 * 1024),
        cost_estimate=pl.CostEstimate(
            flops=40 * rows * kc * width, bytes_accessed=4 * rows * width * 2, transcendentals=0
        ),
    )(qkv, lowrank, second_factor, bias[None, :], extra, gain[None, :])


def gather_shared(piece, chunks=1):
    copies = lax.axis_size("grp")
    if copies != 2 or piece.shape[1] % (copies * chunks):
        return [(lax.all_gather(piece, "fs", axis=0, tiled=True), None)]
    wide = piece.shape[1] // chunks
    part = wide // copies
    pairs = []
    for chunk in range(chunks):
        start = chunk * wide + lax.axis_index("grp") * part
        own = lax.all_gather(
            lax.dynamic_slice_in_dim(piece, start, part, 1), "fs", axis=0, tiled=True
        )
        pairs.append((own, lax.ppermute(own, "grp", [(0, 1), (1, 0)])))
    return pairs


def in_order(pairs):
    if pairs[0][1] is None:
        return pairs[0][0]
    first = lax.axis_index("grp") == 0
    blocks = []
    for own, other in pairs:
        blocks += [jnp.where(first, own, other), jnp.where(first, other, own)]
    return jnp.concatenate(blocks, axis=1)


def times(left, right):
    if right is None:
        return None
    return jnp.dot(left, right, preferred_element_type=jnp.float32)


def shared_dot(left, pairs):
    def rounded(right):
        return None if right is None else times(left, right).astype(jnp.bfloat16)

    return in_order([(rounded(own), rounded(other)) for own, other in pairs])


def gated(second, gate_weight, up_weight):
    if gate_weight is None:
        return None
    gate, up = times(second, gate_weight), times(second, up_weight)
    return (jax.nn.silu(gate) * up).astype(jnp.bfloat16)


def step_back(values, hops):
    count = lax.axis_size("tp")
    return lax.ppermute(values, "tp", [(i, (i - hops) % count) for i in range(count)])


def step_on(values, hops):
    count = lax.axis_size("tp")
    return lax.ppermute(values, "tp", [(i, (i + hops) % count) for i in range(count)])


def scatter_sum(partial, share):
    count = lax.axis_size("tp")
    total = partial[:share].astype(jnp.float32)
    arrived = [step_back(partial[j * share : (j + 1) * share], j) for j in range(1, count)]
    for block in arrived:
        total = total + block.astype(jnp.float32)
    return total


def fused_kernel(
    shape,
    x_ref,
    gain1_ref,
    first_ref,
    second_ref,
    bias_ref,
    extra_ref,
    hgain_ref,
    gain2_ref,
    q_hbm,
    k_hbm,
    v_hbm,
    o_hbm,
    g_hbm,
    u_hbm,
    d_hbm,
    out_hbm,
    qkv_w,
    out_w,
    gate_w,
    up_w,
    down_w,
    normed,
    lowrank,
    qkv,
    headed,
    part,
    got1,
    resid,
    second,
    hidden,
    part2,
    got2,
    done,
    s_right,
    s_left,
    s_grp,
    r_line,
    r_grp,
    local,
    s_sum1,
    r_sum1,
    s_all1,
    r_all1,
    s_sum2,
    r_sum2,
    s_all2,
    r_all2,
    store,
):
    n, count, heads, chunks = shape
    f32, bf16 = jnp.float32, jnp.bfloat16
    z, y, me = lax.axis_index("fs"), lax.axis_index("grp"), lax.axis_index("tp")
    rows, width = x_ref.shape
    share = rows // count
    wide = width // chunks
    kcols, vcols = q_hbm.shape[1], v_hbm.shape[1]

    def whole(ref):
        return ref.shape[1]

    items = [
        (q_hbm, 0, qkv_w, 0, kcols),
        (k_hbm, 0, qkv_w, kcols, kcols),
        (v_hbm, 0, qkv_w, 2 * kcols, vcols),
        (o_hbm, 0, out_w, 0, whole(o_hbm)),
        (g_hbm, 0, gate_w, 0, whole(g_hbm)),
        (u_hbm, 0, up_w, 0, whole(u_hbm)),
    ] + [(d_hbm, c * wide, down_w, c * wide, wide) for c in range(chunks)]
    groups = [[0, 1, 2], [3], [4], [5]] + [[6 + c] for c in range(chunks)]

    def remote(source, target, send, recv, where):
        return pltpu.make_async_remote_copy(
            src_ref=source,
            dst_ref=target,
            send_sem=send,
            recv_sem=recv,
            device_id=where,
            device_id_type=pl.DeviceIdType.MESH,
        )

    def half_rows(i):
        return items[i][0].shape[0] // 2

    def piece(i, origin, half):
        _, _, target, column, size = items[i]
        high = half_rows(i)
        start = pl.multiple_of((2 * origin + half) * high, high)
        return target.at[pl.ds(start, high), pl.ds(column, size)]

    def own_piece(i):
        source, column, _, _, size = items[i]
        high = half_rows(i)
        return source.at[pl.ds(pl.multiple_of(y * high, high), high), pl.ds(column, size)]

    def to_right(i, origin, source):
        return remote(
            source, piece(i, origin, y), s_right.at[i, origin], r_line.at[i, origin], {"fs": z + 1}
        )

    def to_left(i, origin, source):
        return remote(
            source, piece(i, origin, y), s_left.at[i, origin], r_line.at[i, origin], {"fs": z - 1}
        )

    def to_grp(i, origin, half):
        block = piece(i, origin, half)
        return remote(block, block, s_grp.at[i, origin], r_grp.at[i, origin], {"grp": 1 - y})

    def local_copy(i):
        source, column, target, place, size = items[i]
        high = source.shape[0]
        return pltpu.make_async_copy(
            source.at[:, pl.ds(column, size)],
            target.at[pl.ds(pl.multiple_of(z * high, high), high), pl.ds(place, size)],
            local.at[i],
        )

    def start_own(g):
        for i in groups[g]:
            pl.when(z + 1 < n)(lambda i=i: to_right(i, z, own_piece(i)).start())
            pl.when(z >= 1)(lambda i=i: to_left(i, z, own_piece(i)).start())
            local_copy(i).start()

    def pass_on(g, distances):
        for d in distances:
            for i in groups[g]:

                @pl.when(z >= d)
                def _():
                    low = z - d
                    to_right(i, low, piece(i, low, y)).wait_recv()
                    pl.when(z + 1 < n)(lambda: to_right(i, low, piece(i, low, y)).start())
                    to_grp(i, low, y).start()

                @pl.when(z + d < n)
                def _():
                    high = z + d
                    to_left(i, high, piece(i, high, y)).wait_recv()
                    pl.when(z >= 1)(lambda: to_left(i, high, piece(i, high, y)).start())
                    to_grp(i, high, y).start()

    def complete(g):
        for i in groups[g]:
            local_copy(i).wait()
            for d in range(1, n):
                pl.when(z >= d)(lambda i=i, d=d: to_grp(i, z - d, 1 - y).wait_recv())
                pl.when(z + d < n)(lambda i=i, d=d: to_grp(i, z + d, 1 - y).wait_recv())

    def drain(i):
        pl.when(z + 1 < n)(lambda: to_right(i, z, own_piece(i)).wait_send())
        pl.when(z >= 1)(lambda: to_left(i, z, own_piece(i)).wait_send())
        for d in range(1, n):

            @pl.when(z >= d)
            def _():
                low = z - d
                pl.when(z + 1 < n)(lambda: to_right(i, low, piece(i, low, y)).wait_send())
                to_grp(i, low, y).wait_send()

            @pl.when(z + d < n)
            def _():
                high = z + d
                pl.when(z >= 1)(lambda: to_left(i, high, piece(i, high, y)).wait_send())
                to_grp(i, high, y).wait_send()

    def block_rows(t):
        return pl.ds(pl.multiple_of(t * share, share), share)

    def peer(k):
        return lax.rem(me + k, count)

    def from_peer(k):
        return lax.rem(me + count - k, count)

    def sum1(k, source):
        t = peer(k)
        return remote(
            part.at[block_rows(t)], got1.at[source], s_sum1.at[k], r_sum1.at[source], {"tp": t}
        )

    def all1(k, source):
        block = second.at[block_rows(source)]
        return remote(block, block, s_all1.at[k], r_all1.at[source], {"tp": peer(k)})

    def sum2(c, k, source):
        t = peer(k)
        return remote(
            part2.at[c, block_rows(t)],
            got2.at[c, source],
            s_sum2.at[c, k],
            r_sum2.at[c, source],
            {"tp": t},
        )

    def out_block(c, source):
        return out_hbm.at[block_rows(source), pl.ds(c * wide, wide)]

    def all2(c, k, source):
        return remote(
            done.at[c],
            out_block(c, source),
            s_all2.at[c, k],
            r_all2.at[c, source],
            {"tp": peer(k)},
        )

    others = range(1, count)

    barrier = pltpu.get_barrier_semaphore()

    def greet(where):
        pl.semaphore_signal(
            barrier, inc=1, device_id=where, device_id_type=pl.DeviceIdType.MESH
        )

    greet({"grp": 1 - y})
    for k in others:
        greet({"tp": peer(k)})
    pl.when(z + 1 < n)(lambda: greet({"fs": z + 1}))
    pl.when(z >= 1)(lambda: greet({"fs": z - 1}))
    beside = jnp.minimum(z, 1) + jnp.minimum(n - 1 - z, 1)
    pl.semaphore_wait(barrier, count + beside)

    start_own(0)
    start_own(1)

    tall = min(64, share)

    def norm_step(s, carry):
        r = pl.ds(pl.multiple_of(s * tall, tall), tall)
        normed[r] = norm_rows(x_ref[r], gain1_ref[...]).astype(bf16)
        return carry

    lax.fori_loop(0, rows // tall, norm_step, 0)
    lowrank[...] = jnp.dot(normed[...], first_ref[...], preferred_element_type=f32).astype(bf16)

    def tiles(total, body, tile=256):
        def step(s, carry):
            body(pl.multiple_of(s * tile, tile), tile)
            return carry

        lax.fori_loop(0, total // tile, step, 0)
        if total % tile:
            body(total - total % tile, total % tile)

    every = range(1, n)
    pass_on(0, every)
    start_own(2)
    pass_on(1, every)
    complete(0)

    def project(at, size):
        qkv[:, pl.ds(at, size)] = jnp.dot(
            normed[...], qkv_w[:, pl.ds(at, size)], preferred_element_type=f32
        ).astype(bf16)

    tiles(qkv_w.shape[1], project)
    start_own(3)
    attention_kernel(heads, qkv, lowrank, second_ref, bias_ref, extra_ref, hgain_ref, headed)
    pass_on(2, range(1, 2))
    complete(1)

    def mix(at, size):
        part[:, pl.ds(at, size)] = jnp.dot(
            headed[...], out_w[:, pl.ds(at, size)], preferred_element_type=f32
        ).astype(bf16)

    tiles(width, mix)
    for k in others:
        sum1(k, me).start()
    pass_on(2, range(2, n))
    for k in others:
        sum1(k, from_peer(k)).wait_recv()
    low_tall = min(32, share)

    def residual_step(s, carry):
        r = pl.ds(pl.multiple_of(s * low_tall, low_tall), low_tall)
        own = pl.ds(pl.multiple_of(me * share + s * low_tall, low_tall), low_tall)
        total = part[own].astype(f32)
        for k in others:
            total = total + got1[from_peer(k), r].astype(f32)
        value = (x_ref[own].astype(f32) + total).astype(bf16)
        resid[r] = value
        second[own] = norm_rows(value, gain2_ref[...]).astype(bf16)
        return carry

    lax.fori_loop(0, share // low_tall, residual_step, 0)
    start_own(4)
    start_own(5)
    for k in others:
        all1(k, me).start()
    pass_on(3, every)
    complete(2)
    for k in others:
        all1(k, from_peer(k)).wait_recv()
    start_own(6)
    pass_on(4, every)
    complete(3)

    def gate_up(at, size):
        cols = pl.ds(at, size)
        gate = jnp.dot(second[...], gate_w[:, cols], preferred_element_type=f32)
        up = jnp.dot(second[...], up_w[:, cols], preferred_element_type=f32)
        hidden[:, cols] = (jax.nn.silu(gate) * up).astype(bf16)

    tiles(gate_w.shape[1], gate_up)

    def finish(c):
        for k in others:
            sum2(c, k, from_peer(k)).wait_recv()
        own = block_rows(me)
        cols = pl.ds(c * wide, wide)
        total = part2[c, own].astype(f32)
        for k in others:
            total = total + got2[c, from_peer(k)].astype(f32)
        done[c] = (resid[:, cols].astype(f32) + total).astype(bf16)
        for k in others:
            all2(c, k, me).start()
        pltpu.make_async_copy(done.at[c], out_block(c, me), store.at[c]).start()

    for c in range(chunks):
        if 7 + c < len(groups) and c >= 0:
            start_own(7 + c)
        if 5 + c < len(groups):
            pass_on(5 + c, every)
        complete(4 + c)

        def down(at, size, c=c):
            part2[c, :, pl.ds(at, size)] = jnp.dot(
                hidden[...], down_w[:, pl.ds(c * wide + at, size)], preferred_element_type=f32
            ).astype(bf16)

        tiles(wide, down)
        for k in others:
            sum2(c, k, me).start()
        if c:
            finish(c - 1)
    finish(chunks - 1)
    for c in range(chunks):
        pltpu.make_async_copy(done.at[c], out_block(c, me), store.at[c]).wait()
        for k in others:
            all2(c, k, from_peer(k)).wait_recv()
            all2(c, k, me).wait_send()
            sum2(c, k, me).wait_send()
    for k in others:
        sum1(k, me).wait_send()
        all1(k, me).wait_send()
    for i in range(len(items)):
        drain(i)


def fits(x, projections):
    copies, n, count = (lax.axis_size(a) for a in ("grp", "fs", "tp"))
    rows, width = x.shape
    if copies != 2 or n < 2 or count < 2 or rows % (128 * count) or width % 1024:
        return False
    total = 0
    for p in projections:
        if p.shape[0] % 32 or p.shape[1] % 128:
            return False
        total += n * p.size * p.dtype.itemsize
    return total <= 28 * 2**20 and x.size * x.dtype.itemsize <= 2 * 2**20


def fused(x, gain1, q, k, v, first, second, bias, extra, hgain, o, gain2, g, u, d):
    n, count = lax.axis_size("fs"), lax.axis_size("tp")
    rows, width = x.shape
    share = rows // count
    heads = extra.shape[1]
    chunks = 4
    wide = width // chunks
    items = 6 + chunks
    bf16 = jnp.bfloat16
    vmem, hbm = pl.BlockSpec(memory_space=pltpu.VMEM), pl.BlockSpec(memory_space=pl.ANY)
    qkv_cols = 2 * q.shape[1] + v.shape[1]
    held = heads * hgain.shape[0]
    dma = pltpu.SemaphoreType.DMA
    pairs = (chunks, count)
    return pl.pallas_call(
        functools.partial(fused_kernel, (n, count, heads, chunks)),
        out_shape=jax.ShapeDtypeStruct((rows, width), bf16),
        in_specs=[vmem] * 8 + [hbm] * 7,
        out_specs=hbm,
        scratch_shapes=[
            pltpu.VMEM((n * q.shape[0], qkv_cols), bf16),
            pltpu.VMEM((n * o.shape[0], width), bf16),
            pltpu.VMEM((n * g.shape[0], g.shape[1]), bf16),
            pltpu.VMEM((n * u.shape[0], u.shape[1]), bf16),
            pltpu.VMEM((n * d.shape[0], width), bf16),
            pltpu.VMEM((rows, width), bf16),
            pltpu.VMEM((rows, first.shape[1]), bf16),
            pltpu.VMEM((rows, qkv_cols), bf16),
            pltpu.VMEM((rows, held), bf16),
            pltpu.VMEM((rows, width), bf16),
            pltpu.VMEM((count, share, width), bf16),
            pltpu.VMEM((share, width), bf16),
            pltpu.VMEM((rows, width), bf16),
            pltpu.VMEM((rows, g.shape[1]), bf16),
            pltpu.VMEM((chunks, rows, wide), bf16),
            pltpu.VMEM((chunks, count, share, wide), bf16),
            pltpu.VMEM((chunks, share, wide), bf16),
        ]
        + [dma((items, n))] * 5
        + [dma((items,))]
        + [dma((count,))] * 4
        + [dma(pairs)] * 4
        + [dma((chunks,))],
        compiler_params=pltpu.CompilerParams(
            vmem_limit_bytes=62 * 1024 * 1024, collective_id=0, has_side_effects=True
        ),
    )(x, gain1[None, :], first, second, bias[None, :], extra, hgain[None, :], gain2[None, :], q, k, v, o, g, u, d)


def shards(*arrays):
    x = arrays[0]
    projections = [arrays[i] for i in (2, 3, 4, 10, 12, 13, 14)]
    if fits(x, projections):
        return fused(*arrays)
    return spread(*arrays)


def spread(
    layer_input_tokens,
    attention_norm_gain,
    query_projection,
    key_projection,
    value_projection,
    decay_first_factor,
    decay_second_factor,
    decay_logit_bias,
    extra_log_decay,
    head_output_gain,
    attention_output_projection,
    feedforward_norm_gain,
    gate_projection,
    up_projection,
    down_projection,
):
    rows = layer_input_tokens.shape[0]
    count = lax.axis_size("tp")
    me = lax.axis_index("tp")
    share = rows // count
    qkv_full = gather_shared(
        jnp.concatenate([query_projection, key_projection, value_projection], axis=1)
    )
    out_full = gather_shared(attention_output_projection)
    gate_full = gather_shared(gate_projection)
    up_full = gather_shared(up_projection)
    down_full = gather_shared(down_projection, 2)

    normed = norm_rows(layer_input_tokens, attention_norm_gain).astype(jnp.bfloat16)
    lowrank = jnp.dot(normed, decay_first_factor, preferred_element_type=jnp.float32).astype(
        jnp.bfloat16
    )
    qkv = shared_dot(normed, qkv_full)
    headed = attention(
        qkv, lowrank, decay_second_factor, decay_logit_bias, extra_log_decay, head_output_gain
    )
    turned = jnp.concatenate(
        [
            lax.dynamic_slice_in_dim(headed, lax.rem(me - j + count, count) * share, share, 0)
            for j in range(count)
        ],
        axis=0,
    )
    mixer = scatter_sum(shared_dot(turned, out_full), share)
    own = lax.dynamic_slice_in_dim(layer_input_tokens, me * share, share, 0)
    residual = (own.astype(jnp.float32) + mixer).astype(jnp.bfloat16)
    mine = norm_rows(residual, feedforward_norm_gain).astype(jnp.bfloat16)
    second = jnp.concatenate([mine] + [step_on(mine, j) for j in range(1, count)], axis=0)
    hidden = in_order(
        [
            (gated(second, g_own, u_own), gated(second, g_other, u_other))
            for (g_own, g_other), (u_own, u_other) in zip(gate_full, up_full)
        ]
    )
    channel = scatter_sum(shared_dot(hidden, down_full), share)
    finished = (residual.astype(jnp.float32) + channel).astype(jnp.bfloat16)
    return lax.all_gather(finished, "tp", axis=0, tiled=True)


def solution(mesh):
    placed = (
        P(("grp", "fs"), None),
        P(),
        P("fs", "tp"),
        P("fs", "tp"),
        P("fs", "tp"),
        P(),
        P(None, "tp"),
        P("tp"),
        P(("grp", "fs"), "tp"),
        P(),
        P(("tp", "fs"), None),
        P(),
        P("fs", "tp"),
        P("fs", "tp"),
        P(("tp", "fs"), None),
    )
    return jax.shard_map(
        shards, mesh=mesh, in_specs=placed, out_specs=P(("grp", "fs"), None), check_vma=False
    )
```

```python
import functools

import jax
import jax.numpy as jnp
from jax import lax
from jax.experimental import pallas as pl
from jax.experimental.pallas import tpu as pltpu
from jax.sharding import PartitionSpec as P

BLOCK = 64
DECAY_GATE = 16.0


def norm_rows(values, gain):
    wide = values.astype(jnp.float32)
    scale = lax.rsqrt(jnp.mean(wide * wide, axis=-1, keepdims=True) + 1e-06)
    return wide * scale * gain


def attention_kernel(heads, qkv_ref, lowrank_ref, second_ref, bias_ref, extra_ref, gain_ref, out_ref):
    rows = qkv_ref.shape[0]
    kc = second_ref.shape[1] // heads
    vc = out_ref.shape[1] // heads
    count = rows // BLOCK
    f32, bf16 = jnp.float32, jnp.bfloat16
    row_id = lax.broadcasted_iota(jnp.int32, (BLOCK, BLOCK), 0)
    col_id = lax.broadcasted_iota(jnp.int32, (BLOCK, BLOCK), 1)
    lower = row_id >= col_id
    upper = row_id <= col_id
    lower_ones = jnp.where(lower, 1.0, 0.0).astype(f32)
    half = BLOCK // 2
    for h in range(heads):
        kcols = slice(h * kc, (h + 1) * kc)
        logits = (
            jnp.dot(lowrank_ref[...], second_ref[:, kcols], preferred_element_type=f32)
            + bias_ref[:, kcols]
        )
        log_sig = jnp.minimum(logits, 0.0) - jnp.log1p(jnp.exp(-jnp.abs(logits)))
        decay = log_sig / DECAY_GATE + extra_ref[:, h : h + 1]
        queries_fb, updates, closings, scores = [], [], [], []
        for b in range(count):
            r = slice(b * BLOCK, (b + 1) * BLOCK)
            d = decay[r]
            q = qkv_ref[r, h * kc : (h + 1) * kc].astype(f32)
            k = qkv_ref[r, (heads + h) * kc : (heads + h + 1) * kc].astype(f32)
            v = qkv_ref[r, 2 * heads * kc + h * vc : 2 * heads * kc + (h + 1) * vc]
            run = jnp.dot(lower_ones, d, precision=lax.Precision.HIGHEST, preferred_element_type=f32)
            closing = run[BLOCK - 1 : BLOCK]
            back = closing - run + d
            mid_f = run[half - 1 : half]
            mid_b = back[half : half + 1]
            qf = (q * jnp.exp(run - mid_f)).astype(bf16)
            kf = (k * jnp.exp(mid_f - run)).astype(bf16)
            qb = (q * jnp.exp(back - mid_b)).astype(bf16)
            kb = (k * jnp.exp(mid_b - back)).astype(bf16)
            nt = (((1,), (1,)), ((), ()))
            sf = lax.dot_general(qf, kf, nt, preferred_element_type=f32)
            sb = lax.dot_general(qb, kb, nt, preferred_element_type=f32)
            scores.append(
                (jnp.where(lower, sf, 0.0) + jnp.where(upper, sb, 0.0)).astype(bf16)
            )
            queries_fb.append(
                jnp.concatenate([q * jnp.exp(run), q * jnp.exp(back)], axis=1).astype(bf16)
            )
            keys_fb = jnp.concatenate(
                [k * jnp.exp(closing - run), k * jnp.exp(closing - back)], axis=1
            ).astype(bf16)
            updates.append(
                lax.dot_general(v, keys_fb, (((0,), (0,)), ((), ())), preferred_element_type=f32)
            )
            closings.append(jnp.exp(closing))
        state = jnp.zeros((vc, kc), f32)
        ahead = []
        for b in range(count):
            ahead.append(state.astype(bf16))
            state = state * closings[b] + updates[b][:, :kc]
        state = jnp.zeros((vc, kc), f32)
        behind = [None] * count
        for b in reversed(range(count)):
            behind[b] = state.astype(bf16)
            state = state * closings[b] + updates[b][:, kc:]
        for b in range(count):
            r = slice(b * BLOCK, (b + 1) * BLOCK)
            v = qkv_ref[r, 2 * heads * kc + h * vc : 2 * heads * kc + (h + 1) * vc]
            states = jnp.concatenate([ahead[b], behind[b]], axis=1)
            mixed = lax.dot_general(
                queries_fb[b], states, (((1,), (1,)), ((), ())), preferred_element_type=f32
            ) + jnp.dot(scores[b], v, preferred_element_type=f32)
            scale = lax.rsqrt(jnp.mean(mixed * mixed, axis=-1, keepdims=True) + 1e-06)
            out_ref[r, h * vc : (h + 1) * vc] = (mixed * scale * gain_ref[...]).astype(bf16)


def attention(qkv, lowrank, second_factor, bias, extra, gain):
    rows = qkv.shape[0]
    heads = extra.shape[1]
    width = heads * gain.shape[0]
    kc = second_factor.shape[1] // heads
    return pl.pallas_call(
        functools.partial(attention_kernel, heads),
        out_shape=jax.ShapeDtypeStruct((rows, width), jnp.bfloat16),
        in_specs=[pl.BlockSpec(memory_space=pltpu.VMEM)] * 6,
        out_specs=pl.BlockSpec(memory_space=pltpu.VMEM),
        compiler_params=pltpu.CompilerParams(vmem_limit_bytes=32 * 1024 * 1024),
        cost_estimate=pl.CostEstimate(
            flops=40 * rows * kc * width, bytes_accessed=4 * rows * width * 2, transcendentals=0
        ),
    )(qkv, lowrank, second_factor, bias[None, :], extra, gain[None, :])


def gather_shared(piece, chunks=1):
    copies = lax.axis_size("grp")
    if copies != 2 or piece.shape[1] % (copies * chunks):
        return [(lax.all_gather(piece, "fs", axis=0, tiled=True), None)]
    wide = piece.shape[1] // chunks
    part = wide // copies
    pairs = []
    for chunk in range(chunks):
        start = chunk * wide + lax.axis_index("grp") * part
        own = lax.all_gather(
            lax.dynamic_slice_in_dim(piece, start, part, 1), "fs", axis=0, tiled=True
        )
        pairs.append((own, lax.ppermute(own, "grp", [(0, 1), (1, 0)])))
    return pairs


def in_order(pairs):
    if pairs[0][1] is None:
        return pairs[0][0]
    first = lax.axis_index("grp") == 0
    blocks = []
    for own, other in pairs:
        blocks += [jnp.where(first, own, other), jnp.where(first, other, own)]
    return jnp.concatenate(blocks, axis=1)


def times(left, right):
    if right is None:
        return None
    return jnp.dot(left, right, preferred_element_type=jnp.float32)


def shared_dot(left, pairs):
    def rounded(right):
        return None if right is None else times(left, right).astype(jnp.bfloat16)

    return in_order([(rounded(own), rounded(other)) for own, other in pairs])


def gated(second, gate_weight, up_weight):
    if gate_weight is None:
        return None
    gate, up = times(second, gate_weight), times(second, up_weight)
    return (jax.nn.silu(gate) * up).astype(jnp.bfloat16)


def step_back(values, hops):
    count = lax.axis_size("tp")
    return lax.ppermute(values, "tp", [(i, (i - hops) % count) for i in range(count)])


def step_on(values, hops):
    count = lax.axis_size("tp")
    return lax.ppermute(values, "tp", [(i, (i + hops) % count) for i in range(count)])


def scatter_sum(partial, share):
    count = lax.axis_size("tp")
    total = partial[:share].astype(jnp.float32)
    arrived = [step_back(partial[j * share : (j + 1) * share], j) for j in range(1, count)]
    for block in arrived:
        total = total + block.astype(jnp.float32)
    return total


def fused_kernel(
    shape,
    x_ref,
    gain1_ref,
    first_ref,
    second_ref,
    bias_ref,
    extra_ref,
    hgain_ref,
    gain2_ref,
    q_hbm,
    k_hbm,
    v_hbm,
    o_hbm,
    g_hbm,
    u_hbm,
    d_hbm,
    out_hbm,
    qkv_w,
    out_w,
    gate_w,
    up_w,
    down_w,
    normed,
    lowrank,
    extra,
    qkv,
    headed,
    part1,
    core1,
    send1,
    line1,
    resid,
    second,
    hidden,
    part2,
    core2,
    send2,
    line2,
    send3,
    line3,
    result,
    s_right,
    s_left,
    s_grp,
    r_line,
    r_grp,
    local,
    s_down,
    r_down,
    sy_down,
    ry_down,
    l_down,
    s_sum,
    r_sum,
    s_share,
    r_share,
    s_fin,
    r_fin,
    store,
):
    n, count, heads, chunks, small, parts = shape
    f32, bf16 = jnp.float32, jnp.bfloat16
    z, y, me = lax.axis_index("fs"), lax.axis_index("grp"), lax.axis_index("tp")
    rows, width = x_ref.shape
    share = rows // count
    wide = width // chunks
    kcols, vcols = q_hbm.shape[1], v_hbm.shape[1]
    units = g_hbm.shape[1]
    big = units - small
    xi, ci = me // 2, lax.rem(me, 2)
    core_peer = 2 * xi + 1 - ci
    line_peer = 2 * (1 - xi) + ci
    side = z // 2
    mate = z + 1 - 2 * lax.rem(z, 2)
    partner = lax.rem(z + 2, n)
    inner = lax.rem(z + side, 2) == 1
    outer = jnp.logical_not(inner)
    cross = 2 - side
    far = 3 * (1 - side)

    items = [
        (q_hbm, qkv_w, 0, kcols),
        (k_hbm, qkv_w, kcols, kcols),
        (v_hbm, qkv_w, 2 * kcols, vcols),
        (o_hbm, out_w, 0, width),
        (g_hbm, gate_w, 0, big),
        (u_hbm, up_w, 0, big),
    ]
    QKV, OUT, GATE, UP = [0, 1, 2], [3], 4, 5

    def remote(source, target, send, recv, where):
        return pltpu.make_async_remote_copy(
            src_ref=source,
            dst_ref=target,
            send_sem=send,
            recv_sem=recv,
            device_id=where,
            device_id_type=pl.DeviceIdType.MESH,
        )

    def high_of(i):
        return items[i][0].shape[0] // 2

    def rows_of(i, origin, half):
        high = high_of(i)
        return pl.ds(pl.multiple_of((2 * origin + half) * high, high), high)

    def my_rows(i):
        high = high_of(i)
        return pl.ds(pl.multiple_of(y * high, high), high)

    def all_rows(i, origin):
        high = items[i][0].shape[0]
        return pl.ds(pl.multiple_of(origin * high, high), high)

    def lanes(start, size):
        return pl.ds(pl.multiple_of(start, 128), size)

    def piece(i, origin, half):
        _, target, column, size = items[i]
        return target.at[rows_of(i, origin, half), pl.ds(column, size)]

    def to_right(i, origin, source):
        return remote(
            source, piece(i, origin, y), s_right.at[i, origin], r_line.at[i, origin], {"fs": z + 1}
        )

    def to_left(i, origin, source):
        return remote(
            source, piece(i, origin, y), s_left.at[i, origin], r_line.at[i, origin], {"fs": z - 1}
        )

    def to_grp(i, origin, block):
        return remote(block, block, s_grp.at[i, origin], r_grp.at[i, origin], {"grp": 1 - y})

    def local_copy(i):
        source, target, place, size = items[i]
        return pltpu.make_async_copy(
            source, target.at[all_rows(i, z), pl.ds(place, size)], local.at[i]
        )

    def start_own(group):
        for i in group:
            own = items[i][0].at[my_rows(i)]
            pl.when(z + 1 < n)(lambda i=i, own=own: to_right(i, z, own).start())
            pl.when(z >= 1)(lambda i=i, own=own: to_left(i, z, own).start())
            local_copy(i).start()

    def pass_on(group, distances):
        for d in distances:
            for i in group:

                @pl.when(z >= d)
                def _():
                    low = z - d
                    block = piece(i, low, y)
                    to_right(i, low, block).wait_recv()
                    pl.when(z + 1 < n)(lambda: to_right(i, low, block).start())
                    to_grp(i, low, block).start()

                @pl.when(z + d < n)
                def _():
                    high = z + d
                    block = piece(i, high, y)
                    to_left(i, high, block).wait_recv()
                    pl.when(z >= 1)(lambda: to_left(i, high, block).start())
                    to_grp(i, high, block).start()

    def complete(group):
        for i in group:
            local_copy(i).wait()
            for d in range(1, n):
                for cond, origin in ((z >= d, z - d), (z + d < n, z + d)):
                    pl.when(cond)(
                        lambda i=i, o=origin: to_grp(i, o, piece(i, o, 1 - y)).wait_recv()
                    )

    def drain(group):
        for i in group:
            own = items[i][0].at[my_rows(i)]
            pl.when(z + 1 < n)(lambda: to_right(i, z, own).wait_send())
            pl.when(z >= 1)(lambda: to_left(i, z, own).wait_send())
            for d in range(1, n):

                @pl.when(z >= d)
                def _():
                    low = z - d
                    block = piece(i, low, y)
                    pl.when(z + 1 < n)(lambda: to_right(i, low, block).wait_send())
                    to_grp(i, low, block).wait_send()

                @pl.when(z + d < n)
                def _():
                    high = z + d
                    block = piece(i, high, y)
                    pl.when(z >= 1)(lambda: to_left(i, high, block).wait_send())
                    to_grp(i, high, block).wait_send()

    narrow = lanes(side * (big - small), small)

    def block_at(i, origin, half, ends):
        target = items[i][1]
        r = rows_of(i, origin, half)
        return target.at[r, narrow] if ends else target.at[r]

    def own_to_mate(i, ends):
        source = items[i][0]
        if ends:
            sent, block = source.at[my_rows(i), lanes(side * small, big)], block_at(i, z, y, False)
        else:
            sent, block = source.at[my_rows(i), lanes(side * big, small)], block_at(i, z, y, True)
        return remote(sent, block, s_right.at[i, z], r_line.at[i, z], {"fs": mate})

    def own_to_cross(i):
        sent = items[i][0].at[my_rows(i), lanes((1 - side) * small, big)]
        return remote(
            sent, block_at(i, z, y, False), s_left.at[i, z], r_line.at[i, z], {"fs": cross}
        )

    def on_to_mate(i, origin):
        block = block_at(i, origin, y, True)
        return remote(block, block, s_right.at[i, origin], r_line.at[i, origin], {"fs": mate})

    def keep(i, ends):
        source, target = items[i][0], items[i][1]
        r = all_rows(i, z)
        if ends:
            return pltpu.make_async_copy(
                source.at[:, lanes(side * big, small)], target.at[r, narrow], local.at[i]
            )
        return pltpu.make_async_copy(
            source.at[:, lanes(side * small, big)], target.at[r], local.at[i]
        )

    origins = (mate, cross, far)

    def start_cut(i):
        pl.when(inner)(lambda: own_to_mate(i, False).start())
        own_to_cross(i).start()
        pl.when(outer)(lambda: own_to_mate(i, True).start())
        pl.when(inner)(lambda: keep(i, False).start())
        pl.when(outer)(lambda: keep(i, True).start())

    def arrived(i, origin, ends):
        block = block_at(i, origin, y, ends)
        return remote(block, block, s_right.at[i, origin], r_line.at[i, origin], {"fs": mate})

    def pass_cut(i, steps):
        for k in steps:
            origin = origins[k]

            @pl.when(inner)
            def _():
                arrived(i, origin, False).wait_recv()
                if k:
                    on_to_mate(i, origin).start()
                to_grp(i, origin, block_at(i, origin, y, False)).start()

            @pl.when(outer)
            def _():
                arrived(i, origin, True).wait_recv()
                to_grp(i, origin, block_at(i, origin, y, True)).start()

    def complete_cut(i):
        @pl.when(inner)
        def _():
            keep(i, False).wait()
            for origin in origins:
                to_grp(i, origin, block_at(i, origin, 1 - y, False)).wait_recv()

        @pl.when(outer)
        def _():
            keep(i, True).wait()
            for origin in origins:
                to_grp(i, origin, block_at(i, origin, 1 - y, True)).wait_recv()

    def drain_cut(i):
        own_to_cross(i).wait_send()

        @pl.when(inner)
        def _():
            own_to_mate(i, False).wait_send()
            for k in range(3):
                if k:
                    on_to_mate(i, origins[k]).wait_send()
                to_grp(i, origins[k], block_at(i, origins[k], y, False)).wait_send()

        @pl.when(outer)
        def _():
            own_to_mate(i, True).wait_send()
            for k in range(3):
                to_grp(i, origins[k], block_at(i, origins[k], y, True)).wait_send()

    depth = d_hbm.shape[0]
    sub, rest = small - depth, big - 2 * depth

    def down_block(c, start, size):
        return down_w.at[pl.ds(pl.multiple_of(start, 16), size), pl.ds(c * wide, wide)]

    def down_src(c, start, size):
        return d_hbm.at[pl.ds(pl.multiple_of(start, 16), size), pl.ds(c * wide, wide)]

    def mate_rows(c, origin, half, to_inner):
        base = origin * depth - side * small
        if to_inner:
            return down_block(c, base + half * (depth // 2), depth // 2)
        return down_block(c, base + side * (depth - sub) + half * (sub // 2), sub // 2)

    def cross_rows(c, half):
        start = cross * depth + side * (depth - rest) - side * small
        return down_block(c, start + half * (rest // 2), rest // 2)

    def down_to_mate(c, to_inner):
        if to_inner:
            sent = down_src(c, y * (depth // 2), depth // 2)
        else:
            sent = down_src(c, side * (depth - sub) + y * (sub // 2), sub // 2)
        return remote(
            sent, mate_rows(c, z, y, to_inner), s_down.at[c, 0], r_down.at[c, 0], {"fs": mate}
        )

    def down_to_cross(c):
        start = (1 - side) * (depth - rest) + y * (rest // 2)
        place = z * depth + start - (1 - side) * small
        return remote(
            down_src(c, start, rest // 2),
            down_block(c, place, rest // 2),
            s_down.at[c, 1],
            r_down.at[c, 1],
            {"fs": cross},
        )

    def down_local(c):
        return pltpu.make_async_copy(
            down_src(c, 0, depth), down_block(c, z * depth - side * small, depth), l_down.at[c]
        )

    def down_grp(c, k, block):
        return remote(block, block, sy_down.at[c, k], ry_down.at[c, k], {"grp": 1 - y})

    def start_down(c):
        pl.when(outer)(lambda: down_to_mate(c, True).start())

        @pl.when(inner)
        def _():
            down_to_mate(c, False).start()
            down_to_cross(c).start()

        down_local(c).start()

    def down_arrival(c, k, block):
        return remote(block, block, s_down.at[c, k], r_down.at[c, k], {"fs": mate})

    def pass_down(c):
        @pl.when(outer)
        def _():
            block = mate_rows(c, mate, y, False)
            down_arrival(c, 0, block).wait_recv()
            down_grp(c, 0, block).start()

        @pl.when(inner)
        def _():
            for k, block in ((0, mate_rows(c, mate, y, True)), (1, cross_rows(c, y))):
                down_arrival(c, k, block).wait_recv()
                down_grp(c, k, block).start()

    def complete_down(c):
        down_local(c).wait()
        pl.when(outer)(lambda: down_grp(c, 0, mate_rows(c, mate, 1 - y, False)).wait_recv())

        @pl.when(inner)
        def _():
            down_grp(c, 0, mate_rows(c, mate, 1 - y, True)).wait_recv()
            down_grp(c, 1, cross_rows(c, 1 - y)).wait_recv()

    def drain_down(c):
        @pl.when(outer)
        def _():
            down_to_mate(c, True).wait_send()
            down_grp(c, 0, mate_rows(c, mate, y, False)).wait_send()

        @pl.when(inner)
        def _():
            down_to_mate(c, False).wait_send()
            down_to_cross(c).wait_send()
            down_grp(c, 0, mate_rows(c, mate, y, True)).wait_send()
            down_grp(c, 1, cross_rows(c, y)).wait_send()

    def sum_core1(c):
        return remote(
            part1.at[c, :, 1 - ci], core1.at[c], s_sum.at[c, 0], r_sum.at[c, 0], {"tp": core_peer}
        )

    def sum_line1(c):
        return remote(
            send1.at[c], line1.at[c], s_sum.at[c, 1], r_sum.at[c, 1], {"tp": line_peer}
        )

    def sum_core2(c):
        return remote(
            part2.at[c, :, :, 1 - ci],
            core2.at[c],
            s_sum.at[c, 2],
            r_sum.at[c, 2],
            {"tp": core_peer},
        )

    def sum_line2(c):
        return remote(
            send2.at[c], line2.at[c], s_sum.at[c, 3], r_sum.at[c, 3], {"tp": line_peer}
        )

    def sum_line3(c):
        return remote(
            send3.at[c], line3.at[c], s_sum.at[c, 4], r_sum.at[c, 4], {"fs": partner}
        )

    lump = share // parts

    def rows_at(which, t, p):
        start = pl.multiple_of(which * rows + t * share + p * lump, lump)
        return second.at[pl.ds(start, lump)]

    def give(p, slot, which, t, where, target=None):
        block = rows_at(which, t, p)
        return remote(
            block,
            block if target is None else target,
            s_share.at[slot, p],
            r_share.at[slot, p],
            where,
        )

    def to_partner(p):
        return give(p, 0, 0, me, {"fs": partner}, rows_at(1, me, p))

    def across(p, which):
        return give(p, 1 + which, which, me, {"tp": line_peer})

    def across_arrival(p, which):
        return give(p, 1 + which, which, line_peer, {"tp": line_peer})

    def over(p, which, mine):
        return give(p, 3 + 2 * which + (1 - mine), which, me if mine else line_peer, {"tp": core_peer})

    def over_arrival(p, which, mine):
        t = core_peer if mine else 2 * (1 - xi) + 1 - ci
        return give(p, 3 + 2 * which + (1 - mine), which, t, {"tp": core_peer})

    def fin(c, slot, t, where):
        block = result.at[c, t]
        return remote(block, block, s_fin.at[c, slot], r_fin.at[c, slot], where)

    def put(c, t):
        r = pl.ds(pl.multiple_of(t * share, share), share)
        return pltpu.make_async_copy(
            result.at[c, t], out_hbm.at[r, pl.ds(c * wide, wide)], store.at[c, t]
        )

    barrier = pltpu.get_barrier_semaphore()

    def greet(where):
        pl.semaphore_signal(
            barrier, inc=1, device_id=where, device_id_type=pl.DeviceIdType.MESH
        )

    for where in ({"grp": 1 - y}, {"tp": core_peer}, {"tp": line_peer}, {"fs": partner}):
        greet(where)
    pl.when(z + 1 < n)(lambda: greet({"fs": z + 1}))
    pl.when(z >= 1)(lambda: greet({"fs": z - 1}))
    pl.semaphore_wait(barrier, 4 + jnp.minimum(z, 1) + jnp.minimum(n - 1 - z, 1))

    start_own(QKV)

    @pl.when(outer)
    def _():
        unused = (1 - side) * small
        hidden[:, lanes(unused, big - small)] = jnp.zeros((2 * rows, big - small), bf16)
        down_w[pl.ds(pl.multiple_of(unused, 128), big - small)] = jnp.zeros(
            (big - small, width), bf16
        )

    tall = min(64, share)

    def norm_step(s, carry):
        r = pl.ds(pl.multiple_of(s * tall, tall), tall)
        normed[r] = norm_rows(x_ref[r], gain1_ref[...]).astype(bf16)
        return carry

    lax.fori_loop(0, rows // tall, norm_step, 0)
    lowrank[...] = lax.dot_general(
        normed[...], first_ref[...], (((1,), (1,)), ((), ())), preferred_element_type=f32
    ).astype(bf16)
    extra[...] = extra_ref[...].T

    def tiles(total, body, tile=256):
        def step(s, carry):
            body(pl.multiple_of(s * tile, tile), tile)
            return carry

        lax.fori_loop(0, total // tile, step, 0)
        if total % tile:
            body(total - total % tile, total % tile)

    pass_on(QKV, (1, 2))
    start_own(OUT)
    pass_on(QKV, (3,))
    start_cut(GATE)
    pass_on(OUT, (1,))
    complete(QKV)

    def project(at, size):
        qkv[:, pl.ds(at, size)] = jnp.dot(
            normed[...], qkv_w[:, pl.ds(at, size)], preferred_element_type=f32
        ).astype(bf16)

    tiles(qkv_w.shape[1], project)
    pass_on(OUT, (2,))
    attention_kernel(heads, qkv, lowrank, second_ref, bias_ref, extra, hgain_ref, headed)
    pass_on(OUT, (3,))
    start_cut(UP)
    complete(OUT)

    for c in range(chunks):
        mixed = jnp.dot(
            headed[...], out_w[:, c * wide : (c + 1) * wide], preferred_element_type=f32
        ).astype(bf16)
        part1[c] = mixed.reshape(2, 2, share, wide)
        sum_core1(c).start()
    pass_cut(GATE, (0,))
    for c in range(chunks):
        sum_core1(c).wait_recv()
        send1[c] = (part1[c, 1 - xi, ci].astype(f32) + core1[c, 1 - xi].astype(f32)).astype(bf16)
        sum_line1(c).start()
    pass_cut(GATE, (1,))
    own = pl.ds(pl.multiple_of(me * share, share), share)
    for c in range(chunks):
        sum_line1(c).wait_recv()
        cols = slice(c * wide, (c + 1) * wide)
        total = part1[c, xi, ci].astype(f32) + core1[c, xi].astype(f32) + line1[c].astype(f32)
        resid[:, cols] = (x_ref[own, cols].astype(f32) + total).astype(bf16)
    for p in range(parts):
        value = resid[p * lump : (p + 1) * lump]
        start = pl.multiple_of(me * share + p * lump, lump)
        second[pl.ds(start, lump)] = norm_rows(value, gain2_ref[...]).astype(bf16)
        to_partner(p).start()
        across(p, 0).start()
        over(p, 0, 1).start()

    pass_cut(GATE, (2,))
    pass_cut(UP, (0,))
    for p in range(parts):
        across_arrival(p, 0).wait_recv()
        over(p, 0, 0).start()
    pass_cut(UP, (1,))
    for p in range(parts):
        give(p, 0, 1, me, {"fs": partner}).wait_recv()
        across(p, 1).start()
        over(p, 1, 1).start()
    pass_cut(UP, (2,))
    for c in range(chunks):
        start_down(c)
    complete_cut(GATE)
    complete_cut(UP)
    for p in range(parts):
        over_arrival(p, 0, 1).wait_recv()
        over_arrival(p, 0, 0).wait_recv()

    def gate_up(which):
        def step(s, carry):
            cols = pl.ds(pl.multiple_of(first_tile + s * 128, 128), 128)
            r = slice(which * rows, (which + 1) * rows)
            both = jnp.dot(
                second[r],
                jnp.concatenate([gate_w[:, cols], up_w[:, cols]], axis=1),
                preferred_element_type=f32,
            )
            hidden[r, cols] = (jax.nn.silu(both[:, :128]) * both[:, 128:]).astype(bf16)
            return carry

        first_tile = jnp.where(inner, 0, side * (big - small))
        lax.fori_loop(0, jnp.where(inner, big // 128, small // 128), step, 0)

    gate_up(0)
    for p in range(parts):
        across_arrival(p, 1).wait_recv()
        over(p, 1, 0).start()
    for p in range(parts):
        over_arrival(p, 1, 1).wait_recv()
        over_arrival(p, 1, 0).wait_recv()
    gate_up(1)

    def sum_a(c):
        pass_down(c)
        complete_down(c)
        for which in range(2):
            out = jnp.dot(
                hidden[which * rows : (which + 1) * rows],
                down_w[:, c * wide : (c + 1) * wide],
                preferred_element_type=f32,
            ).astype(bf16)
            part2[c, which] = out.reshape(2, 2, share, wide)
        sum_core2(c).start()

    def sum_b(c):
        sum_core2(c).wait_recv()
        for which in range(2):
            send2[c, which] = (
                part2[c, which, 1 - xi, ci].astype(f32) + core2[c, which, 1 - xi].astype(f32)
            ).astype(bf16)
        sum_line2(c).start()

    def held(c, which):
        return (
            part2[c, which, xi, ci].astype(f32)
            + core2[c, which, xi].astype(f32)
            + line2[c, which].astype(f32)
        )

    def sum_c(c):
        sum_line2(c).wait_recv()
        send3[c] = held(c, 1).astype(bf16)
        sum_line3(c).start()

    def sum_d(c):
        sum_line3(c).wait_recv()
        total = held(c, 0) + line3[c].astype(f32)
        value = resid[:, c * wide : (c + 1) * wide].astype(f32) + total
        result[c, me] = value.astype(bf16)
        fin(c, 0, me, {"tp": line_peer}).start()
        fin(c, 1, me, {"tp": core_peer}).start()
        put(c, me).start()

    def sum_e(c):
        fin(c, 0, line_peer, {"tp": line_peer}).wait_recv()
        fin(c, 2, line_peer, {"tp": core_peer}).start()
        put(c, line_peer).start()

    corner = 2 * (1 - xi) + 1 - ci

    def sum_f(c):
        fin(c, 1, core_peer, {"tp": core_peer}).wait_recv()
        put(c, core_peer).start()
        fin(c, 2, corner, {"tp": core_peer}).wait_recv()
        put(c, corner).start()

    stages = (sum_a, sum_b, sum_c, sum_d, sum_e, sum_f)
    for step in range(chunks + len(stages) - 1):
        for k, stage in enumerate(stages):
            if 0 <= step - k < chunks:
                stage(step - k)

    for c in range(chunks):
        for t in (me, core_peer, line_peer, corner):
            put(c, t).wait()
        fin(c, 0, me, {"tp": line_peer}).wait_send()
        fin(c, 1, me, {"tp": core_peer}).wait_send()
        fin(c, 2, line_peer, {"tp": core_peer}).wait_send()
        for copy in (sum_core1, sum_line1, sum_core2, sum_line2, sum_line3):
            copy(c).wait_send()
        drain_down(c)
    for p in range(parts):
        to_partner(p).wait_send()
        for which in range(2):
            across(p, which).wait_send()
            over(p, which, 1).wait_send()
            over(p, which, 0).wait_send()
    drain(QKV)
    drain(OUT)
    drain_cut(GATE)
    drain_cut(UP)


def narrow_units(units):
    return units // 128 // 2 * 128


def fits(x, q, k, v, o, g, u, d):
    copies, n, count = (lax.axis_size(a) for a in ("grp", "fs", "tp"))
    rows, width = x.shape
    if (copies, n, count) != (2, 4, 4) or rows % (64 * count) or width % 512:
        return False
    for p in (q, k, v, o, g, u, d):
        if p.shape[0] % 32 or p.shape[1] % 128:
            return False
    units, depth = g.shape[1], d.shape[0]
    small = narrow_units(units)
    sub, rest = small - depth, units - small - 2 * depth
    if min(sub, rest) <= 0 or sub % 32 or rest % 32:
        return False
    held = n * (q.size + k.size + v.size + o.size) + 3 * (units - small) * n * g.shape[0]
    return 2 * held + 24 * x.size <= 54 * 2**20


def fused(x, gain1, q, k, v, first, second, bias, extra, hgain, o, gain2, g, u, d):
    n, count = lax.axis_size("fs"), lax.axis_size("tp")
    rows, width = x.shape
    share = rows // count
    heads = extra.shape[1]
    chunks, parts = 4, 2
    wide = width // chunks
    bf16, f32 = jnp.bfloat16, jnp.float32
    vmem, hbm = pl.BlockSpec(memory_space=pltpu.VMEM), pl.BlockSpec(memory_space=pl.ANY)
    qkv_cols = 2 * q.shape[1] + v.shape[1]
    held = heads * hgain.shape[0]
    units = g.shape[1]
    small = narrow_units(units)
    big = units - small
    buffers = [
        ((n * q.shape[0], qkv_cols), bf16),
        ((n * o.shape[0], width), bf16),
        ((n * g.shape[0], big), bf16),
        ((n * u.shape[0], big), bf16),
        ((big, width), bf16),
        ((rows, width), bf16),
        ((rows, first.shape[1]), bf16),
        ((rows, heads), f32),
        ((rows, qkv_cols), bf16),
        ((rows, held), bf16),
        ((chunks, 2, 2, share, wide), bf16),
        ((chunks, 2, share, wide), bf16),
        ((chunks, share, wide), bf16),
        ((chunks, share, wide), bf16),
        ((share, width), bf16),
        ((2 * rows, width), bf16),
        ((2 * rows, big), bf16),
        ((chunks, 2, 2, 2, share, wide), bf16),
        ((chunks, 2, 2, share, wide), bf16),
        ((chunks, 2, share, wide), bf16),
        ((chunks, 2, share, wide), bf16),
        ((chunks, share, wide), bf16),
        ((chunks, share, wide), bf16),
        ((chunks, count, share, wide), bf16),
    ]
    counts = [(6, n)] * 5 + [(6,)] + [(chunks, 2)] * 4 + [(chunks,)]
    counts += [(chunks, 5)] * 2 + [(7, parts)] * 2 + [(chunks, 3)] * 2 + [(chunks, count)]
    return pl.pallas_call(
        functools.partial(fused_kernel, (n, count, heads, chunks, small, parts)),
        out_shape=jax.ShapeDtypeStruct((rows, width), bf16),
        in_specs=[vmem] * 8 + [hbm] * 7,
        out_specs=hbm,
        scratch_shapes=[pltpu.VMEM(s, t) for s, t in buffers]
        + [pltpu.SemaphoreType.DMA(s) for s in counts],
        compiler_params=pltpu.CompilerParams(
            vmem_limit_bytes=62 * 1024 * 1024, collective_id=0, has_side_effects=True
        ),
    )(x, gain1[None, :], first.T, second, bias[None, :], extra.T, hgain[None, :], gain2[None, :], q, k, v, o, g, u, d)


def shards(*arrays):
    if fits(*[arrays[i] for i in (0, 2, 3, 4, 10, 12, 13, 14)]):
        return fused(*arrays)
    return spread(*arrays)


def spread(
    layer_input_tokens,
    attention_norm_gain,
    query_projection,
    key_projection,
    value_projection,
    decay_first_factor,
    decay_second_factor,
    decay_logit_bias,
    extra_log_decay,
    head_output_gain,
    attention_output_projection,
    feedforward_norm_gain,
    gate_projection,
    up_projection,
    down_projection,
):
    rows = layer_input_tokens.shape[0]
    count = lax.axis_size("tp")
    me = lax.axis_index("tp")
    share = rows // count
    qkv_full = gather_shared(
        jnp.concatenate([query_projection, key_projection, value_projection], axis=1)
    )
    out_full = gather_shared(attention_output_projection)
    gate_full = gather_shared(gate_projection)
    up_full = gather_shared(up_projection)
    down_full = gather_shared(down_projection, 2)

    normed = norm_rows(layer_input_tokens, attention_norm_gain).astype(jnp.bfloat16)
    lowrank = jnp.dot(normed, decay_first_factor, preferred_element_type=jnp.float32).astype(
        jnp.bfloat16
    )
    qkv = shared_dot(normed, qkv_full)
    headed = attention(
        qkv, lowrank, decay_second_factor, decay_logit_bias, extra_log_decay, head_output_gain
    )
    turned = jnp.concatenate(
        [
            lax.dynamic_slice_in_dim(headed, lax.rem(me - j + count, count) * share, share, 0)
            for j in range(count)
        ],
        axis=0,
    )
    mixer = scatter_sum(shared_dot(turned, out_full), share)
    own = lax.dynamic_slice_in_dim(layer_input_tokens, me * share, share, 0)
    residual = (own.astype(jnp.float32) + mixer).astype(jnp.bfloat16)
    mine = norm_rows(residual, feedforward_norm_gain).astype(jnp.bfloat16)
    second = jnp.concatenate([mine] + [step_on(mine, j) for j in range(1, count)], axis=0)
    hidden = in_order(
        [
            (gated(second, g_own, u_own), gated(second, g_other, u_other))
            for (g_own, g_other), (u_own, u_other) in zip(gate_full, up_full)
        ]
    )
    channel = scatter_sum(shared_dot(hidden, down_full), share)
    finished = (residual.astype(jnp.float32) + channel).astype(jnp.bfloat16)
    return lax.all_gather(finished, "tp", axis=0, tiled=True)


def solution(mesh):
    placed = (
        P(("grp", "fs"), None),
        P(),
        P("fs", "tp"),
        P("fs", "tp"),
        P("fs", "tp"),
        P(),
        P(None, "tp"),
        P("tp"),
        P(("grp", "fs"), "tp"),
        P(),
        P(("tp", "fs"), None),
        P(),
        P("fs", "tp"),
        P("fs", "tp"),
        P(("tp", "fs"), None),
    )
    return jax.shard_map(
        shards, mesh=mesh, in_specs=placed, out_specs=P(("grp", "fs"), None), check_vma=False
    )
```

```python
import functools

import jax
import jax.numpy as jnp
from jax import lax
from jax.experimental import pallas as pl
from jax.experimental.pallas import tpu as pltpu
from jax.sharding import PartitionSpec as P

BLOCK = 64
DECAY_GATE = 16.0


def norm_rows(values, gain):
    wide = values.astype(jnp.float32)
    scale = lax.rsqrt(jnp.mean(wide * wide, axis=-1, keepdims=True) + 1e-06)
    return wide * scale * gain


def attention_kernel(heads, qkv_ref, lowrank_ref, second_ref, bias_ref, extra_ref, gain_ref, out_ref):
    rows = qkv_ref.shape[0]
    kc = second_ref.shape[1] // heads
    vc = out_ref.shape[1] // heads
    count = rows // BLOCK
    f32, bf16 = jnp.float32, jnp.bfloat16
    row_id = lax.broadcasted_iota(jnp.int32, (BLOCK, BLOCK), 0)
    col_id = lax.broadcasted_iota(jnp.int32, (BLOCK, BLOCK), 1)
    lower = row_id >= col_id
    upper = row_id <= col_id
    lower_ones = jnp.where(lower, 1.0, 0.0).astype(f32)
    half = BLOCK // 2
    for h in range(heads):
        kcols = slice(h * kc, (h + 1) * kc)
        logits = (
            jnp.dot(lowrank_ref[...], second_ref[:, kcols], preferred_element_type=f32)
            + bias_ref[:, kcols]
        )
        log_sig = jnp.minimum(logits, 0.0) - jnp.log1p(jnp.exp(-jnp.abs(logits)))
        decay = log_sig / DECAY_GATE + extra_ref[:, h : h + 1]
        queries_fb, updates, closings, scores = [], [], [], []
        for b in range(count):
            r = slice(b * BLOCK, (b + 1) * BLOCK)
            d = decay[r]
            q = qkv_ref[r, h * kc : (h + 1) * kc].astype(f32)
            k = qkv_ref[r, (heads + h) * kc : (heads + h + 1) * kc].astype(f32)
            v = qkv_ref[r, 2 * heads * kc + h * vc : 2 * heads * kc + (h + 1) * vc]
            run = jnp.dot(lower_ones, d, precision=lax.Precision.HIGHEST, preferred_element_type=f32)
            closing = run[BLOCK - 1 : BLOCK]
            back = closing - run + d
            mid_f = run[half - 1 : half]
            mid_b = back[half : half + 1]
            qf = (q * jnp.exp(run - mid_f)).astype(bf16)
            kf = (k * jnp.exp(mid_f - run)).astype(bf16)
            qb = (q * jnp.exp(back - mid_b)).astype(bf16)
            kb = (k * jnp.exp(mid_b - back)).astype(bf16)
            nt = (((1,), (1,)), ((), ()))
            sf = lax.dot_general(qf, kf, nt, preferred_element_type=f32)
            sb = lax.dot_general(qb, kb, nt, preferred_element_type=f32)
            scores.append(
                (jnp.where(lower, sf, 0.0) + jnp.where(upper, sb, 0.0)).astype(bf16)
            )
            queries_fb.append(
                jnp.concatenate([q * jnp.exp(run), q * jnp.exp(back)], axis=1).astype(bf16)
            )
            keys_fb = jnp.concatenate(
                [k * jnp.exp(closing - run), k * jnp.exp(closing - back)], axis=1
            ).astype(bf16)
            updates.append(
                lax.dot_general(v, keys_fb, (((0,), (0,)), ((), ())), preferred_element_type=f32)
            )
            closings.append(jnp.exp(closing))
        state = jnp.zeros((vc, kc), f32)
        ahead = []
        for b in range(count):
            ahead.append(state.astype(bf16))
            state = state * closings[b] + updates[b][:, :kc]
        state = jnp.zeros((vc, kc), f32)
        behind = [None] * count
        for b in reversed(range(count)):
            behind[b] = state.astype(bf16)
            state = state * closings[b] + updates[b][:, kc:]
        for b in range(count):
            r = slice(b * BLOCK, (b + 1) * BLOCK)
            v = qkv_ref[r, 2 * heads * kc + h * vc : 2 * heads * kc + (h + 1) * vc]
            states = jnp.concatenate([ahead[b], behind[b]], axis=1)
            mixed = lax.dot_general(
                queries_fb[b], states, (((1,), (1,)), ((), ())), preferred_element_type=f32
            ) + jnp.dot(scores[b], v, preferred_element_type=f32)
            scale = lax.rsqrt(jnp.mean(mixed * mixed, axis=-1, keepdims=True) + 1e-06)
            out_ref[r, h * vc : (h + 1) * vc] = (mixed * scale * gain_ref[...]).astype(bf16)


def attention(qkv, lowrank, second_factor, bias, extra, gain):
    rows = qkv.shape[0]
    heads = extra.shape[1]
    width = heads * gain.shape[0]
    kc = second_factor.shape[1] // heads
    return pl.pallas_call(
        functools.partial(attention_kernel, heads),
        out_shape=jax.ShapeDtypeStruct((rows, width), jnp.bfloat16),
        in_specs=[pl.BlockSpec(memory_space=pltpu.VMEM)] * 6,
        out_specs=pl.BlockSpec(memory_space=pltpu.VMEM),
        compiler_params=pltpu.CompilerParams(vmem_limit_bytes=32 * 1024 * 1024),
        cost_estimate=pl.CostEstimate(
            flops=40 * rows * kc * width, bytes_accessed=4 * rows * width * 2, transcendentals=0
        ),
    )(qkv, lowrank, second_factor, bias[None, :], extra, gain[None, :])


def gather_shared(piece, chunks=1):
    copies = lax.axis_size("grp")
    if copies != 2 or piece.shape[1] % (copies * chunks):
        return [(lax.all_gather(piece, "fs", axis=0, tiled=True), None)]
    wide = piece.shape[1] // chunks
    part = wide // copies
    pairs = []
    for chunk in range(chunks):
        start = chunk * wide + lax.axis_index("grp") * part
        own = lax.all_gather(
            lax.dynamic_slice_in_dim(piece, start, part, 1), "fs", axis=0, tiled=True
        )
        pairs.append((own, lax.ppermute(own, "grp", [(0, 1), (1, 0)])))
    return pairs


def in_order(pairs):
    if pairs[0][1] is None:
        return pairs[0][0]
    first = lax.axis_index("grp") == 0
    blocks = []
    for own, other in pairs:
        blocks += [jnp.where(first, own, other), jnp.where(first, other, own)]
    return jnp.concatenate(blocks, axis=1)


def times(left, right):
    if right is None:
        return None
    return jnp.dot(left, right, preferred_element_type=jnp.float32)


def shared_dot(left, pairs):
    def rounded(right):
        return None if right is None else times(left, right).astype(jnp.bfloat16)

    return in_order([(rounded(own), rounded(other)) for own, other in pairs])


def gated(second, gate_weight, up_weight):
    if gate_weight is None:
        return None
    gate, up = times(second, gate_weight), times(second, up_weight)
    return (jax.nn.silu(gate) * up).astype(jnp.bfloat16)


def step_back(values, hops):
    count = lax.axis_size("tp")
    return lax.ppermute(values, "tp", [(i, (i - hops) % count) for i in range(count)])


def step_on(values, hops):
    count = lax.axis_size("tp")
    return lax.ppermute(values, "tp", [(i, (i + hops) % count) for i in range(count)])


def scatter_sum(partial, share):
    count = lax.axis_size("tp")
    total = partial[:share].astype(jnp.float32)
    arrived = [step_back(partial[j * share : (j + 1) * share], j) for j in range(1, count)]
    for block in arrived:
        total = total + block.astype(jnp.float32)
    return total


def fused_kernel(
    shape,
    gain1_ref,
    first_ref,
    second_ref,
    bias_ref,
    extra_ref,
    hgain_ref,
    gain2_ref,
    x_hbm,
    q_hbm,
    k_hbm,
    v_hbm,
    o_hbm,
    g_hbm,
    u_hbm,
    d_hbm,
    out_hbm,
    x_ref,
    qkv_w,
    out_w,
    gate_w,
    up_w,
    down_w,
    normed,
    lowrank,
    extra,
    qkv,
    headed,
    part1,
    core1,
    send1,
    line1,
    resid,
    second,
    hidden,
    part2,
    core2,
    send2,
    line2,
    send3,
    line3,
    result,
    s_right,
    s_left,
    s_grp,
    r_line,
    r_grp,
    local,
    s_down,
    r_down,
    sy_down,
    ry_down,
    l_down,
    s_sum,
    r_sum,
    s_share,
    r_share,
    s_fin,
    r_fin,
    store,
    load,
):
    n, count, heads, chunks, small, parts = shape
    f32, bf16 = jnp.float32, jnp.bfloat16
    z, y, me = lax.axis_index("fs"), lax.axis_index("grp"), lax.axis_index("tp")
    rows, width = x_ref.shape
    share = rows // count
    wide = width // chunks
    kcols, vcols = q_hbm.shape[1], v_hbm.shape[1]
    units = g_hbm.shape[1]
    big = units - small
    xi, ci = me // 2, lax.rem(me, 2)
    core_peer = 2 * xi + 1 - ci
    line_peer = 2 * (1 - xi) + ci
    side = z // 2
    mate = z + 1 - 2 * lax.rem(z, 2)
    partner = lax.rem(z + 2, n)
    inner = lax.rem(z + side, 2) == 1
    outer = jnp.logical_not(inner)
    cross = 2 - side
    far = 3 * (1 - side)

    strip = 256
    items = []

    def add(source, target, start, total, place, step):
        first = len(items)
        for at in range(0, total, step):
            size = min(step, total - at)
            items.append((source, target, start + at, size, place + at))
        return list(range(first, len(items)))

    QKV = add(q_hbm, qkv_w, 0, kcols, 0, strip)
    QKV += add(k_hbm, qkv_w, 0, kcols, kcols, strip)
    QKV += add(v_hbm, qkv_w, 0, vcols, 2 * kcols, strip)
    OUT = add(o_hbm, out_w, 0, width, 0, wide)
    NARROW, EXTRA = [], []
    for at in range(0, big, strip):
        most = small if at < small else big
        size = min(strip, most - at)
        pair = add(g_hbm, gate_w, at, size, at, strip) + add(u_hbm, up_w, at, size, at, strip)
        (NARROW if at < small else EXTRA).append(pair)

    def remote(source, target, send, recv, where):
        return pltpu.make_async_remote_copy(
            src_ref=source,
            dst_ref=target,
            send_sem=send,
            recv_sem=recv,
            device_id=where,
            device_id_type=pl.DeviceIdType.MESH,
        )

    def high_of(i):
        return items[i][0].shape[0] // 2

    def rows_of(i, origin, half):
        high = high_of(i)
        return pl.ds(pl.multiple_of((2 * origin + half) * high, high), high)

    def all_rows(i, origin):
        high = items[i][0].shape[0]
        return pl.ds(pl.multiple_of(origin * high, high), high)

    def lanes(start, size):
        return pl.ds(pl.multiple_of(start, 128), size)

    def piece(i, origin, half):
        _, target, _, size, place = items[i]
        return target.at[rows_of(i, origin, half), pl.ds(place, size)]

    def own_rows(i, half):
        source, _, start, size, _ = items[i]
        high = high_of(i)
        return source.at[pl.ds(pl.multiple_of(half * high, high), high), pl.ds(start, size)]

    def spare(i, sent):
        return remote(sent, piece(i, z, 1 - y), s_grp.at[i, z], r_grp.at[i, z], {"fs": mate})

    def to_right(i, origin, source):
        return remote(
            source, piece(i, origin, y), s_right.at[i, origin], r_line.at[i, origin], {"fs": z + 1}
        )

    def to_left(i, origin, source):
        return remote(
            source, piece(i, origin, y), s_left.at[i, origin], r_line.at[i, origin], {"fs": z - 1}
        )

    def to_grp(i, origin, block):
        return remote(block, block, s_grp.at[i, origin], r_grp.at[i, origin], {"grp": 1 - y})

    def local_copy(i):
        source, target, start, size, place = items[i]
        return pltpu.make_async_copy(
            source.at[:, pl.ds(start, size)],
            target.at[all_rows(i, z), pl.ds(place, size)],
            local.at[i],
        )

    def start_own(group):
        for i in group:
            own = own_rows(i, y)
            pl.when(z + 1 < n)(lambda i=i, own=own: to_right(i, z, own).start())
            pl.when(z >= 1)(lambda i=i, own=own: to_left(i, z, own).start())
            local_copy(i).start()
        for i in group:
            pl.when(outer)(lambda i=i: spare(i, own_rows(i, 1 - y)).start())

    def sides(d):
        return (
            (z >= d, z - d, z + 1 < n, to_right, z >= 2),
            (z + d < n, z + d, z >= 1, to_left, z < n - 2),
        )

    def pass_on(group, distances):
        for d in distances:
            for i in group:
                for there, origin, more, send, shared in sides(d):

                    @pl.when(there)
                    def _():
                        block = piece(i, origin, y)
                        send(i, origin, block).wait_recv()
                        pl.when(more)(lambda: send(i, origin, block).start())
                        if d == 1:
                            pl.when(shared)(lambda: to_grp(i, origin, block).start())
                        else:
                            to_grp(i, origin, block).start()

    def complete(group):
        for i in group:
            local_copy(i).wait()
            for d in range(1, n):
                for cond, origin in ((z >= d, z - d), (z + d < n, z + d)):
                    pl.when(cond)(
                        lambda i=i, o=origin: to_grp(i, o, piece(i, o, 1 - y)).wait_recv()
                    )

    def drain(group):
        for i in group:
            own = own_rows(i, y)
            pl.when(z + 1 < n)(lambda: to_right(i, z, own).wait_send())
            pl.when(z >= 1)(lambda: to_left(i, z, own).wait_send())
            pl.when(outer)(lambda: spare(i, own_rows(i, 1 - y)).wait_send())
            for d in range(1, n):
                for there, origin, more, send, shared in sides(d):

                    @pl.when(there)
                    def _():
                        block = piece(i, origin, y)
                        pl.when(more)(lambda: send(i, origin, block).wait_send())
                        if d == 1:
                            pl.when(shared)(lambda: to_grp(i, origin, block).wait_send())
                        else:
                            to_grp(i, origin, block).wait_send()

    origins = (mate, cross, far)
    EXTRAS = [i for pair in EXTRA for i in pair]

    def cut_rows(i, half, to):
        source, _, start, size, _ = items[i]
        high = high_of(i)
        offset = start if i in EXTRAS else to * big + start
        return source.at[pl.ds(pl.multiple_of(half * high, high), high), lanes(offset, size)]

    def to_mate(i, origin, sent):
        return remote(
            sent, piece(i, origin, y), s_right.at[i, origin], r_line.at[i, origin], {"fs": mate}
        )

    def to_cross(i):
        return remote(
            cut_rows(i, y, 1 - side),
            piece(i, z, y),
            s_left.at[i, z],
            r_line.at[i, z],
            {"fs": cross},
        )

    def keep(i):
        source, target, start, size, place = items[i]
        offset = start if i in EXTRAS else side * big + start
        return pltpu.make_async_copy(
            source.at[:, lanes(offset, size)],
            target.at[all_rows(i, z), pl.ds(place, size)],
            local.at[i],
        )

    def start_cut(pair):
        for i in pair:
            if i in EXTRAS:
                pl.when(outer)(lambda i=i: to_mate(i, z, cut_rows(i, y, side)).start())
                pl.when(inner)(lambda i=i: keep(i).start())
            else:
                to_mate(i, z, cut_rows(i, y, side)).start()
                keep(i).start()
            to_cross(i).start()
        for i in pair:
            if i in EXTRAS:
                pl.when(outer)(lambda i=i: spare(i, cut_rows(i, 1 - y, side)).start())

    def pass_cut(pair, k):
        def step(i):
            origin = origins[k]
            block = piece(i, origin, y)
            to_mate(i, origin, block).wait_recv()
            if i in EXTRAS:
                if k:
                    to_grp(i, origin, block).start()
                return
            if k:
                pl.when(inner)(lambda: to_mate(i, origin, block).start())
            to_grp(i, origin, block).start()

        for i in pair:
            if i in EXTRAS:
                pl.when(inner)(lambda i=i: step(i))
            else:
                step(i)

    def complete_cut(pair):
        def step(i):
            keep(i).wait()
            for origin in origins:
                to_grp(i, origin, piece(i, origin, 1 - y)).wait_recv()

        for i in pair:
            if i in EXTRAS:
                pl.when(inner)(lambda i=i: step(i))
            else:
                step(i)

    def drain_cut(pair):
        for i in pair:
            to_cross(i).wait_send()
            if i in EXTRAS:

                @pl.when(outer)
                def _():
                    to_mate(i, z, cut_rows(i, y, side)).wait_send()
                    spare(i, cut_rows(i, 1 - y, side)).wait_send()

                @pl.when(inner)
                def _():
                    for k in (1, 2):
                        to_grp(i, origins[k], piece(i, origins[k], y)).wait_send()

            else:
                to_mate(i, z, cut_rows(i, y, side)).wait_send()
                for k in range(3):
                    block = piece(i, origins[k], y)
                    if k:
                        pl.when(inner)(
                            lambda k=k, b=block: to_mate(i, origins[k], b).wait_send()
                        )
                    to_grp(i, origins[k], block).wait_send()

    depth = d_hbm.shape[0]
    sub, rest = small - depth, big - 2 * depth

    def down_block(c, start, size):
        return down_w.at[pl.ds(pl.multiple_of(start, 16), size), pl.ds(c * wide, wide)]

    def down_src(c, start, size):
        return d_hbm.at[pl.ds(pl.multiple_of(start, 16), size), pl.ds(c * wide, wide)]

    def end_place(c, start, size):
        return down_block(c, side * sub + start, size)

    def near_place(c, start, size):
        return down_block(c, (1 - side) * depth + start, size)

    def near_src(c, start, size):
        return down_src(c, side * rest + start, size)

    def middle_place(c, whose, start, size):
        return down_block(c, small + whose * rest + start, size)

    def middle_src(c, start, size):
        return down_src(c, (1 - side) * sub + start, size)

    def halved(c, size, half, place):
        return place(c, half * (size // 2), size // 2)

    def from_mate(c, half, to_inner):
        if to_inner:
            return halved(c, depth, half, end_place)
        return halved(c, sub, half, near_place)

    def middle(c, whose, half):
        return middle_place(c, whose, half * (rest // 2), rest // 2)

    def down_to_mate(c, to_inner):
        sent = halved(c, depth, y, down_src) if to_inner else halved(c, sub, y, near_src)
        return remote(
            sent, from_mate(c, y, to_inner), s_down.at[c, 0], r_down.at[c, 0], {"fs": mate}
        )

    def down_to_cross(c):
        return remote(
            halved(c, rest, y, middle_src),
            middle(c, side, y),
            s_down.at[c, 1],
            r_down.at[c, 1],
            {"fs": cross},
        )

    def down_local(c, k):
        if k == 0:
            return pltpu.make_async_copy(
                down_src(c, 0, depth), end_place(c, 0, depth), l_down.at[c, 0]
            )
        if k == 1:
            return pltpu.make_async_copy(
                near_src(c, 0, sub), near_place(c, 0, sub), l_down.at[c, 0]
            )
        return pltpu.make_async_copy(
            middle_src(c, 0, rest), middle_place(c, side, 0, rest), l_down.at[c, 1]
        )

    def down_grp(c, k, block):
        return remote(block, block, sy_down.at[c, k], ry_down.at[c, k], {"grp": 1 - y})

    def start_down(c):
        @pl.when(outer)
        def _():
            down_to_mate(c, True).start()
            down_local(c, 0).start()

        @pl.when(inner)
        def _():
            down_to_mate(c, False).start()
            down_to_cross(c).start()
            down_local(c, 1).start()
            down_local(c, 2).start()

    def down_arrival(c, k, block):
        return remote(block, block, s_down.at[c, k], r_down.at[c, k], {"fs": mate})

    def pass_down(c):
        @pl.when(outer)
        def _():
            block = from_mate(c, y, False)
            down_arrival(c, 0, block).wait_recv()
            down_grp(c, 0, block).start()

        @pl.when(inner)
        def _():
            for k, block in ((0, from_mate(c, y, True)), (1, middle(c, 1 - side, y))):
                down_arrival(c, k, block).wait_recv()
                down_grp(c, k, block).start()

    def complete_down(c):
        @pl.when(outer)
        def _():
            down_local(c, 0).wait()
            down_grp(c, 0, from_mate(c, 1 - y, False)).wait_recv()

        @pl.when(inner)
        def _():
            down_local(c, 1).wait()
            down_local(c, 2).wait()
            down_grp(c, 0, from_mate(c, 1 - y, True)).wait_recv()
            down_grp(c, 1, middle(c, 1 - side, 1 - y)).wait_recv()

    def drain_down(c):
        @pl.when(outer)
        def _():
            down_to_mate(c, True).wait_send()
            down_grp(c, 0, from_mate(c, y, False)).wait_send()

        @pl.when(inner)
        def _():
            down_to_mate(c, False).wait_send()
            down_to_cross(c).wait_send()
            down_grp(c, 0, from_mate(c, y, True)).wait_send()
            down_grp(c, 1, middle(c, 1 - side, y)).wait_send()

    def sum_core1(c):
        return remote(
            part1.at[c, :, 1 - ci], core1.at[c], s_sum.at[c, 0], r_sum.at[c, 0], {"tp": core_peer}
        )

    def sum_line1(c):
        return remote(
            send1.at[c], line1.at[c], s_sum.at[c, 1], r_sum.at[c, 1], {"tp": line_peer}
        )

    def sum_core2(c):
        return remote(
            part2.at[c, :, :, 1 - ci],
            core2.at[c],
            s_sum.at[c, 2],
            r_sum.at[c, 2],
            {"tp": core_peer},
        )

    def sum_line2(c):
        return remote(
            send2.at[c], line2.at[c], s_sum.at[c, 3], r_sum.at[c, 3], {"tp": line_peer}
        )

    def sum_line3(c):
        return remote(
            send3.at[c], line3.at[c], s_sum.at[c, 4], r_sum.at[c, 4], {"fs": partner}
        )

    lump = share // parts

    def rows_at(which, t, p):
        start = pl.multiple_of(which * rows + t * share + p * lump, lump)
        return second.at[pl.ds(start, lump)]

    def give(p, slot, which, t, where, target=None):
        block = rows_at(which, t, p)
        return remote(
            block,
            block if target is None else target,
            s_share.at[slot, p],
            r_share.at[slot, p],
            where,
        )

    def to_partner(p):
        return give(p, 0, 0, me, {"fs": partner}, rows_at(1, me, p))

    def across(p, which):
        return give(p, 1 + which, which, me, {"tp": line_peer})

    def across_arrival(p, which):
        return give(p, 1 + which, which, line_peer, {"tp": line_peer})

    def over(p, which, mine):
        return give(p, 3 + 2 * which + (1 - mine), which, me if mine else line_peer, {"tp": core_peer})

    def over_arrival(p, which, mine):
        t = core_peer if mine else 2 * (1 - xi) + 1 - ci
        return give(p, 3 + 2 * which + (1 - mine), which, t, {"tp": core_peer})

    def fin(c, slot, t, where):
        block = result.at[c, t]
        return remote(block, block, s_fin.at[c, slot], r_fin.at[c, slot], where)

    def put(c, t):
        r = pl.ds(pl.multiple_of(t * share, share), share)
        return pltpu.make_async_copy(
            result.at[c, t], out_hbm.at[r, pl.ds(c * wide, wide)], store.at[c, t]
        )

    barrier = pltpu.get_barrier_semaphore()

    def greet(where):
        pl.semaphore_signal(
            barrier, inc=1, device_id=where, device_id_type=pl.DeviceIdType.MESH
        )

    get_x = pltpu.make_async_copy(x_hbm, x_ref, load)
    get_x.start()
    for where in ({"grp": 1 - y}, {"tp": core_peer}, {"tp": line_peer}, {"fs": partner}):
        greet(where)
    pl.when(z + 1 < n)(lambda: greet({"fs": z + 1}))
    pl.when(z >= 1)(lambda: greet({"fs": z - 1}))
    pl.semaphore_wait(barrier, 4 + jnp.minimum(z, 1) + jnp.minimum(n - 1 - z, 1))

    start_own(QKV)

    @pl.when(outer)
    def _():
        hidden[:, small:] = jnp.zeros((2 * rows, big - small), bf16)
        down_w[small:] = jnp.zeros((big - small, width), bf16)

    get_x.wait()
    tall = min(64, share)

    def norm_step(s, carry):
        r = pl.ds(pl.multiple_of(s * tall, tall), tall)
        normed[r] = norm_rows(x_ref[r], gain1_ref[...]).astype(bf16)
        return carry

    lax.fori_loop(0, rows // tall, norm_step, 0)
    lowrank[...] = lax.dot_general(
        normed[...], first_ref[...], (((1,), (1,)), ((), ())), preferred_element_type=f32
    ).astype(bf16)
    extra[...] = extra_ref[...].T

    def tiles(total, body, tile=256):
        def step(s, carry):
            body(pl.multiple_of(s * tile, tile), tile)
            return carry

        lax.fori_loop(0, total // tile, step, 0)
        if total % tile:
            body(total - total % tile, total % tile)

    pass_on(QKV, (1, 2))
    start_own(OUT)
    pass_on(QKV, (3,))
    start_cut(NARROW[0])
    complete(QKV)

    def project(at, size):
        qkv[:, pl.ds(at, size)] = jnp.dot(
            normed[...], qkv_w[:, pl.ds(at, size)], preferred_element_type=f32
        ).astype(bf16)

    tiles(qkv_w.shape[1], project)
    pass_on(OUT, (1, 2))
    attention_kernel(heads, qkv, lowrank, second_ref, bias_ref, extra, hgain_ref, headed)
    pass_on(OUT, (3,))
    for pair in NARROW[1:]:
        start_cut(pair)
    complete(OUT)

    for c in range(chunks):
        mixed = jnp.dot(
            headed[...], out_w[:, c * wide : (c + 1) * wide], preferred_element_type=f32
        ).astype(bf16)
        part1[c] = mixed.reshape(2, 2, share, wide)
        sum_core1(c).start()
    pass_cut(NARROW[0], 0)
    for c in range(chunks):
        sum_core1(c).wait_recv()
        send1[c] = (part1[c, 1 - xi, ci].astype(f32) + core1[c, 1 - xi].astype(f32)).astype(bf16)
        sum_line1(c).start()
    for pair in EXTRA:
        start_cut(pair)
    pass_cut(NARROW[0], 1)
    own = pl.ds(pl.multiple_of(me * share, share), share)
    for c in range(chunks):
        sum_line1(c).wait_recv()
        cols = slice(c * wide, (c + 1) * wide)
        total = part1[c, xi, ci].astype(f32) + core1[c, xi].astype(f32) + line1[c].astype(f32)
        resid[:, cols] = (x_ref[own, cols].astype(f32) + total).astype(bf16)
    for p in range(parts):
        value = resid[p * lump : (p + 1) * lump]
        start = pl.multiple_of(me * share + p * lump, lump)
        second[pl.ds(start, lump)] = norm_rows(value, gain2_ref[...]).astype(bf16)
        to_partner(p).start()
        across(p, 0).start()
        over(p, 0, 1).start()

    def gate_up(which, pairs):
        r = slice(which * rows, (which + 1) * rows)

        def run(start, size):
            def step(s, carry):
                cols = pl.ds(pl.multiple_of(start + s * 128, 128), 128)
                both = jnp.dot(
                    second[r],
                    jnp.concatenate([gate_w[:, cols], up_w[:, cols]], axis=1),
                    preferred_element_type=f32,
                )
                hidden[r, cols] = (jax.nn.silu(both[:, :128]) * both[:, 128:]).astype(bf16)
                return carry

            lax.fori_loop(0, size // 128, step, 0)

        first, last = items[pairs[0][0]], items[pairs[-1][0]]
        run(first[4], last[4] + last[3] - first[4])

    pass_cut(NARROW[0], 2)
    for pair in NARROW[1:]:
        pass_cut(pair, 0)
    for p in range(parts):
        across_arrival(p, 0).wait_recv()
        over(p, 0, 0).start()
    for pair in NARROW[1:]:
        pass_cut(pair, 1)
    for p in range(parts):
        give(p, 0, 1, me, {"fs": partner}).wait_recv()
        across(p, 1).start()
        over(p, 1, 1).start()
    for pair in NARROW[1:]:
        pass_cut(pair, 2)
    for c in range(chunks):
        start_down(c)
    for p in range(parts):
        over_arrival(p, 0, 1).wait_recv()
        over_arrival(p, 0, 0).wait_recv()
    complete_cut(NARROW[0])
    gate_up(0, NARROW[:1])
    for pair in EXTRA:
        pass_cut(pair, 0)
        pass_cut(pair, 1)
    for p in range(parts):
        across_arrival(p, 1).wait_recv()
        over(p, 1, 0).start()
    for pair in NARROW[1:]:
        complete_cut(pair)
    gate_up(0, NARROW[1:])
    for p in range(parts):
        over_arrival(p, 1, 1).wait_recv()
        over_arrival(p, 1, 0).wait_recv()
    gate_up(1, NARROW)
    for pair in EXTRA:
        pass_cut(pair, 2)
    for pair in EXTRA:
        complete_cut(pair)

        @pl.when(inner)
        def _():
            for which in range(2):
                gate_up(which, [pair])

    def sum_a(c):
        pass_down(c)
        complete_down(c)
        for which in range(2):
            out = jnp.dot(
                hidden[which * rows : (which + 1) * rows],
                down_w[:, c * wide : (c + 1) * wide],
                preferred_element_type=f32,
            ).astype(bf16)
            part2[c, which] = out.reshape(2, 2, share, wide)
        sum_core2(c).start()

    def sum_b(c):
        sum_core2(c).wait_recv()
        for which in range(2):
            send2[c, which] = (
                part2[c, which, 1 - xi, ci].astype(f32) + core2[c, which, 1 - xi].astype(f32)
            ).astype(bf16)
        sum_line2(c).start()

    def held(c, which):
        return (
            part2[c, which, xi, ci].astype(f32)
            + core2[c, which, xi].astype(f32)
            + line2[c, which].astype(f32)
        )

    def sum_c(c):
        sum_line2(c).wait_recv()
        send3[c] = held(c, 1).astype(bf16)
        sum_line3(c).start()

    def sum_d(c):
        sum_line3(c).wait_recv()
        total = held(c, 0) + line3[c].astype(f32)
        value = resid[:, c * wide : (c + 1) * wide].astype(f32) + total
        result[c, me] = value.astype(bf16)
        fin(c, 0, me, {"tp": line_peer}).start()
        fin(c, 1, me, {"tp": core_peer}).start()
        put(c, me).start()

    def sum_e(c):
        fin(c, 0, line_peer, {"tp": line_peer}).wait_recv()
        fin(c, 2, line_peer, {"tp": core_peer}).start()
        put(c, line_peer).start()

    corner = 2 * (1 - xi) + 1 - ci

    def sum_f(c):
        fin(c, 1, core_peer, {"tp": core_peer}).wait_recv()
        put(c, core_peer).start()
        fin(c, 2, corner, {"tp": core_peer}).wait_recv()
        put(c, corner).start()

    stages = (sum_a, sum_b, sum_c, sum_d, sum_e, sum_f)
    for step in range(chunks + len(stages) - 1):
        for k, stage in enumerate(stages):
            if 0 <= step - k < chunks:
                stage(step - k)

    for c in range(chunks):
        for t in (me, core_peer, line_peer, corner):
            put(c, t).wait()
        fin(c, 0, me, {"tp": line_peer}).wait_send()
        fin(c, 1, me, {"tp": core_peer}).wait_send()
        fin(c, 2, line_peer, {"tp": core_peer}).wait_send()
        for copy in (sum_core1, sum_line1, sum_core2, sum_line2, sum_line3):
            copy(c).wait_send()
        drain_down(c)
    for p in range(parts):
        to_partner(p).wait_send()
        for which in range(2):
            across(p, which).wait_send()
            over(p, which, 1).wait_send()
            over(p, which, 0).wait_send()
    drain(QKV)
    drain(OUT)
    for pair in NARROW + EXTRA:
        drain_cut(pair)


def narrow_units(units):
    return units // 128 * 3 // 8 * 128


def fits(x, q, k, v, o, g, u, d):
    copies, n, count = (lax.axis_size(a) for a in ("grp", "fs", "tp"))
    rows, width = x.shape
    if (copies, n, count) != (2, 4, 4) or rows % (64 * count) or width % 512:
        return False
    for p in (q, k, v, o, g, u, d):
        if p.shape[0] % 32 or p.shape[1] % 128:
            return False
    units, depth = g.shape[1], d.shape[0]
    small = narrow_units(units)
    sub, rest = small - depth, units - small - 2 * depth
    if min(sub, rest) <= 0 or sub % 32 or rest % 32:
        return False
    if small % 256:
        return False
    held = n * (q.size + k.size + v.size + o.size) + 3 * (units - small) * n * g.shape[0]
    return 2 * held + 24 * x.size <= 54 * 2**20


def fused(x, gain1, q, k, v, first, second, bias, extra, hgain, o, gain2, g, u, d):
    n, count = lax.axis_size("fs"), lax.axis_size("tp")
    rows, width = x.shape
    share = rows // count
    heads = extra.shape[1]
    chunks, parts = 4, 2
    wide = width // chunks
    bf16, f32 = jnp.bfloat16, jnp.float32
    vmem, hbm = pl.BlockSpec(memory_space=pltpu.VMEM), pl.BlockSpec(memory_space=pl.ANY)
    qkv_cols = 2 * q.shape[1] + v.shape[1]
    held = heads * hgain.shape[0]
    units = g.shape[1]
    small = narrow_units(units)
    big = units - small
    buffers = [
        ((rows, width), bf16),
        ((n * q.shape[0], qkv_cols), bf16),
        ((n * o.shape[0], width), bf16),
        ((n * g.shape[0], big), bf16),
        ((n * u.shape[0], big), bf16),
        ((big, width), bf16),
        ((rows, width), bf16),
        ((rows, first.shape[1]), bf16),
        ((rows, heads), f32),
        ((rows, qkv_cols), bf16),
        ((rows, held), bf16),
        ((chunks, 2, 2, share, wide), bf16),
        ((chunks, 2, share, wide), bf16),
        ((chunks, share, wide), bf16),
        ((chunks, share, wide), bf16),
        ((share, width), bf16),
        ((2 * rows, width), bf16),
        ((2 * rows, big), bf16),
        ((chunks, 2, 2, 2, share, wide), bf16),
        ((chunks, 2, 2, share, wide), bf16),
        ((chunks, 2, share, wide), bf16),
        ((chunks, 2, share, wide), bf16),
        ((chunks, share, wide), bf16),
        ((chunks, share, wide), bf16),
        ((chunks, count, share, wide), bf16),
    ]
    lots = sum(-(-size // 256) for size in (q.shape[1], k.shape[1], v.shape[1])) + chunks
    lots += 2 * (small // 256 + -(-(big - small) // 256))
    counts = [(lots, n)] * 5 + [(lots,)] + [(chunks, 2)] * 5
    counts += [(chunks, 5)] * 2 + [(7, parts)] * 2 + [(chunks, 3)] * 2 + [(chunks, count)]
    return pl.pallas_call(
        functools.partial(fused_kernel, (n, count, heads, chunks, small, parts)),
        out_shape=jax.ShapeDtypeStruct((rows, width), bf16),
        in_specs=[vmem] * 7 + [hbm] * 8,
        out_specs=hbm,
        scratch_shapes=[pltpu.VMEM(s, t) for s, t in buffers]
        + [pltpu.SemaphoreType.DMA(s) for s in counts]
        + [pltpu.SemaphoreType.DMA],
        compiler_params=pltpu.CompilerParams(
            vmem_limit_bytes=62 * 1024 * 1024, collective_id=0, has_side_effects=True
        ),
    )(
        gain1[None, :],
        first.T,
        second,
        bias[None, :],
        extra.T,
        hgain[None, :],
        gain2[None, :],
        *(x, q, k, v, o, g, u, d),
    )


def shards(*arrays):
    if fits(*[arrays[i] for i in (0, 2, 3, 4, 10, 12, 13, 14)]):
        return fused(*arrays)
    return spread(*arrays)


def spread(
    layer_input_tokens,
    attention_norm_gain,
    query_projection,
    key_projection,
    value_projection,
    decay_first_factor,
    decay_second_factor,
    decay_logit_bias,
    extra_log_decay,
    head_output_gain,
    attention_output_projection,
    feedforward_norm_gain,
    gate_projection,
    up_projection,
    down_projection,
):
    rows = layer_input_tokens.shape[0]
    count = lax.axis_size("tp")
    me = lax.axis_index("tp")
    share = rows // count
    qkv_full = gather_shared(
        jnp.concatenate([query_projection, key_projection, value_projection], axis=1)
    )
    out_full = gather_shared(attention_output_projection)
    gate_full = gather_shared(gate_projection)
    up_full = gather_shared(up_projection)
    down_full = gather_shared(down_projection, 2)

    normed = norm_rows(layer_input_tokens, attention_norm_gain).astype(jnp.bfloat16)
    lowrank = jnp.dot(normed, decay_first_factor, preferred_element_type=jnp.float32).astype(
        jnp.bfloat16
    )
    qkv = shared_dot(normed, qkv_full)
    headed = attention(
        qkv, lowrank, decay_second_factor, decay_logit_bias, extra_log_decay, head_output_gain
    )
    turned = jnp.concatenate(
        [
            lax.dynamic_slice_in_dim(headed, lax.rem(me - j + count, count) * share, share, 0)
            for j in range(count)
        ],
        axis=0,
    )
    mixer = scatter_sum(shared_dot(turned, out_full), share)
    own = lax.dynamic_slice_in_dim(layer_input_tokens, me * share, share, 0)
    residual = (own.astype(jnp.float32) + mixer).astype(jnp.bfloat16)
    mine = norm_rows(residual, feedforward_norm_gain).astype(jnp.bfloat16)
    second = jnp.concatenate([mine] + [step_on(mine, j) for j in range(1, count)], axis=0)
    hidden = in_order(
        [
            (gated(second, g_own, u_own), gated(second, g_other, u_other))
            for (g_own, g_other), (u_own, u_other) in zip(gate_full, up_full)
        ]
    )
    channel = scatter_sum(shared_dot(hidden, down_full), share)
    finished = (residual.astype(jnp.float32) + channel).astype(jnp.bfloat16)
    return lax.all_gather(finished, "tp", axis=0, tiled=True)


def solution(mesh):
    placed = (
        P(("grp", "fs"), None),
        P(),
        P("fs", "tp"),
        P("fs", "tp"),
        P("fs", "tp"),
        P(),
        P(None, "tp"),
        P("tp"),
        P(("grp", "fs"), "tp"),
        P(),
        P(("tp", "fs"), None),
        P(),
        P("fs", "tp"),
        P("fs", "tp"),
        P(("tp", "fs"), None),
    )
    return jax.shard_map(
        shards, mesh=mesh, in_specs=placed, out_specs=P(("grp", "fs"), None), check_vma=False
    )
```

```python
import functools

import jax
import jax.numpy as jnp
from jax import lax
from jax.experimental import pallas as pl
from jax.experimental.pallas import tpu as pltpu
from jax.sharding import PartitionSpec as P

BLOCK = 64
DECAY_GATE = 16.0


def norm_rows(values, gain):
    wide = values.astype(jnp.float32)
    scale = lax.rsqrt(jnp.mean(wide * wide, axis=-1, keepdims=True) + 1e-06)
    return wide * scale * gain


def attention_kernel(heads, qkv_ref, lowrank_ref, second_ref, bias_ref, extra_ref, gain_ref, out_ref, which=None):
    rows = qkv_ref.shape[0]
    kc = second_ref.shape[1] // heads
    vc = out_ref.shape[1] // heads
    count = rows // BLOCK
    f32, bf16 = jnp.float32, jnp.bfloat16
    row_id = lax.broadcasted_iota(jnp.int32, (BLOCK, BLOCK), 0)
    col_id = lax.broadcasted_iota(jnp.int32, (BLOCK, BLOCK), 1)
    lower = row_id >= col_id
    upper = row_id <= col_id
    lower_ones = jnp.where(lower, 1.0, 0.0).astype(f32)
    half = BLOCK // 2
    for h in which or range(heads):
        kcols = slice(h * kc, (h + 1) * kc)
        logits = (
            jnp.dot(lowrank_ref[...], second_ref[:, kcols], preferred_element_type=f32)
            + bias_ref[:, kcols]
        )
        log_sig = jnp.minimum(logits, 0.0) - jnp.log1p(jnp.exp(-jnp.abs(logits)))
        decay = log_sig / DECAY_GATE + extra_ref[:, h : h + 1]
        queries_fb, updates, closings, scores = [], [], [], []
        for b in range(count):
            r = slice(b * BLOCK, (b + 1) * BLOCK)
            d = decay[r]
            q = qkv_ref[r, h * kc : (h + 1) * kc].astype(f32)
            k = qkv_ref[r, (heads + h) * kc : (heads + h + 1) * kc].astype(f32)
            v = qkv_ref[r, 2 * heads * kc + h * vc : 2 * heads * kc + (h + 1) * vc]
            run = jnp.dot(lower_ones, d, precision=lax.Precision.HIGHEST, preferred_element_type=f32)
            closing = run[BLOCK - 1 : BLOCK]
            back = closing - run + d
            mid_f = run[half - 1 : half]
            mid_b = back[half : half + 1]
            qf = (q * jnp.exp(run - mid_f)).astype(bf16)
            kf = (k * jnp.exp(mid_f - run)).astype(bf16)
            qb = (q * jnp.exp(back - mid_b)).astype(bf16)
            kb = (k * jnp.exp(mid_b - back)).astype(bf16)
            nt = (((1,), (1,)), ((), ()))
            sf = lax.dot_general(qf, kf, nt, preferred_element_type=f32)
            sb = lax.dot_general(qb, kb, nt, preferred_element_type=f32)
            scores.append(
                (jnp.where(lower, sf, 0.0) + jnp.where(upper, sb, 0.0)).astype(bf16)
            )
            queries_fb.append(
                jnp.concatenate([q * jnp.exp(run), q * jnp.exp(back)], axis=1).astype(bf16)
            )
            keys_fb = jnp.concatenate(
                [k * jnp.exp(closing - run), k * jnp.exp(closing - back)], axis=1
            ).astype(bf16)
            updates.append(
                lax.dot_general(v, keys_fb, (((0,), (0,)), ((), ())), preferred_element_type=f32)
            )
            closings.append(jnp.exp(closing))
        state = jnp.zeros((vc, kc), f32)
        ahead = []
        for b in range(count):
            ahead.append(state.astype(bf16))
            state = state * closings[b] + updates[b][:, :kc]
        state = jnp.zeros((vc, kc), f32)
        behind = [None] * count
        for b in reversed(range(count)):
            behind[b] = state.astype(bf16)
            state = state * closings[b] + updates[b][:, kc:]
        for b in range(count):
            r = slice(b * BLOCK, (b + 1) * BLOCK)
            v = qkv_ref[r, 2 * heads * kc + h * vc : 2 * heads * kc + (h + 1) * vc]
            states = jnp.concatenate([ahead[b], behind[b]], axis=1)
            mixed = lax.dot_general(
                queries_fb[b], states, (((1,), (1,)), ((), ())), preferred_element_type=f32
            ) + jnp.dot(scores[b], v, preferred_element_type=f32)
            scale = lax.rsqrt(jnp.mean(mixed * mixed, axis=-1, keepdims=True) + 1e-06)
            out_ref[r, h * vc : (h + 1) * vc] = (mixed * scale * gain_ref[...]).astype(bf16)


def attention(qkv, lowrank, second_factor, bias, extra, gain):
    rows = qkv.shape[0]
    heads = extra.shape[1]
    width = heads * gain.shape[0]
    kc = second_factor.shape[1] // heads
    return pl.pallas_call(
        functools.partial(attention_kernel, heads),
        out_shape=jax.ShapeDtypeStruct((rows, width), jnp.bfloat16),
        in_specs=[pl.BlockSpec(memory_space=pltpu.VMEM)] * 6,
        out_specs=pl.BlockSpec(memory_space=pltpu.VMEM),
        compiler_params=pltpu.CompilerParams(vmem_limit_bytes=32 * 1024 * 1024),
        cost_estimate=pl.CostEstimate(
            flops=40 * rows * kc * width, bytes_accessed=4 * rows * width * 2, transcendentals=0
        ),
    )(qkv, lowrank, second_factor, bias[None, :], extra, gain[None, :])


def gather_shared(piece, chunks=1):
    copies = lax.axis_size("grp")
    if copies != 2 or piece.shape[1] % (copies * chunks):
        return [(lax.all_gather(piece, "fs", axis=0, tiled=True), None)]
    wide = piece.shape[1] // chunks
    part = wide // copies
    pairs = []
    for chunk in range(chunks):
        start = chunk * wide + lax.axis_index("grp") * part
        own = lax.all_gather(
            lax.dynamic_slice_in_dim(piece, start, part, 1), "fs", axis=0, tiled=True
        )
        pairs.append((own, lax.ppermute(own, "grp", [(0, 1), (1, 0)])))
    return pairs


def in_order(pairs):
    if pairs[0][1] is None:
        return pairs[0][0]
    first = lax.axis_index("grp") == 0
    blocks = []
    for own, other in pairs:
        blocks += [jnp.where(first, own, other), jnp.where(first, other, own)]
    return jnp.concatenate(blocks, axis=1)


def times(left, right):
    if right is None:
        return None
    return jnp.dot(left, right, preferred_element_type=jnp.float32)


def shared_dot(left, pairs):
    def rounded(right):
        return None if right is None else times(left, right).astype(jnp.bfloat16)

    return in_order([(rounded(own), rounded(other)) for own, other in pairs])


def gated(second, gate_weight, up_weight):
    if gate_weight is None:
        return None
    gate, up = times(second, gate_weight), times(second, up_weight)
    return (jax.nn.silu(gate) * up).astype(jnp.bfloat16)


def step_back(values, hops):
    count = lax.axis_size("tp")
    return lax.ppermute(values, "tp", [(i, (i - hops) % count) for i in range(count)])


def step_on(values, hops):
    count = lax.axis_size("tp")
    return lax.ppermute(values, "tp", [(i, (i + hops) % count) for i in range(count)])


def scatter_sum(partial, share):
    count = lax.axis_size("tp")
    total = partial[:share].astype(jnp.float32)
    arrived = [step_back(partial[j * share : (j + 1) * share], j) for j in range(1, count)]
    for block in arrived:
        total = total + block.astype(jnp.float32)
    return total


def fused_kernel(
    shape,
    gain1_ref,
    first_ref,
    second_ref,
    bias_ref,
    extra_ref,
    hgain_ref,
    gain2_ref,
    x_hbm,
    q_hbm,
    k_hbm,
    v_hbm,
    o_hbm,
    g_hbm,
    u_hbm,
    d_hbm,
    out_hbm,
    x_ref,
    qkv_w,
    out_w,
    gate_w,
    up_w,
    down_w,
    normed,
    lowrank,
    extra,
    qkv,
    headed,
    part1,
    core1,
    send1,
    line1,
    resid,
    second,
    hidden,
    part2,
    core2,
    send2,
    line2,
    send3,
    line3,
    result,
    s_right,
    s_left,
    s_grp,
    r_line,
    r_grp,
    local,
    s_down,
    r_down,
    sy_down,
    ry_down,
    l_down,
    s_sum,
    r_sum,
    s_share,
    r_share,
    s_fin,
    r_fin,
    store,
    load,
):
    n, count, heads, chunks, small, parts = shape
    f32, bf16 = jnp.float32, jnp.bfloat16
    z, y, me = lax.axis_index("fs"), lax.axis_index("grp"), lax.axis_index("tp")
    rows, width = x_ref.shape
    share = rows // count
    wide = width // chunks
    kcols, vcols = q_hbm.shape[1], v_hbm.shape[1]
    units = g_hbm.shape[1]
    big = units - small
    xi, ci = me // 2, lax.rem(me, 2)
    core_peer = 2 * xi + 1 - ci
    line_peer = 2 * (1 - xi) + ci
    side = z // 2
    mate = z + 1 - 2 * lax.rem(z, 2)
    partner = lax.rem(z + 2, n)
    inner = lax.rem(z + side, 2) == 1
    outer = jnp.logical_not(inner)
    cross = 2 - side
    far = 3 * (1 - side)

    strip = 256
    items = []

    def add(source, target, start, total, place, step):
        first = len(items)
        for at in range(0, total, step):
            size = min(step, total - at)
            items.append((source, target, start + at, size, place + at))
        return list(range(first, len(items)))

    QKV = add(q_hbm, qkv_w, 0, kcols, 0, strip)
    QKV += add(k_hbm, qkv_w, 0, kcols, kcols, strip)
    QKV += add(v_hbm, qkv_w, 0, vcols, 2 * kcols, strip)
    OUT = add(o_hbm, out_w, 0, width, 0, wide)
    NARROW, EXTRA = [], []
    for at in range(0, big, strip):
        most = small if at < small else big
        size = min(strip, most - at)
        pair = add(g_hbm, gate_w, at, size, at, strip) + add(u_hbm, up_w, at, size, at, strip)
        (NARROW if at < small else EXTRA).append(pair)

    def remote(source, target, send, recv, where):
        return pltpu.make_async_remote_copy(
            src_ref=source,
            dst_ref=target,
            send_sem=send,
            recv_sem=recv,
            device_id=where,
            device_id_type=pl.DeviceIdType.MESH,
        )

    def high_of(i):
        return items[i][0].shape[0] // 2

    def rows_of(i, origin, half):
        high = high_of(i)
        return pl.ds(pl.multiple_of((2 * origin + half) * high, high), high)

    def all_rows(i, origin):
        high = items[i][0].shape[0]
        return pl.ds(pl.multiple_of(origin * high, high), high)

    def lanes(start, size):
        return pl.ds(pl.multiple_of(start, 128), size)

    def piece(i, origin, half):
        _, target, _, size, place = items[i]
        return target.at[rows_of(i, origin, half), pl.ds(place, size)]

    def own_rows(i, half):
        source, _, start, size, _ = items[i]
        high = high_of(i)
        return source.at[pl.ds(pl.multiple_of(half * high, high), high), pl.ds(start, size)]

    def spare(i, sent):
        return remote(sent, piece(i, z, 1 - y), s_grp.at[i, z], r_grp.at[i, z], {"fs": mate})

    def to_right(i, origin, source):
        return remote(
            source, piece(i, origin, y), s_right.at[i, origin], r_line.at[i, origin], {"fs": z + 1}
        )

    def to_left(i, origin, source):
        return remote(
            source, piece(i, origin, y), s_left.at[i, origin], r_line.at[i, origin], {"fs": z - 1}
        )

    def to_grp(i, origin, block):
        return remote(block, block, s_grp.at[i, origin], r_grp.at[i, origin], {"grp": 1 - y})

    def local_copy(i):
        source, target, start, size, place = items[i]
        return pltpu.make_async_copy(
            source.at[:, pl.ds(start, size)],
            target.at[all_rows(i, z), pl.ds(place, size)],
            local.at[i],
        )

    def start_own(group):
        for i in group:
            own = own_rows(i, y)
            pl.when(z + 1 < n)(lambda i=i, own=own: to_right(i, z, own).start())
            pl.when(z >= 1)(lambda i=i, own=own: to_left(i, z, own).start())
            local_copy(i).start()
        for i in group:
            pl.when(outer)(lambda i=i: spare(i, own_rows(i, 1 - y)).start())

    def sides(d):
        return (
            (z >= d, z - d, z + 1 < n, to_right, z >= 2),
            (z + d < n, z + d, z >= 1, to_left, z < n - 2),
        )

    def pass_on(group, distances):
        for d in distances:
            for i in group:
                for there, origin, more, send, shared in sides(d):

                    @pl.when(there)
                    def _():
                        block = piece(i, origin, y)
                        send(i, origin, block).wait_recv()
                        pl.when(more)(lambda: send(i, origin, block).start())
                        if d == 1:
                            pl.when(shared)(lambda: to_grp(i, origin, block).start())
                        else:
                            to_grp(i, origin, block).start()

    def complete(group):
        for i in group:
            local_copy(i).wait()
            for d in range(1, n):
                for cond, origin in ((z >= d, z - d), (z + d < n, z + d)):
                    pl.when(cond)(
                        lambda i=i, o=origin: to_grp(i, o, piece(i, o, 1 - y)).wait_recv()
                    )

    def drain(group):
        for i in group:
            own = own_rows(i, y)
            pl.when(z + 1 < n)(lambda: to_right(i, z, own).wait_send())
            pl.when(z >= 1)(lambda: to_left(i, z, own).wait_send())
            pl.when(outer)(lambda: spare(i, own_rows(i, 1 - y)).wait_send())
            for d in range(1, n):
                for there, origin, more, send, shared in sides(d):

                    @pl.when(there)
                    def _():
                        block = piece(i, origin, y)
                        pl.when(more)(lambda: send(i, origin, block).wait_send())
                        if d == 1:
                            pl.when(shared)(lambda: to_grp(i, origin, block).wait_send())
                        else:
                            to_grp(i, origin, block).wait_send()

    origins = (mate, cross, far)
    EXTRAS = [i for pair in EXTRA for i in pair]

    def cut_rows(i, half, to):
        source, _, start, size, _ = items[i]
        high = high_of(i)
        offset = start if i in EXTRAS else to * big + start
        return source.at[pl.ds(pl.multiple_of(half * high, high), high), lanes(offset, size)]

    def to_mate(i, origin, sent):
        return remote(
            sent, piece(i, origin, y), s_right.at[i, origin], r_line.at[i, origin], {"fs": mate}
        )

    def to_cross(i):
        return remote(
            cut_rows(i, y, 1 - side),
            piece(i, z, y),
            s_left.at[i, z],
            r_line.at[i, z],
            {"fs": cross},
        )

    def keep(i):
        source, target, start, size, place = items[i]
        offset = start if i in EXTRAS else side * big + start
        return pltpu.make_async_copy(
            source.at[:, lanes(offset, size)],
            target.at[all_rows(i, z), pl.ds(place, size)],
            local.at[i],
        )

    def start_near(pair, ends):
        for i in pair:
            if i not in EXTRAS:
                to_mate(i, z, cut_rows(i, y, side)).start()
                keep(i).start()
            elif ends:
                to_mate(i, z, cut_rows(i, y, side)).start()
            else:
                keep(i).start()

    def start_cross(pair):
        for i in pair:
            to_cross(i).start()

    def start_spare(pair):
        for i in pair:
            spare(i, cut_rows(i, 1 - y, side)).start()

    def pass_cut(pair, k):
        def step(i):
            origin = origins[k]
            block = piece(i, origin, y)
            to_mate(i, origin, block).wait_recv()
            if i in EXTRAS:
                if k:
                    to_grp(i, origin, block).start()
                return
            if k:
                pl.when(inner)(lambda: to_mate(i, origin, block).start())
            to_grp(i, origin, block).start()

        for i in pair:
            if i in EXTRAS:
                pl.when(inner)(lambda i=i: step(i))
            else:
                step(i)

    def complete_cut(pair):
        def step(i):
            keep(i).wait()
            for origin in origins:
                to_grp(i, origin, piece(i, origin, 1 - y)).wait_recv()

        for i in pair:
            if i in EXTRAS:
                pl.when(inner)(lambda i=i: step(i))
            else:
                step(i)

    def drain_cut(pair):
        for i in pair:
            to_cross(i).wait_send()
            if i in EXTRAS:

                @pl.when(outer)
                def _():
                    to_mate(i, z, cut_rows(i, y, side)).wait_send()
                    spare(i, cut_rows(i, 1 - y, side)).wait_send()

                @pl.when(inner)
                def _():
                    for k in (1, 2):
                        to_grp(i, origins[k], piece(i, origins[k], y)).wait_send()

            else:
                to_mate(i, z, cut_rows(i, y, side)).wait_send()
                for k in range(3):
                    block = piece(i, origins[k], y)
                    if k:
                        pl.when(inner)(
                            lambda k=k, b=block: to_mate(i, origins[k], b).wait_send()
                        )
                    to_grp(i, origins[k], block).wait_send()

    depth = d_hbm.shape[0]
    sub, rest = small - depth, big - 2 * depth

    def down_block(c, start, size):
        return down_w.at[pl.ds(pl.multiple_of(start, 16), size), pl.ds(c * wide, wide)]

    def down_src(c, start, size):
        return d_hbm.at[pl.ds(pl.multiple_of(start, 16), size), pl.ds(c * wide, wide)]

    def end_place(c, start, size):
        return down_block(c, side * sub + start, size)

    def near_place(c, start, size):
        return down_block(c, (1 - side) * depth + start, size)

    def near_src(c, start, size):
        return down_src(c, side * rest + start, size)

    def middle_place(c, whose, start, size):
        return down_block(c, small + whose * rest + start, size)

    def middle_src(c, start, size):
        return down_src(c, (1 - side) * sub + start, size)

    def halved(c, size, half, place):
        return place(c, half * (size // 2), size // 2)

    def from_mate(c, half, to_inner):
        if to_inner:
            return halved(c, depth, half, end_place)
        return halved(c, sub, half, near_place)

    def middle(c, whose, half):
        return middle_place(c, whose, half * (rest // 2), rest // 2)

    def down_to_mate(c, to_inner):
        sent = halved(c, depth, y, down_src) if to_inner else halved(c, sub, y, near_src)
        return remote(
            sent, from_mate(c, y, to_inner), s_down.at[c, 0], r_down.at[c, 0], {"fs": mate}
        )

    def down_to_cross(c):
        return remote(
            halved(c, rest, y, middle_src),
            middle(c, side, y),
            s_down.at[c, 1],
            r_down.at[c, 1],
            {"fs": cross},
        )

    def down_local(c, k):
        if k == 0:
            return pltpu.make_async_copy(
                down_src(c, 0, depth), end_place(c, 0, depth), l_down.at[c, 0]
            )
        if k == 1:
            return pltpu.make_async_copy(
                near_src(c, 0, sub), near_place(c, 0, sub), l_down.at[c, 0]
            )
        return pltpu.make_async_copy(
            middle_src(c, 0, rest), middle_place(c, side, 0, rest), l_down.at[c, 1]
        )

    def down_grp(c, k, block):
        return remote(block, block, sy_down.at[c, k], ry_down.at[c, k], {"grp": 1 - y})

    def start_down(c):
        @pl.when(outer)
        def _():
            down_to_mate(c, True).start()
            down_local(c, 0).start()

        @pl.when(inner)
        def _():
            down_to_mate(c, False).start()
            down_local(c, 1).start()

    def start_middle(c):
        down_to_cross(c).start()
        down_local(c, 2).start()

    def down_arrival(c, k, block):
        return remote(block, block, s_down.at[c, k], r_down.at[c, k], {"fs": mate})

    def pass_down(c):
        @pl.when(outer)
        def _():
            block = from_mate(c, y, False)
            down_arrival(c, 0, block).wait_recv()
            down_grp(c, 0, block).start()

        @pl.when(inner)
        def _():
            for k, block in ((0, from_mate(c, y, True)), (1, middle(c, 1 - side, y))):
                down_arrival(c, k, block).wait_recv()
                down_grp(c, k, block).start()

    def complete_down(c):
        @pl.when(outer)
        def _():
            down_local(c, 0).wait()
            down_grp(c, 0, from_mate(c, 1 - y, False)).wait_recv()

        @pl.when(inner)
        def _():
            down_local(c, 1).wait()
            down_local(c, 2).wait()
            down_grp(c, 0, from_mate(c, 1 - y, True)).wait_recv()
            down_grp(c, 1, middle(c, 1 - side, 1 - y)).wait_recv()

    def drain_down(c):
        @pl.when(outer)
        def _():
            down_to_mate(c, True).wait_send()
            down_grp(c, 0, from_mate(c, y, False)).wait_send()

        @pl.when(inner)
        def _():
            down_to_mate(c, False).wait_send()
            down_to_cross(c).wait_send()
            down_grp(c, 0, from_mate(c, y, True)).wait_send()
            down_grp(c, 1, middle(c, 1 - side, y)).wait_send()

    def sum_core1(c):
        return remote(
            part1.at[c, :, 1 - ci], core1.at[c], s_sum.at[c, 0], r_sum.at[c, 0], {"tp": core_peer}
        )

    def sum_line1(c):
        return remote(
            send1.at[c], line1.at[c], s_sum.at[c, 1], r_sum.at[c, 1], {"tp": line_peer}
        )

    def sum_core2(c):
        return remote(
            part2.at[c, :, :, 1 - ci],
            core2.at[c],
            s_sum.at[c, 2],
            r_sum.at[c, 2],
            {"tp": core_peer},
        )

    def sum_line2(c):
        return remote(
            send2.at[c], line2.at[c], s_sum.at[c, 3], r_sum.at[c, 3], {"tp": line_peer}
        )

    def sum_line3(c):
        return remote(
            send3.at[c], line3.at[c], s_sum.at[c, 4], r_sum.at[c, 4], {"fs": partner}
        )

    lump = share // parts

    def rows_at(which, t, p):
        start = pl.multiple_of(which * rows + t * share + p * lump, lump)
        return second.at[pl.ds(start, lump)]

    def give(p, slot, which, t, where, target=None):
        block = rows_at(which, t, p)
        return remote(
            block,
            block if target is None else target,
            s_share.at[slot, p],
            r_share.at[slot, p],
            where,
        )

    def to_partner(p):
        return give(p, 0, 0, me, {"fs": partner}, rows_at(1, me, p))

    def across(p, which):
        return give(p, 1 + which, which, me, {"tp": line_peer})

    def across_arrival(p, which):
        return give(p, 1 + which, which, line_peer, {"tp": line_peer})

    def over(p, which, mine):
        return give(p, 3 + 2 * which + (1 - mine), which, me if mine else line_peer, {"tp": core_peer})

    def over_arrival(p, which, mine):
        t = core_peer if mine else 2 * (1 - xi) + 1 - ci
        return give(p, 3 + 2 * which + (1 - mine), which, t, {"tp": core_peer})

    def fin(c, slot, t, where):
        block = result.at[c, t]
        return remote(block, block, s_fin.at[c, slot], r_fin.at[c, slot], where)

    def put(c, t):
        r = pl.ds(pl.multiple_of(t * share, share), share)
        return pltpu.make_async_copy(
            result.at[c, t], out_hbm.at[r, pl.ds(c * wide, wide)], store.at[c, t]
        )

    barrier = pltpu.get_barrier_semaphore()

    def greet(where):
        pl.semaphore_signal(
            barrier, inc=1, device_id=where, device_id_type=pl.DeviceIdType.MESH
        )

    get_x = pltpu.make_async_copy(x_hbm, x_ref, load)
    get_x.start()
    for where in ({"grp": 1 - y}, {"tp": core_peer}, {"tp": line_peer}, {"fs": partner}):
        greet(where)
    pl.when(z + 1 < n)(lambda: greet({"fs": z + 1}))
    pl.when(z >= 1)(lambda: greet({"fs": z - 1}))
    pl.semaphore_wait(barrier, 4 + jnp.minimum(z, 1) + jnp.minimum(n - 1 - z, 1))

    start_own(QKV)

    @pl.when(outer)
    def _():
        hidden[:, small:] = jnp.zeros((2 * rows, big - small), bf16)
        down_w[small:] = jnp.zeros((big - small, width), bf16)

    get_x.wait()
    tall = min(64, share)

    def norm_step(s, carry):
        r = pl.ds(pl.multiple_of(s * tall, tall), tall)
        normed[r] = norm_rows(x_ref[r], gain1_ref[...]).astype(bf16)
        return carry

    lax.fori_loop(0, rows // tall, norm_step, 0)
    lowrank[...] = lax.dot_general(
        normed[...], first_ref[...], (((1,), (1,)), ((), ())), preferred_element_type=f32
    ).astype(bf16)
    extra[...] = extra_ref[...].T

    def tiles(total, body, tile=256):
        def step(s, carry):
            body(pl.multiple_of(s * tile, tile), tile)
            return carry

        lax.fori_loop(0, total // tile, step, 0)
        if total % tile:
            body(total - total % tile, total % tile)

    pl.when(outer)(lambda: start_own(OUT))
    pass_on(QKV, (1, 2))

    @pl.when(inner)
    def _():
        start_own(OUT)

    @pl.when(outer)
    def _():
        for pair in NARROW:
            start_cross(pair)
            start_near(pair, True)

    pass_on(QKV, (3,))
    complete(QKV)

    def project(at, size):
        qkv[:, pl.ds(at, size)] = jnp.dot(
            normed[...], qkv_w[:, pl.ds(at, size)], preferred_element_type=f32
        ).astype(bf16)

    tiles(qkv_w.shape[1], project)
    pass_on(OUT, (1,))

    @pl.when(inner)
    def _():
        for pair in NARROW:
            start_cross(pair)

    for h in range(heads):
        attention_kernel(heads, qkv, lowrank, second_ref, bias_ref, extra, hgain_ref, headed, [h])
        if h == 0:
            pass_on(OUT, (2,))

            @pl.when(inner)
            def _():
                start_near(NARROW[0], False)
                for pair in EXTRA:
                    start_cross(pair)

    @pl.when(outer)
    def _():
        for pair in EXTRA:
            start_cross(pair)
            start_near(pair, True)

    pass_on(OUT, (3,))

    @pl.when(inner)
    def _():
        for pair in NARROW[1:]:
            start_near(pair, False)
        for c in range(chunks):
            start_middle(c)

    complete(OUT)

    for c in range(chunks):
        mixed = jnp.dot(
            headed[...], out_w[:, c * wide : (c + 1) * wide], preferred_element_type=f32
        ).astype(bf16)
        part1[c] = mixed.reshape(2, 2, share, wide)
        sum_core1(c).start()
    pass_cut(NARROW[0], 0)
    for c in range(chunks):
        sum_core1(c).wait_recv()
        send1[c] = (part1[c, 1 - xi, ci].astype(f32) + core1[c, 1 - xi].astype(f32)).astype(bf16)
        sum_line1(c).start()
    pl.when(inner)(lambda: [start_near(pair, False) for pair in EXTRA] and None)
    pass_cut(NARROW[0], 1)
    own = pl.ds(pl.multiple_of(me * share, share), share)
    for c in range(chunks):
        sum_line1(c).wait_recv()
        cols = slice(c * wide, (c + 1) * wide)
        total = part1[c, xi, ci].astype(f32) + core1[c, xi].astype(f32) + line1[c].astype(f32)
        resid[:, cols] = (x_ref[own, cols].astype(f32) + total).astype(bf16)
    for p in range(parts):
        value = resid[p * lump : (p + 1) * lump]
        start = pl.multiple_of(me * share + p * lump, lump)
        second[pl.ds(start, lump)] = norm_rows(value, gain2_ref[...]).astype(bf16)
        to_partner(p).start()
        across(p, 0).start()
        over(p, 0, 1).start()

    def gate_up(which, pairs):
        r = slice(which * rows, (which + 1) * rows)

        def run(start, size):
            def step(s, carry):
                cols = pl.ds(pl.multiple_of(start + s * 128, 128), 128)
                both = jnp.dot(
                    second[r],
                    jnp.concatenate([gate_w[:, cols], up_w[:, cols]], axis=1),
                    preferred_element_type=f32,
                )
                hidden[r, cols] = (jax.nn.silu(both[:, :128]) * both[:, 128:]).astype(bf16)
                return carry

            lax.fori_loop(0, size // 128, step, 0)

        first, last = items[pairs[0][0]], items[pairs[-1][0]]
        run(first[4], last[4] + last[3] - first[4])

    def relay_own():
        for p in range(parts):
            across_arrival(p, 0).wait_recv()
            over(p, 0, 0).start()

    def relay_partner():
        for p in range(parts):
            give(p, 0, 1, me, {"fs": partner}).wait_recv()
            across(p, 1).start()
            over(p, 1, 1).start()

    @pl.when(outer)
    def _():
        for c in range(chunks):
            start_down(c)
        for pair in EXTRA:
            start_spare(pair)
        pass_cut(NARROW[0], 2)
        for pair in NARROW[1:]:
            pass_cut(pair, 0)
        relay_own()
        for pair in NARROW[1:]:
            pass_cut(pair, 1)
        relay_partner()
        for pair in NARROW[1:]:
            pass_cut(pair, 2)

    @pl.when(inner)
    def _():
        pass_cut(NARROW[0], 2)
        for k in range(2):
            for pair in NARROW[1:]:
                pass_cut(pair, k)
        relay_own()
        for pair in NARROW[1:]:
            pass_cut(pair, 2)
        for c in range(chunks):
            start_down(c)
        for pair in EXTRA:
            for k in range(3):
                pass_cut(pair, k)
        relay_partner()

    for p in range(parts):
        over_arrival(p, 0, 1).wait_recv()
        over_arrival(p, 0, 0).wait_recv()
    complete_cut(NARROW[0])
    gate_up(0, NARROW[:1])
    pass_down(0)
    for p in range(parts):
        across_arrival(p, 1).wait_recv()
        over(p, 1, 0).start()
    for pair in NARROW[1:]:
        complete_cut(pair)
    gate_up(0, NARROW[1:])
    pass_down(1)
    for p in range(parts):
        over_arrival(p, 1, 1).wait_recv()
        over_arrival(p, 1, 0).wait_recv()
    gate_up(1, NARROW)
    for c in range(2, chunks):
        pass_down(c)
    for pair in EXTRA:
        complete_cut(pair)

        @pl.when(inner)
        def _():
            for which in range(2):
                gate_up(which, [pair])

    def sum_a(c):
        complete_down(c)
        for which in range(2):
            out = jnp.dot(
                hidden[which * rows : (which + 1) * rows],
                down_w[:, c * wide : (c + 1) * wide],
                preferred_element_type=f32,
            ).astype(bf16)
            part2[c, which] = out.reshape(2, 2, share, wide)
        sum_core2(c).start()

    def sum_b(c):
        sum_core2(c).wait_recv()
        for which in range(2):
            send2[c, which] = (
                part2[c, which, 1 - xi, ci].astype(f32) + core2[c, which, 1 - xi].astype(f32)
            ).astype(bf16)
        sum_line2(c).start()

    def held(c, which):
        return (
            part2[c, which, xi, ci].astype(f32)
            + core2[c, which, xi].astype(f32)
            + line2[c, which].astype(f32)
        )

    def sum_c(c):
        sum_line2(c).wait_recv()
        send3[c] = held(c, 1).astype(bf16)
        sum_line3(c).start()

    def sum_d(c):
        sum_line3(c).wait_recv()
        total = held(c, 0) + line3[c].astype(f32)
        value = resid[:, c * wide : (c + 1) * wide].astype(f32) + total
        result[c, me] = value.astype(bf16)
        fin(c, 0, me, {"tp": line_peer}).start()
        fin(c, 1, me, {"tp": core_peer}).start()
        put(c, me).start()

    def sum_e(c):
        fin(c, 0, line_peer, {"tp": line_peer}).wait_recv()
        fin(c, 2, line_peer, {"tp": core_peer}).start()
        put(c, line_peer).start()

    corner = 2 * (1 - xi) + 1 - ci

    def sum_f(c):
        fin(c, 1, core_peer, {"tp": core_peer}).wait_recv()
        put(c, core_peer).start()
        fin(c, 2, corner, {"tp": core_peer}).wait_recv()
        put(c, corner).start()

    stages = (sum_a, sum_b, sum_c, sum_d, sum_e, sum_f)
    for step in range(chunks + len(stages) - 1):
        for k, stage in enumerate(stages):
            if 0 <= step - k < chunks:
                stage(step - k)

    for c in range(chunks):
        for t in (me, core_peer, line_peer, corner):
            put(c, t).wait()
        fin(c, 0, me, {"tp": line_peer}).wait_send()
        fin(c, 1, me, {"tp": core_peer}).wait_send()
        fin(c, 2, line_peer, {"tp": core_peer}).wait_send()
        for copy in (sum_core1, sum_line1, sum_core2, sum_line2, sum_line3):
            copy(c).wait_send()
        drain_down(c)
    for p in range(parts):
        to_partner(p).wait_send()
        for which in range(2):
            across(p, which).wait_send()
            over(p, which, 1).wait_send()
            over(p, which, 0).wait_send()
    drain(QKV)
    drain(OUT)
    for pair in NARROW + EXTRA:
        drain_cut(pair)


def narrow_units(units):
    return units // 128 * 3 // 8 * 128


def fits(x, q, k, v, o, g, u, d):
    copies, n, count = (lax.axis_size(a) for a in ("grp", "fs", "tp"))
    rows, width = x.shape
    if (copies, n, count) != (2, 4, 4) or rows % (64 * count) or width % 512:
        return False
    for p in (q, k, v, o, g, u, d):
        if p.shape[0] % 32 or p.shape[1] % 128:
            return False
    units, depth = g.shape[1], d.shape[0]
    small = narrow_units(units)
    sub, rest = small - depth, units - small - 2 * depth
    if min(sub, rest) <= 0 or sub % 32 or rest % 32:
        return False
    if small % 256:
        return False
    held = n * (q.size + k.size + v.size + o.size) + 3 * (units - small) * n * g.shape[0]
    return 2 * held + 24 * x.size <= 54 * 2**20


def fused(x, gain1, q, k, v, first, second, bias, extra, hgain, o, gain2, g, u, d):
    n, count = lax.axis_size("fs"), lax.axis_size("tp")
    rows, width = x.shape
    share = rows // count
    heads = extra.shape[1]
    chunks, parts = 4, 2
    wide = width // chunks
    bf16, f32 = jnp.bfloat16, jnp.float32
    vmem, hbm = pl.BlockSpec(memory_space=pltpu.VMEM), pl.BlockSpec(memory_space=pl.ANY)
    qkv_cols = 2 * q.shape[1] + v.shape[1]
    held = heads * hgain.shape[0]
    units = g.shape[1]
    small = narrow_units(units)
    big = units - small
    buffers = [
        ((rows, width), bf16),
        ((n * q.shape[0], qkv_cols), bf16),
        ((n * o.shape[0], width), bf16),
        ((n * g.shape[0], big), bf16),
        ((n * u.shape[0], big), bf16),
        ((big, width), bf16),
        ((rows, width), bf16),
        ((rows, first.shape[1]), bf16),
        ((rows, heads), f32),
        ((rows, qkv_cols), bf16),
        ((rows, held), bf16),
        ((chunks, 2, 2, share, wide), bf16),
        ((chunks, 2, share, wide), bf16),
        ((chunks, share, wide), bf16),
        ((chunks, share, wide), bf16),
        ((share, width), bf16),
        ((2 * rows, width), bf16),
        ((2 * rows, big), bf16),
        ((chunks, 2, 2, 2, share, wide), bf16),
        ((chunks, 2, 2, share, wide), bf16),
        ((chunks, 2, share, wide), bf16),
        ((chunks, 2, share, wide), bf16),
        ((chunks, share, wide), bf16),
        ((chunks, share, wide), bf16),
        ((chunks, count, share, wide), bf16),
    ]
    lots = sum(-(-size // 256) for size in (q.shape[1], k.shape[1], v.shape[1])) + chunks
    lots += 2 * (small // 256 + -(-(big - small) // 256))
    counts = [(lots, n)] * 5 + [(lots,)] + [(chunks, 2)] * 5
    counts += [(chunks, 5)] * 2 + [(7, parts)] * 2 + [(chunks, 3)] * 2 + [(chunks, count)]
    return pl.pallas_call(
        functools.partial(fused_kernel, (n, count, heads, chunks, small, parts)),
        out_shape=jax.ShapeDtypeStruct((rows, width), bf16),
        in_specs=[vmem] * 7 + [hbm] * 8,
        out_specs=hbm,
        scratch_shapes=[pltpu.VMEM(s, t) for s, t in buffers]
        + [pltpu.SemaphoreType.DMA(s) for s in counts]
        + [pltpu.SemaphoreType.DMA],
        compiler_params=pltpu.CompilerParams(
            vmem_limit_bytes=62 * 1024 * 1024, collective_id=0, has_side_effects=True
        ),
    )(
        gain1[None, :],
        first.T,
        second,
        bias[None, :],
        extra.T,
        hgain[None, :],
        gain2[None, :],
        *(x, q, k, v, o, g, u, d),
    )


def shards(*arrays):
    if fits(*[arrays[i] for i in (0, 2, 3, 4, 10, 12, 13, 14)]):
        return fused(*arrays)
    return spread(*arrays)


def spread(
    layer_input_tokens,
    attention_norm_gain,
    query_projection,
    key_projection,
    value_projection,
    decay_first_factor,
    decay_second_factor,
    decay_logit_bias,
    extra_log_decay,
    head_output_gain,
    attention_output_projection,
    feedforward_norm_gain,
    gate_projection,
    up_projection,
    down_projection,
):
    rows = layer_input_tokens.shape[0]
    count = lax.axis_size("tp")
    me = lax.axis_index("tp")
    share = rows // count
    qkv_full = gather_shared(
        jnp.concatenate([query_projection, key_projection, value_projection], axis=1)
    )
    out_full = gather_shared(attention_output_projection)
    gate_full = gather_shared(gate_projection)
    up_full = gather_shared(up_projection)
    down_full = gather_shared(down_projection, 2)

    normed = norm_rows(layer_input_tokens, attention_norm_gain).astype(jnp.bfloat16)
    lowrank = jnp.dot(normed, decay_first_factor, preferred_element_type=jnp.float32).astype(
        jnp.bfloat16
    )
    qkv = shared_dot(normed, qkv_full)
    headed = attention(
        qkv, lowrank, decay_second_factor, decay_logit_bias, extra_log_decay, head_output_gain
    )
    turned = jnp.concatenate(
        [
            lax.dynamic_slice_in_dim(headed, lax.rem(me - j + count, count) * share, share, 0)
            for j in range(count)
        ],
        axis=0,
    )
    mixer = scatter_sum(shared_dot(turned, out_full), share)
    own = lax.dynamic_slice_in_dim(layer_input_tokens, me * share, share, 0)
    residual = (own.astype(jnp.float32) + mixer).astype(jnp.bfloat16)
    mine = norm_rows(residual, feedforward_norm_gain).astype(jnp.bfloat16)
    second = jnp.concatenate([mine] + [step_on(mine, j) for j in range(1, count)], axis=0)
    hidden = in_order(
        [
            (gated(second, g_own, u_own), gated(second, g_other, u_other))
            for (g_own, g_other), (u_own, u_other) in zip(gate_full, up_full)
        ]
    )
    channel = scatter_sum(shared_dot(hidden, down_full), share)
    finished = (residual.astype(jnp.float32) + channel).astype(jnp.bfloat16)
    return lax.all_gather(finished, "tp", axis=0, tiled=True)


def solution(mesh):
    placed = (
        P(("grp", "fs"), None),
        P(),
        P("fs", "tp"),
        P("fs", "tp"),
        P("fs", "tp"),
        P(),
        P(None, "tp"),
        P("tp"),
        P(("grp", "fs"), "tp"),
        P(),
        P(("tp", "fs"), None),
        P(),
        P("fs", "tp"),
        P("fs", "tp"),
        P(("tp", "fs"), None),
    )
    return jax.shard_map(
        shards, mesh=mesh, in_specs=placed, out_specs=P(("grp", "fs"), None), check_vma=False
    )
```

```python
import functools

import jax
import jax.numpy as jnp
from jax import lax
from jax.experimental import pallas as pl
from jax.experimental.pallas import tpu as pltpu
from jax.sharding import PartitionSpec as P

BLOCK = 64
DECAY_GATE = 16.0


def norm_rows(values, gain):
    wide = values.astype(jnp.float32)
    scale = lax.rsqrt(jnp.mean(wide * wide, axis=-1, keepdims=True) + 1e-06)
    return wide * scale * gain


def attention_kernel(heads, qkv_ref, lowrank_ref, second_ref, bias_ref, extra_ref, gain_ref, out_ref, which=None):
    rows = qkv_ref.shape[0]
    kc = second_ref.shape[1] // heads
    vc = out_ref.shape[1] // heads
    count = rows // BLOCK
    f32, bf16 = jnp.float32, jnp.bfloat16
    row_id = lax.broadcasted_iota(jnp.int32, (BLOCK, BLOCK), 0)
    col_id = lax.broadcasted_iota(jnp.int32, (BLOCK, BLOCK), 1)
    lower = row_id >= col_id
    upper = row_id <= col_id
    lower_ones = jnp.where(lower, 1.0, 0.0).astype(f32)
    half = BLOCK // 2
    for h in which or range(heads):
        kcols = slice(h * kc, (h + 1) * kc)
        logits = (
            jnp.dot(lowrank_ref[...], second_ref[:, kcols], preferred_element_type=f32)
            + bias_ref[:, kcols]
        )
        log_sig = jnp.minimum(logits, 0.0) - jnp.log1p(jnp.exp(-jnp.abs(logits)))
        decay = log_sig / DECAY_GATE + extra_ref[:, h : h + 1]
        queries_fb, updates, closings, scores = [], [], [], []
        for b in range(count):
            r = slice(b * BLOCK, (b + 1) * BLOCK)
            d = decay[r]
            q = qkv_ref[r, h * kc : (h + 1) * kc].astype(f32)
            k = qkv_ref[r, (heads + h) * kc : (heads + h + 1) * kc].astype(f32)
            v = qkv_ref[r, 2 * heads * kc + h * vc : 2 * heads * kc + (h + 1) * vc]
            run = jnp.dot(lower_ones, d, precision=lax.Precision.HIGHEST, preferred_element_type=f32)
            closing = run[BLOCK - 1 : BLOCK]
            back = closing - run + d
            mid_f = run[half - 1 : half]
            mid_b = back[half : half + 1]
            qf = (q * jnp.exp(run - mid_f)).astype(bf16)
            kf = (k * jnp.exp(mid_f - run)).astype(bf16)
            qb = (q * jnp.exp(back - mid_b)).astype(bf16)
            kb = (k * jnp.exp(mid_b - back)).astype(bf16)
            nt = (((1,), (1,)), ((), ()))
            sf = lax.dot_general(qf, kf, nt, preferred_element_type=f32)
            sb = lax.dot_general(qb, kb, nt, preferred_element_type=f32)
            scores.append(
                (jnp.where(lower, sf, 0.0) + jnp.where(upper, sb, 0.0)).astype(bf16)
            )
            queries_fb.append(
                jnp.concatenate([q * jnp.exp(run), q * jnp.exp(back)], axis=1).astype(bf16)
            )
            keys_fb = jnp.concatenate(
                [k * jnp.exp(closing - run), k * jnp.exp(closing - back)], axis=1
            ).astype(bf16)
            updates.append(
                lax.dot_general(v, keys_fb, (((0,), (0,)), ((), ())), preferred_element_type=f32)
            )
            closings.append(jnp.exp(closing))
        state = jnp.zeros((vc, kc), f32)
        ahead = []
        for b in range(count):
            ahead.append(state.astype(bf16))
            state = state * closings[b] + updates[b][:, :kc]
        state = jnp.zeros((vc, kc), f32)
        behind = [None] * count
        for b in reversed(range(count)):
            behind[b] = state.astype(bf16)
            state = state * closings[b] + updates[b][:, kc:]
        for b in range(count):
            r = slice(b * BLOCK, (b + 1) * BLOCK)
            v = qkv_ref[r, 2 * heads * kc + h * vc : 2 * heads * kc + (h + 1) * vc]
            states = jnp.concatenate([ahead[b], behind[b]], axis=1)
            mixed = lax.dot_general(
                queries_fb[b], states, (((1,), (1,)), ((), ())), preferred_element_type=f32
            ) + jnp.dot(scores[b], v, preferred_element_type=f32)
            scale = lax.rsqrt(jnp.mean(mixed * mixed, axis=-1, keepdims=True) + 1e-06)
            out_ref[r, h * vc : (h + 1) * vc] = (mixed * scale * gain_ref[...]).astype(bf16)


def attention(qkv, lowrank, second_factor, bias, extra, gain):
    rows = qkv.shape[0]
    heads = extra.shape[1]
    width = heads * gain.shape[0]
    kc = second_factor.shape[1] // heads
    return pl.pallas_call(
        functools.partial(attention_kernel, heads),
        out_shape=jax.ShapeDtypeStruct((rows, width), jnp.bfloat16),
        in_specs=[pl.BlockSpec(memory_space=pltpu.VMEM)] * 6,
        out_specs=pl.BlockSpec(memory_space=pltpu.VMEM),
        compiler_params=pltpu.CompilerParams(vmem_limit_bytes=32 * 1024 * 1024),
        cost_estimate=pl.CostEstimate(
            flops=40 * rows * kc * width, bytes_accessed=4 * rows * width * 2, transcendentals=0
        ),
    )(qkv, lowrank, second_factor, bias[None, :], extra, gain[None, :])


def gather_shared(piece, chunks=1):
    copies = lax.axis_size("grp")
    if copies != 2 or piece.shape[1] % (copies * chunks):
        return [(lax.all_gather(piece, "fs", axis=0, tiled=True), None)]
    wide = piece.shape[1] // chunks
    part = wide // copies
    pairs = []
    for chunk in range(chunks):
        start = chunk * wide + lax.axis_index("grp") * part
        own = lax.all_gather(
            lax.dynamic_slice_in_dim(piece, start, part, 1), "fs", axis=0, tiled=True
        )
        pairs.append((own, lax.ppermute(own, "grp", [(0, 1), (1, 0)])))
    return pairs


def in_order(pairs):
    if pairs[0][1] is None:
        return pairs[0][0]
    first = lax.axis_index("grp") == 0
    blocks = []
    for own, other in pairs:
        blocks += [jnp.where(first, own, other), jnp.where(first, other, own)]
    return jnp.concatenate(blocks, axis=1)


def times(left, right):
    if right is None:
        return None
    return jnp.dot(left, right, preferred_element_type=jnp.float32)


def shared_dot(left, pairs):
    def rounded(right):
        return None if right is None else times(left, right).astype(jnp.bfloat16)

    return in_order([(rounded(own), rounded(other)) for own, other in pairs])


def gated(second, gate_weight, up_weight):
    if gate_weight is None:
        return None
    gate, up = times(second, gate_weight), times(second, up_weight)
    return (jax.nn.silu(gate) * up).astype(jnp.bfloat16)


def step_back(values, hops):
    count = lax.axis_size("tp")
    return lax.ppermute(values, "tp", [(i, (i - hops) % count) for i in range(count)])


def step_on(values, hops):
    count = lax.axis_size("tp")
    return lax.ppermute(values, "tp", [(i, (i + hops) % count) for i in range(count)])


def scatter_sum(partial, share):
    count = lax.axis_size("tp")
    total = partial[:share].astype(jnp.float32)
    arrived = [step_back(partial[j * share : (j + 1) * share], j) for j in range(1, count)]
    for block in arrived:
        total = total + block.astype(jnp.float32)
    return total


def fused_kernel(
    shape,
    gain1_ref,
    first_ref,
    second_ref,
    bias_ref,
    extra_ref,
    hgain_ref,
    gain2_ref,
    x_hbm,
    q_hbm,
    k_hbm,
    v_hbm,
    o_hbm,
    g_hbm,
    u_hbm,
    d_hbm,
    out_hbm,
    x_ref,
    qkv_w,
    out_w,
    gate_w,
    up_w,
    down_w,
    normed,
    lowrank,
    extra,
    qkv,
    headed,
    part1,
    core1,
    send1,
    line1,
    resid,
    second,
    hidden,
    part2,
    core2,
    send2,
    line2,
    send3,
    line3,
    result,
    s_right,
    s_left,
    s_grp,
    r_line,
    r_grp,
    local,
    s_down,
    r_down,
    sy_down,
    ry_down,
    l_down,
    s_sum,
    r_sum,
    s_share,
    r_share,
    s_fin,
    r_fin,
    store,
    load,
):
    n, count, heads, chunks, small, parts = shape
    f32, bf16 = jnp.float32, jnp.bfloat16
    z, y, me = lax.axis_index("fs"), lax.axis_index("grp"), lax.axis_index("tp")
    rows, width = x_ref.shape
    share = rows // count
    wide = width // chunks
    kcols, vcols = q_hbm.shape[1], v_hbm.shape[1]
    units = g_hbm.shape[1]
    big = units - small
    xi, ci = me // 2, lax.rem(me, 2)
    core_peer = 2 * xi + 1 - ci
    line_peer = 2 * (1 - xi) + ci
    side = z // 2
    mate = z + 1 - 2 * lax.rem(z, 2)
    partner = lax.rem(z + 2, n)
    inner = lax.rem(z + side, 2) == 1
    outer = jnp.logical_not(inner)
    cross = 2 - side
    far = 3 * (1 - side)

    strip = 256
    items = []

    def add(source, target, start, total, place, step):
        first = len(items)
        for at in range(0, total, step):
            size = min(step, total - at)
            items.append((source, target, start + at, size, place + at))
        return list(range(first, len(items)))

    QKV = add(q_hbm, qkv_w, 0, kcols, 0, strip)
    QKV += add(k_hbm, qkv_w, 0, kcols, kcols, strip)
    QKV += add(v_hbm, qkv_w, 0, vcols, 2 * kcols, strip)
    OUT = add(o_hbm, out_w, 0, width, 0, width // 4)
    NARROW, EXTRA = [], []
    for at in range(0, big, strip):
        most = small if at < small else big
        size = min(strip, most - at)
        pair = add(g_hbm, gate_w, at, size, at, strip) + add(u_hbm, up_w, at, size, at, strip)
        (NARROW if at < small else EXTRA).append(pair)

    def remote(source, target, send, recv, where):
        return pltpu.make_async_remote_copy(
            src_ref=source,
            dst_ref=target,
            send_sem=send,
            recv_sem=recv,
            device_id=where,
            device_id_type=pl.DeviceIdType.MESH,
        )

    def high_of(i):
        return items[i][0].shape[0] // 2

    def rows_of(i, origin, half):
        high = high_of(i)
        return pl.ds(pl.multiple_of((2 * origin + half) * high, high), high)

    def all_rows(i, origin):
        high = items[i][0].shape[0]
        return pl.ds(pl.multiple_of(origin * high, high), high)

    def lanes(start, size):
        return pl.ds(pl.multiple_of(start, 128), size)

    def piece(i, origin, half):
        _, target, _, size, place = items[i]
        return target.at[rows_of(i, origin, half), pl.ds(place, size)]

    def own_rows(i, half):
        source, _, start, size, _ = items[i]
        high = high_of(i)
        return source.at[pl.ds(pl.multiple_of(half * high, high), high), pl.ds(start, size)]

    def spare(i, sent):
        return remote(sent, piece(i, z, 1 - y), s_grp.at[i, z], r_grp.at[i, z], {"fs": mate})

    def to_right(i, origin, source):
        return remote(
            source, piece(i, origin, y), s_right.at[i, origin], r_line.at[i, origin], {"fs": z + 1}
        )

    def to_left(i, origin, source):
        return remote(
            source, piece(i, origin, y), s_left.at[i, origin], r_line.at[i, origin], {"fs": z - 1}
        )

    def to_grp(i, origin, block):
        return remote(block, block, s_grp.at[i, origin], r_grp.at[i, origin], {"grp": 1 - y})

    def local_copy(i):
        source, target, start, size, place = items[i]
        return pltpu.make_async_copy(
            source.at[:, pl.ds(start, size)],
            target.at[all_rows(i, z), pl.ds(place, size)],
            local.at[i],
        )

    def start_own(group):
        for i in group:
            own = own_rows(i, y)
            pl.when(z + 1 < n)(lambda i=i, own=own: to_right(i, z, own).start())
            pl.when(z >= 1)(lambda i=i, own=own: to_left(i, z, own).start())
            local_copy(i).start()
        for i in group:
            pl.when(outer)(lambda i=i: spare(i, own_rows(i, 1 - y)).start())

    def sides(d):
        return (
            (z >= d, z - d, z + 1 < n, to_right, z >= 2),
            (z + d < n, z + d, z >= 1, to_left, z < n - 2),
        )

    def pass_on(group, distances):
        for d in distances:
            for i in group:
                for there, origin, more, send, shared in sides(d):

                    @pl.when(there)
                    def _():
                        block = piece(i, origin, y)
                        send(i, origin, block).wait_recv()
                        pl.when(more)(lambda: send(i, origin, block).start())
                        if d == 1:
                            pl.when(shared)(lambda: to_grp(i, origin, block).start())
                        else:
                            to_grp(i, origin, block).start()

    def complete(group):
        for i in group:
            local_copy(i).wait()
            for d in range(1, n):
                for cond, origin in ((z >= d, z - d), (z + d < n, z + d)):
                    pl.when(cond)(
                        lambda i=i, o=origin: to_grp(i, o, piece(i, o, 1 - y)).wait_recv()
                    )

    def drain(group):
        for i in group:
            own = own_rows(i, y)
            pl.when(z + 1 < n)(lambda: to_right(i, z, own).wait_send())
            pl.when(z >= 1)(lambda: to_left(i, z, own).wait_send())
            pl.when(outer)(lambda: spare(i, own_rows(i, 1 - y)).wait_send())
            for d in range(1, n):
                for there, origin, more, send, shared in sides(d):

                    @pl.when(there)
                    def _():
                        block = piece(i, origin, y)
                        pl.when(more)(lambda: send(i, origin, block).wait_send())
                        if d == 1:
                            pl.when(shared)(lambda: to_grp(i, origin, block).wait_send())
                        else:
                            to_grp(i, origin, block).wait_send()

    origins = (mate, cross, far)
    EXTRAS = [i for pair in EXTRA for i in pair]

    def cut_rows(i, half, to):
        source, _, start, size, _ = items[i]
        high = high_of(i)
        offset = start if i in EXTRAS else to * big + start
        return source.at[pl.ds(pl.multiple_of(half * high, high), high), lanes(offset, size)]

    def to_mate(i, origin, sent):
        return remote(
            sent, piece(i, origin, y), s_right.at[i, origin], r_line.at[i, origin], {"fs": mate}
        )

    def to_cross(i):
        return remote(
            cut_rows(i, y, 1 - side),
            piece(i, z, y),
            s_left.at[i, z],
            r_line.at[i, z],
            {"fs": cross},
        )

    def keep(i):
        source, target, start, size, place = items[i]
        offset = start if i in EXTRAS else side * big + start
        return pltpu.make_async_copy(
            source.at[:, lanes(offset, size)],
            target.at[all_rows(i, z), pl.ds(place, size)],
            local.at[i],
        )

    def start_near(pair, ends):
        for i in pair:
            if i not in EXTRAS:
                to_mate(i, z, cut_rows(i, y, side)).start()
                keep(i).start()
            elif ends:
                to_mate(i, z, cut_rows(i, y, side)).start()
            else:
                keep(i).start()

    def start_cross(pair):
        for i in pair:
            to_cross(i).start()

    def start_spare(pair):
        for i in pair:
            spare(i, cut_rows(i, 1 - y, side)).start()

    def pass_cut(pair, k):
        def step(i):
            origin = origins[k]
            block = piece(i, origin, y)
            to_mate(i, origin, block).wait_recv()
            if i in EXTRAS:
                if k:
                    to_grp(i, origin, block).start()
                return
            if k:
                pl.when(inner)(lambda: to_mate(i, origin, block).start())
            to_grp(i, origin, block).start()

        for i in pair:
            if i in EXTRAS:
                pl.when(inner)(lambda i=i: step(i))
            else:
                step(i)

    def complete_cut(pair):
        def step(i):
            keep(i).wait()
            for origin in origins:
                to_grp(i, origin, piece(i, origin, 1 - y)).wait_recv()

        for i in pair:
            if i in EXTRAS:
                pl.when(inner)(lambda i=i: step(i))
            else:
                step(i)

    def drain_cut(pair):
        for i in pair:
            to_cross(i).wait_send()
            if i in EXTRAS:

                @pl.when(outer)
                def _():
                    to_mate(i, z, cut_rows(i, y, side)).wait_send()
                    spare(i, cut_rows(i, 1 - y, side)).wait_send()

                @pl.when(inner)
                def _():
                    for k in (1, 2):
                        to_grp(i, origins[k], piece(i, origins[k], y)).wait_send()

            else:
                to_mate(i, z, cut_rows(i, y, side)).wait_send()
                for k in range(3):
                    block = piece(i, origins[k], y)
                    if k:
                        pl.when(inner)(
                            lambda k=k, b=block: to_mate(i, origins[k], b).wait_send()
                        )
                    to_grp(i, origins[k], block).wait_send()

    depth = d_hbm.shape[0]
    sub, rest = small - depth, big - 2 * depth

    def down_block(c, start, size):
        return down_w.at[pl.ds(pl.multiple_of(start, 16), size), pl.ds(c * wide, wide)]

    def down_src(c, start, size):
        return d_hbm.at[pl.ds(pl.multiple_of(start, 16), size), pl.ds(c * wide, wide)]

    def end_place(c, start, size):
        return down_block(c, side * sub + start, size)

    def near_place(c, start, size):
        return down_block(c, (1 - side) * depth + start, size)

    def near_src(c, start, size):
        return down_src(c, side * rest + start, size)

    def middle_place(c, whose, start, size):
        return down_block(c, small + whose * rest + start, size)

    def middle_src(c, start, size):
        return down_src(c, (1 - side) * sub + start, size)

    def halved(c, size, half, place):
        return place(c, half * (size // 2), size // 2)

    def from_mate(c, half, to_inner):
        if to_inner:
            return halved(c, depth, half, end_place)
        return halved(c, sub, half, near_place)

    def middle(c, whose, half):
        return middle_place(c, whose, half * (rest // 2), rest // 2)

    def down_to_mate(c, to_inner):
        sent = halved(c, depth, y, down_src) if to_inner else halved(c, sub, y, near_src)
        return remote(
            sent, from_mate(c, y, to_inner), s_down.at[c, 0], r_down.at[c, 0], {"fs": mate}
        )

    def down_to_cross(c):
        return remote(
            halved(c, rest, y, middle_src),
            middle(c, side, y),
            s_down.at[c, 1],
            r_down.at[c, 1],
            {"fs": cross},
        )

    def down_local(c, k):
        if k == 0:
            return pltpu.make_async_copy(
                down_src(c, 0, depth), end_place(c, 0, depth), l_down.at[c, 0]
            )
        if k == 1:
            return pltpu.make_async_copy(
                near_src(c, 0, sub), near_place(c, 0, sub), l_down.at[c, 0]
            )
        return pltpu.make_async_copy(
            middle_src(c, 0, rest), middle_place(c, side, 0, rest), l_down.at[c, 1]
        )

    def down_grp(c, k, block):
        return remote(block, block, sy_down.at[c, k], ry_down.at[c, k], {"grp": 1 - y})

    def start_down(c):
        @pl.when(outer)
        def _():
            down_to_mate(c, True).start()
            down_local(c, 0).start()

        @pl.when(inner)
        def _():
            down_to_mate(c, False).start()
            down_local(c, 1).start()

    def start_middle(c):
        down_to_cross(c).start()
        down_local(c, 2).start()

    def down_arrival(c, k, block):
        return remote(block, block, s_down.at[c, k], r_down.at[c, k], {"fs": mate})

    def pass_down(c):
        @pl.when(outer)
        def _():
            block = from_mate(c, y, False)
            down_arrival(c, 0, block).wait_recv()
            down_grp(c, 0, block).start()

        @pl.when(inner)
        def _():
            for k, block in ((0, from_mate(c, y, True)), (1, middle(c, 1 - side, y))):
                down_arrival(c, k, block).wait_recv()
                down_grp(c, k, block).start()

    def complete_down(c):
        @pl.when(outer)
        def _():
            down_local(c, 0).wait()
            down_grp(c, 0, from_mate(c, 1 - y, False)).wait_recv()

        @pl.when(inner)
        def _():
            down_local(c, 1).wait()
            down_local(c, 2).wait()
            down_grp(c, 0, from_mate(c, 1 - y, True)).wait_recv()
            down_grp(c, 1, middle(c, 1 - side, 1 - y)).wait_recv()

    def drain_down(c):
        @pl.when(outer)
        def _():
            down_to_mate(c, True).wait_send()
            down_grp(c, 0, from_mate(c, y, False)).wait_send()

        @pl.when(inner)
        def _():
            down_to_mate(c, False).wait_send()
            down_to_cross(c).wait_send()
            down_grp(c, 0, from_mate(c, y, True)).wait_send()
            down_grp(c, 1, middle(c, 1 - side, y)).wait_send()

    def sum_core1(c):
        return remote(
            part1.at[c, :, 1 - ci], core1.at[c], s_sum.at[c, 0], r_sum.at[c, 0], {"tp": core_peer}
        )

    def sum_line1(c):
        return remote(
            send1.at[c], line1.at[c], s_sum.at[c, 1], r_sum.at[c, 1], {"tp": line_peer}
        )

    def sum_core2(c):
        return remote(
            part2.at[c, :, :, 1 - ci],
            core2.at[c],
            s_sum.at[c, 2],
            r_sum.at[c, 2],
            {"tp": core_peer},
        )

    def line_first(c):
        return c % 2 == 1 and c < chunks // 2

    def sum_line2(c):
        where = {"fs": partner} if line_first(c) else {"tp": line_peer}
        return remote(send2.at[c], line2.at[c], s_sum.at[c, 3], r_sum.at[c, 3], where)

    def sum_line3(c):
        where = {"tp": line_peer} if line_first(c) else {"fs": partner}
        return remote(send3.at[c], line3.at[c], s_sum.at[c, 4], r_sum.at[c, 4], where)

    lump = share // parts

    def rows_at(which, t, p):
        start = pl.multiple_of(which * rows + t * share + p * lump, lump)
        return second.at[pl.ds(start, lump)]

    def give(p, slot, which, t, where, target=None):
        block = rows_at(which, t, p)
        return remote(
            block,
            block if target is None else target,
            s_share.at[slot, p],
            r_share.at[slot, p],
            where,
        )

    def to_partner(p):
        return give(p, 0, 0, me, {"fs": partner}, rows_at(1, me, p))

    def across(p, which):
        return give(p, 1 + which, which, me, {"tp": line_peer})

    def across_arrival(p, which):
        return give(p, 1 + which, which, line_peer, {"tp": line_peer})

    def over(p, which, mine):
        return give(p, 3 + 2 * which + (1 - mine), which, me if mine else line_peer, {"tp": core_peer})

    def over_arrival(p, which, mine):
        t = core_peer if mine else 2 * (1 - xi) + 1 - ci
        return give(p, 3 + 2 * which + (1 - mine), which, t, {"tp": core_peer})

    def fin(c, slot, t, where):
        block = result.at[c, t]
        return remote(block, block, s_fin.at[c, slot], r_fin.at[c, slot], where)

    def put(c, t):
        r = pl.ds(pl.multiple_of(t * share, share), share)
        return pltpu.make_async_copy(
            result.at[c, t], out_hbm.at[r, pl.ds(c * wide, wide)], store.at[c, t]
        )

    barrier = pltpu.get_barrier_semaphore()

    def greet(where):
        pl.semaphore_signal(
            barrier, inc=1, device_id=where, device_id_type=pl.DeviceIdType.MESH
        )

    get_x = pltpu.make_async_copy(x_hbm, x_ref, load)
    get_x.start()
    for where in ({"grp": 1 - y}, {"tp": core_peer}, {"tp": line_peer}, {"fs": partner}):
        greet(where)
    pl.when(z + 1 < n)(lambda: greet({"fs": z + 1}))
    pl.when(z >= 1)(lambda: greet({"fs": z - 1}))
    pl.semaphore_wait(barrier, 4 + jnp.minimum(z, 1) + jnp.minimum(n - 1 - z, 1))

    start_own(QKV)

    @pl.when(outer)
    def _():
        hidden[:, small:] = jnp.zeros((2 * rows, big - small), bf16)
        down_w[small:] = jnp.zeros((big - small, width), bf16)

    get_x.wait()
    tall = min(64, share)

    def norm_step(s, carry):
        r = pl.ds(pl.multiple_of(s * tall, tall), tall)
        normed[r] = norm_rows(x_ref[r], gain1_ref[...]).astype(bf16)
        return carry

    lax.fori_loop(0, rows // tall, norm_step, 0)
    lowrank[...] = lax.dot_general(
        normed[...], first_ref[...], (((1,), (1,)), ((), ())), preferred_element_type=f32
    ).astype(bf16)
    extra[...] = extra_ref[...].T

    def tiles(total, body, tile=256):
        def step(s, carry):
            body(pl.multiple_of(s * tile, tile), tile)
            return carry

        lax.fori_loop(0, total // tile, step, 0)
        if total % tile:
            body(total - total % tile, total % tile)

    pl.when(outer)(lambda: start_own(OUT))
    pass_on(QKV, (1, 2))

    @pl.when(inner)
    def _():
        start_own(OUT)

    @pl.when(outer)
    def _():
        for pair in NARROW:
            start_cross(pair)
            start_near(pair, True)

    pass_on(QKV, (3,))
    complete(QKV)

    def project(at, size):
        qkv[:, pl.ds(at, size)] = jnp.dot(
            normed[...], qkv_w[:, pl.ds(at, size)], preferred_element_type=f32
        ).astype(bf16)

    tiles(qkv_w.shape[1], project)
    pass_on(OUT, (1,))

    @pl.when(inner)
    def _():
        for pair in NARROW:
            start_cross(pair)

    for h in range(heads):
        attention_kernel(heads, qkv, lowrank, second_ref, bias_ref, extra, hgain_ref, headed, [h])
        if h == 0:
            pass_on(OUT, (2,))

            @pl.when(inner)
            def _():
                start_near(NARROW[0], False)
                for pair in EXTRA:
                    start_cross(pair)
                pass_cut(NARROW[0], 0)

    @pl.when(outer)
    def _():
        for pair in EXTRA:
            start_cross(pair)
            start_near(pair, True)
            start_spare(pair)

    pass_on(OUT, (3,))

    @pl.when(inner)
    def _():
        for pair in NARROW[1:]:
            start_near(pair, False)

    complete(OUT)

    for c in range(chunks):
        mixed = jnp.dot(
            headed[...], out_w[:, c * wide : (c + 1) * wide], preferred_element_type=f32
        ).astype(bf16)
        part1[c] = mixed.reshape(2, 2, share, wide)
        sum_core1(c).start()
    pl.when(outer)(lambda: pass_cut(NARROW[0], 0))
    for c in range(chunks):
        sum_core1(c).wait_recv()
        send1[c] = (part1[c, 1 - xi, ci].astype(f32) + core1[c, 1 - xi].astype(f32)).astype(bf16)
        sum_line1(c).start()
    pl.when(outer)(lambda: pass_cut(NARROW[0], 1))

    @pl.when(inner)
    def _():
        for pair in EXTRA:
            start_near(pair, False)
        pass_cut(NARROW[0], 1)
        for pair in NARROW[1:]:
            pass_cut(pair, 0)
    own = pl.ds(pl.multiple_of(me * share, share), share)
    for c in range(chunks):
        sum_line1(c).wait_recv()
        cols = slice(c * wide, (c + 1) * wide)
        total = part1[c, xi, ci].astype(f32) + core1[c, xi].astype(f32) + line1[c].astype(f32)
        resid[:, cols] = (x_ref[own, cols].astype(f32) + total).astype(bf16)
    for p in range(parts):
        value = resid[p * lump : (p + 1) * lump]
        start = pl.multiple_of(me * share + p * lump, lump)
        second[pl.ds(start, lump)] = norm_rows(value, gain2_ref[...]).astype(bf16)
        to_partner(p).start()
        across(p, 0).start()
        over(p, 0, 1).start()

    def gate_up(which, pairs):
        r = slice(which * rows, (which + 1) * rows)

        def run(start, size):
            def step(s, carry):
                cols = pl.ds(pl.multiple_of(start + s * 128, 128), 128)
                both = jnp.dot(
                    second[r],
                    jnp.concatenate([gate_w[:, cols], up_w[:, cols]], axis=1),
                    preferred_element_type=f32,
                )
                hidden[r, cols] = (jax.nn.silu(both[:, :128]) * both[:, 128:]).astype(bf16)
                return carry

            lax.fori_loop(0, size // 128, step, 0)

        first, last = items[pairs[0][0]], items[pairs[-1][0]]
        run(first[4], last[4] + last[3] - first[4])

    def relay_own():
        for p in range(parts):
            across_arrival(p, 0).wait_recv()
            over(p, 0, 0).start()

    def relay_partner():
        for p in range(parts):
            give(p, 0, 1, me, {"fs": partner}).wait_recv()
            across(p, 1).start()
            over(p, 1, 1).start()

    @pl.when(outer)
    def _():
        for c in range(chunks):
            start_down(c)
        pass_cut(NARROW[0], 2)
        for pair in NARROW[1:]:
            pass_cut(pair, 0)
        relay_own()
        for k in (1, 2):
            for pair in NARROW[1:]:
                pass_cut(pair, k)

    @pl.when(inner)
    def _():
        pass_cut(NARROW[0], 2)
        for pair in NARROW[1:]:
            pass_cut(pair, 1)
        relay_own()
        for pair in NARROW[1:]:
            pass_cut(pair, 2)
        for pair in EXTRA:
            for k in range(3):
                pass_cut(pair, k)
        for c in range(chunks):
            start_down(c)
            start_middle(c)

    for p in range(parts):
        over_arrival(p, 0, 1).wait_recv()
        over_arrival(p, 0, 0).wait_recv()
    complete_cut(NARROW[0])
    gate_up(0, NARROW[:1])

    def gate_up_rest():
        for pair in NARROW[1:]:
            complete_cut(pair)
        gate_up(0, NARROW[1:])

    def relay_last():
        for p in range(parts):
            across_arrival(p, 1).wait_recv()
            over(p, 1, 0).start()

    def receive_last():
        for p in range(parts):
            over_arrival(p, 1, 1).wait_recv()
            over_arrival(p, 1, 0).wait_recv()

    def pass_downs(quarter):
        for c in range(quarter * chunks // 4, (quarter + 1) * chunks // 4):
            pass_down(c)

    @pl.when(outer)
    def _():
        relay_partner()
        gate_up_rest()
        relay_last()
        pass_downs(0)
        receive_last()
        gate_up(1, NARROW)
        for quarter in range(1, 4):
            pass_downs(quarter)

    @pl.when(inner)
    def _():
        gate_up_rest()
        relay_partner()
        pass_downs(0)
        for pair in EXTRA:
            complete_cut(pair)
        gate_up(0, EXTRA)
        relay_last()
        pass_downs(1)
        receive_last()
        gate_up(1, NARROW)
        pass_downs(2)
        gate_up(1, EXTRA)
        pass_downs(3)

    def sum_a(c):
        complete_down(c)
        for which in range(2):
            out = jnp.dot(
                hidden[which * rows : (which + 1) * rows],
                down_w[:, c * wide : (c + 1) * wide],
                preferred_element_type=f32,
            ).astype(bf16)
            part2[c, which] = out.reshape(2, 2, share, wide)
        sum_core2(c).start()

    def chip(c, which, across_x):
        return part2[c, which, across_x, ci].astype(f32) + core2[c, which, across_x].astype(f32)

    def sum_b(c):
        sum_core2(c).wait_recv()
        for k in range(2):
            value = chip(c, 1, k) if line_first(c) else chip(c, k, 1 - xi)
            send2[c, k] = value.astype(bf16)
        sum_line2(c).start()

    def mine(c):
        if line_first(c):
            return chip(c, 0, xi) + line2[c, xi].astype(f32)
        return chip(c, 0, xi) + line2[c, 0].astype(f32)

    def theirs(c):
        if line_first(c):
            return chip(c, 0, 1 - xi) + line2[c, 1 - xi].astype(f32)
        return chip(c, 1, xi) + line2[c, 1].astype(f32)

    def sum_c(c):
        sum_line2(c).wait_recv()
        send3[c] = theirs(c).astype(bf16)
        sum_line3(c).start()

    def sum_d(c):
        sum_line3(c).wait_recv()
        total = mine(c) + line3[c].astype(f32)
        value = resid[:, c * wide : (c + 1) * wide].astype(f32) + total
        result[c, me] = value.astype(bf16)
        fin(c, 0, me, {"tp": line_peer}).start()
        fin(c, 1, me, {"tp": core_peer}).start()
        put(c, me).start()

    def sum_e(c):
        fin(c, 0, line_peer, {"tp": line_peer}).wait_recv()
        fin(c, 2, line_peer, {"tp": core_peer}).start()
        put(c, line_peer).start()

    corner = 2 * (1 - xi) + 1 - ci

    def sum_f(c):
        fin(c, 1, core_peer, {"tp": core_peer}).wait_recv()
        put(c, core_peer).start()
        fin(c, 2, corner, {"tp": core_peer}).wait_recv()
        put(c, corner).start()

    for c in range(chunks + 1):
        if c < chunks:
            sum_a(c)
        if c:
            sum_b(c - 1)
    for _, k, c in sum_order(chunks, line_first):
        stage = (sum_c, sum_d, sum_e)[k]
        stage(c)
    for c in range(chunks):
        sum_f(c)

    for c in range(chunks):
        for t in (me, core_peer, line_peer, corner):
            put(c, t).wait()
        fin(c, 0, me, {"tp": line_peer}).wait_send()
        fin(c, 1, me, {"tp": core_peer}).wait_send()
        fin(c, 2, line_peer, {"tp": core_peer}).wait_send()
        for copy in (sum_core1, sum_line1, sum_core2, sum_line2, sum_line3):
            copy(c).wait_send()
        drain_down(c)
    for p in range(parts):
        to_partner(p).wait_send()
        for which in range(2):
            across(p, which).wait_send()
            over(p, which, 1).wait_send()
            over(p, which, 0).wait_send()
    drain(QKV)
    drain(OUT)
    for pair in NARROW + EXTRA:
        drain_cut(pair)


def sum_order(chunks, line_first):
    x, line, events = 0, 0, []
    for c in range(chunks):
        if line_first(c):
            line += 4
            events.append((line, 0, c))
        else:
            x += 2
            events.append((x, 0, c))
    for at, _, c in sorted(events):
        if line_first(c):
            x = max(x, at) + 1
            events.append((x, 1, c))
        else:
            line = max(line, at) + 2
            events.append((line, 1, c))
    for at, k, c in sorted(events):
        if k == 1:
            x = max(x, at) + 1
            events.append((x, 2, c))
    return sorted(events)


def narrow_units(units):
    return units // 128 * 3 // 8 * 128


def fits(x, q, k, v, o, g, u, d):
    copies, n, count = (lax.axis_size(a) for a in ("grp", "fs", "tp"))
    rows, width = x.shape
    if (copies, n, count) != (2, 4, 4) or rows % (64 * count) or width % 2048:
        return False
    for p in (q, k, v, o, g, u, d):
        if p.shape[0] % 32 or p.shape[1] % 128:
            return False
    units, depth = g.shape[1], d.shape[0]
    small = narrow_units(units)
    sub, rest = small - depth, units - small - 2 * depth
    if min(sub, rest) <= 0 or sub % 32 or rest % 32:
        return False
    if small % 256:
        return False
    held = n * (q.size + k.size + v.size + o.size) + 3 * (units - small) * n * g.shape[0]
    return 2 * held + 24 * x.size <= 54 * 2**20


def fused(x, gain1, q, k, v, first, second, bias, extra, hgain, o, gain2, g, u, d):
    n, count = lax.axis_size("fs"), lax.axis_size("tp")
    rows, width = x.shape
    share = rows // count
    heads = extra.shape[1]
    chunks, parts = 8, 4
    wide = width // chunks
    bf16, f32 = jnp.bfloat16, jnp.float32
    vmem, hbm = pl.BlockSpec(memory_space=pltpu.VMEM), pl.BlockSpec(memory_space=pl.ANY)
    qkv_cols = 2 * q.shape[1] + v.shape[1]
    held = heads * hgain.shape[0]
    units = g.shape[1]
    small = narrow_units(units)
    big = units - small
    buffers = [
        ((rows, width), bf16),
        ((n * q.shape[0], qkv_cols), bf16),
        ((n * o.shape[0], width), bf16),
        ((n * g.shape[0], big), bf16),
        ((n * u.shape[0], big), bf16),
        ((big, width), bf16),
        ((rows, width), bf16),
        ((rows, first.shape[1]), bf16),
        ((rows, heads), f32),
        ((rows, qkv_cols), bf16),
        ((rows, held), bf16),
        ((chunks, 2, 2, share, wide), bf16),
        ((chunks, 2, share, wide), bf16),
        ((chunks, share, wide), bf16),
        ((chunks, share, wide), bf16),
        ((share, width), bf16),
        ((2 * rows, width), bf16),
        ((2 * rows, big), bf16),
        ((chunks, 2, 2, 2, share, wide), bf16),
        ((chunks, 2, 2, share, wide), bf16),
        ((chunks, 2, share, wide), bf16),
        ((chunks, 2, share, wide), bf16),
        ((chunks, share, wide), bf16),
        ((chunks, share, wide), bf16),
        ((chunks, count, share, wide), bf16),
    ]
    lots = sum(-(-size // 256) for size in (q.shape[1], k.shape[1], v.shape[1])) + 4
    lots += 2 * (small // 256 + -(-(big - small) // 256))
    counts = [(lots, n)] * 5 + [(lots,)] + [(chunks, 2)] * 5
    counts += [(chunks, 5)] * 2 + [(7, parts)] * 2 + [(chunks, 3)] * 2 + [(chunks, count)]
    return pl.pallas_call(
        functools.partial(fused_kernel, (n, count, heads, chunks, small, parts)),
        out_shape=jax.ShapeDtypeStruct((rows, width), bf16),
        in_specs=[vmem] * 7 + [hbm] * 8,
        out_specs=hbm,
        scratch_shapes=[pltpu.VMEM(s, t) for s, t in buffers]
        + [pltpu.SemaphoreType.DMA(s) for s in counts]
        + [pltpu.SemaphoreType.DMA],
        compiler_params=pltpu.CompilerParams(
            vmem_limit_bytes=62 * 1024 * 1024, collective_id=0, has_side_effects=True
        ),
    )(
        gain1[None, :],
        first.T,
        second,
        bias[None, :],
        extra.T,
        hgain[None, :],
        gain2[None, :],
        *(x, q, k, v, o, g, u, d),
    )


def shards(*arrays):
    if fits(*[arrays[i] for i in (0, 2, 3, 4, 10, 12, 13, 14)]):
        return fused(*arrays)
    return spread(*arrays)


def spread(
    layer_input_tokens,
    attention_norm_gain,
    query_projection,
    key_projection,
    value_projection,
    decay_first_factor,
    decay_second_factor,
    decay_logit_bias,
    extra_log_decay,
    head_output_gain,
    attention_output_projection,
    feedforward_norm_gain,
    gate_projection,
    up_projection,
    down_projection,
):
    rows = layer_input_tokens.shape[0]
    count = lax.axis_size("tp")
    me = lax.axis_index("tp")
    share = rows // count
    qkv_full = gather_shared(
        jnp.concatenate([query_projection, key_projection, value_projection], axis=1)
    )
    out_full = gather_shared(attention_output_projection)
    gate_full = gather_shared(gate_projection)
    up_full = gather_shared(up_projection)
    down_full = gather_shared(down_projection, 2)

    normed = norm_rows(layer_input_tokens, attention_norm_gain).astype(jnp.bfloat16)
    lowrank = jnp.dot(normed, decay_first_factor, preferred_element_type=jnp.float32).astype(
        jnp.bfloat16
    )
    qkv = shared_dot(normed, qkv_full)
    headed = attention(
        qkv, lowrank, decay_second_factor, decay_logit_bias, extra_log_decay, head_output_gain
    )
    turned = jnp.concatenate(
        [
            lax.dynamic_slice_in_dim(headed, lax.rem(me - j + count, count) * share, share, 0)
            for j in range(count)
        ],
        axis=0,
    )
    mixer = scatter_sum(shared_dot(turned, out_full), share)
    own = lax.dynamic_slice_in_dim(layer_input_tokens, me * share, share, 0)
    residual = (own.astype(jnp.float32) + mixer).astype(jnp.bfloat16)
    mine = norm_rows(residual, feedforward_norm_gain).astype(jnp.bfloat16)
    second = jnp.concatenate([mine] + [step_on(mine, j) for j in range(1, count)], axis=0)
    hidden = in_order(
        [
            (gated(second, g_own, u_own), gated(second, g_other, u_other))
            for (g_own, g_other), (u_own, u_other) in zip(gate_full, up_full)
        ]
    )
    channel = scatter_sum(shared_dot(hidden, down_full), share)
    finished = (residual.astype(jnp.float32) + channel).astype(jnp.bfloat16)
    return lax.all_gather(finished, "tp", axis=0, tiled=True)


def solution(mesh):
    placed = (
        P(("grp", "fs"), None),
        P(),
        P("fs", "tp"),
        P("fs", "tp"),
        P("fs", "tp"),
        P(),
        P(None, "tp"),
        P("tp"),
        P(("grp", "fs"), "tp"),
        P(),
        P(("tp", "fs"), None),
        P(),
        P("fs", "tp"),
        P("fs", "tp"),
        P(("tp", "fs"), None),
    )
    return jax.shard_map(
        shards, mesh=mesh, in_specs=placed, out_specs=P(("grp", "fs"), None), check_vma=False
    )
```

```python
import functools

import jax
import jax.numpy as jnp
from jax import lax
from jax.experimental import pallas as pl
from jax.experimental.pallas import tpu as pltpu
from jax.sharding import PartitionSpec as P

BLOCK = 64
DECAY_GATE = 16.0


def norm_rows(values, gain):
    wide = values.astype(jnp.float32)
    scale = lax.rsqrt(jnp.mean(wide * wide, axis=-1, keepdims=True) + 1e-06)
    return wide * scale * gain


def attention_kernel(heads, qkv_ref, lowrank_ref, second_ref, bias_ref, extra_ref, gain_ref, out_ref, which=None):
    rows = qkv_ref.shape[0]
    kc = second_ref.shape[1] // heads
    vc = out_ref.shape[1] // heads
    count = rows // BLOCK
    f32, bf16 = jnp.float32, jnp.bfloat16
    row_id = lax.broadcasted_iota(jnp.int32, (BLOCK, BLOCK), 0)
    col_id = lax.broadcasted_iota(jnp.int32, (BLOCK, BLOCK), 1)
    lower = row_id >= col_id
    upper = row_id <= col_id
    lower_ones = jnp.where(lower, 1.0, 0.0).astype(f32)
    half = BLOCK // 2
    for h in which or range(heads):
        kcols = slice(h * kc, (h + 1) * kc)
        logits = (
            jnp.dot(lowrank_ref[...], second_ref[:, kcols], preferred_element_type=f32)
            + bias_ref[:, kcols]
        )
        log_sig = jnp.minimum(logits, 0.0) - jnp.log1p(jnp.exp(-jnp.abs(logits)))
        decay = log_sig / DECAY_GATE + extra_ref[:, h : h + 1]
        queries_fb, updates, closings, scores = [], [], [], []
        for b in range(count):
            r = slice(b * BLOCK, (b + 1) * BLOCK)
            d = decay[r]
            q = qkv_ref[r, h * kc : (h + 1) * kc].astype(f32)
            k = qkv_ref[r, (heads + h) * kc : (heads + h + 1) * kc].astype(f32)
            v = qkv_ref[r, 2 * heads * kc + h * vc : 2 * heads * kc + (h + 1) * vc]
            run = jnp.dot(lower_ones, d, precision=lax.Precision.HIGHEST, preferred_element_type=f32)
            closing = run[BLOCK - 1 : BLOCK]
            back = closing - run + d
            mid_f = run[half - 1 : half]
            mid_b = back[half : half + 1]
            qf = (q * jnp.exp(run - mid_f)).astype(bf16)
            kf = (k * jnp.exp(mid_f - run)).astype(bf16)
            qb = (q * jnp.exp(back - mid_b)).astype(bf16)
            kb = (k * jnp.exp(mid_b - back)).astype(bf16)
            nt = (((1,), (1,)), ((), ()))
            sf = lax.dot_general(qf, kf, nt, preferred_element_type=f32)
            sb = lax.dot_general(qb, kb, nt, preferred_element_type=f32)
            scores.append(
                (jnp.where(lower, sf, 0.0) + jnp.where(upper, sb, 0.0)).astype(bf16)
            )
            queries_fb.append(
                jnp.concatenate([q * jnp.exp(run), q * jnp.exp(back)], axis=1).astype(bf16)
            )
            keys_fb = jnp.concatenate(
                [k * jnp.exp(closing - run), k * jnp.exp(closing - back)], axis=1
            ).astype(bf16)
            updates.append(
                lax.dot_general(v, keys_fb, (((0,), (0,)), ((), ())), preferred_element_type=f32)
            )
            closings.append(jnp.exp(closing))
        state = jnp.zeros((vc, kc), f32)
        ahead = []
        for b in range(count):
            ahead.append(state.astype(bf16))
            state = state * closings[b] + updates[b][:, :kc]
        state = jnp.zeros((vc, kc), f32)
        behind = [None] * count
        for b in reversed(range(count)):
            behind[b] = state.astype(bf16)
            state = state * closings[b] + updates[b][:, kc:]
        for b in range(count):
            r = slice(b * BLOCK, (b + 1) * BLOCK)
            v = qkv_ref[r, 2 * heads * kc + h * vc : 2 * heads * kc + (h + 1) * vc]
            states = jnp.concatenate([ahead[b], behind[b]], axis=1)
            mixed = lax.dot_general(
                queries_fb[b], states, (((1,), (1,)), ((), ())), preferred_element_type=f32
            ) + jnp.dot(scores[b], v, preferred_element_type=f32)
            scale = lax.rsqrt(jnp.mean(mixed * mixed, axis=-1, keepdims=True) + 1e-06)
            out_ref[r, h * vc : (h + 1) * vc] = (mixed * scale * gain_ref[...]).astype(bf16)


def attention(qkv, lowrank, second_factor, bias, extra, gain):
    rows = qkv.shape[0]
    heads = extra.shape[1]
    width = heads * gain.shape[0]
    kc = second_factor.shape[1] // heads
    return pl.pallas_call(
        functools.partial(attention_kernel, heads),
        out_shape=jax.ShapeDtypeStruct((rows, width), jnp.bfloat16),
        in_specs=[pl.BlockSpec(memory_space=pltpu.VMEM)] * 6,
        out_specs=pl.BlockSpec(memory_space=pltpu.VMEM),
        compiler_params=pltpu.CompilerParams(vmem_limit_bytes=32 * 1024 * 1024),
        cost_estimate=pl.CostEstimate(
            flops=40 * rows * kc * width, bytes_accessed=4 * rows * width * 2, transcendentals=0
        ),
    )(qkv, lowrank, second_factor, bias[None, :], extra, gain[None, :])


def gather_shared(piece, chunks=1):
    copies = lax.axis_size("grp")
    if copies != 2 or piece.shape[1] % (copies * chunks):
        return [(lax.all_gather(piece, "fs", axis=0, tiled=True), None)]
    wide = piece.shape[1] // chunks
    part = wide // copies
    pairs = []
    for chunk in range(chunks):
        start = chunk * wide + lax.axis_index("grp") * part
        own = lax.all_gather(
            lax.dynamic_slice_in_dim(piece, start, part, 1), "fs", axis=0, tiled=True
        )
        pairs.append((own, lax.ppermute(own, "grp", [(0, 1), (1, 0)])))
    return pairs


def in_order(pairs):
    if pairs[0][1] is None:
        return pairs[0][0]
    first = lax.axis_index("grp") == 0
    blocks = []
    for own, other in pairs:
        blocks += [jnp.where(first, own, other), jnp.where(first, other, own)]
    return jnp.concatenate(blocks, axis=1)


def times(left, right):
    if right is None:
        return None
    return jnp.dot(left, right, preferred_element_type=jnp.float32)


def shared_dot(left, pairs):
    def rounded(right):
        return None if right is None else times(left, right).astype(jnp.bfloat16)

    return in_order([(rounded(own), rounded(other)) for own, other in pairs])


def gated(second, gate_weight, up_weight):
    if gate_weight is None:
        return None
    gate, up = times(second, gate_weight), times(second, up_weight)
    return (jax.nn.silu(gate) * up).astype(jnp.bfloat16)


def step_back(values, hops):
    count = lax.axis_size("tp")
    return lax.ppermute(values, "tp", [(i, (i - hops) % count) for i in range(count)])


def step_on(values, hops):
    count = lax.axis_size("tp")
    return lax.ppermute(values, "tp", [(i, (i + hops) % count) for i in range(count)])


def scatter_sum(partial, share):
    count = lax.axis_size("tp")
    total = partial[:share].astype(jnp.float32)
    arrived = [step_back(partial[j * share : (j + 1) * share], j) for j in range(1, count)]
    for block in arrived:
        total = total + block.astype(jnp.float32)
    return total


def fused_kernel(
    shape,
    gain1_ref,
    first_ref,
    second_ref,
    bias_ref,
    extra_ref,
    hgain_ref,
    gain2_ref,
    x_hbm,
    q_hbm,
    k_hbm,
    v_hbm,
    o_hbm,
    g_hbm,
    u_hbm,
    d_hbm,
    out_hbm,
    x_ref,
    qkv_w,
    out_w,
    gate_w,
    up_w,
    down_w,
    normed,
    lowrank,
    extra,
    qkv,
    headed,
    part1,
    core1,
    send1,
    line1,
    resid,
    second,
    hidden,
    part2,
    core2,
    send2,
    line2,
    send3,
    line3,
    result,
    s_right,
    s_left,
    s_grp,
    r_line,
    r_grp,
    local,
    s_down,
    r_down,
    sy_down,
    ry_down,
    l_down,
    s_sum,
    r_sum,
    s_share,
    r_share,
    s_fin,
    r_fin,
    store,
    load,
):
    n, count, heads, chunks, small, parts = shape
    f32, bf16 = jnp.float32, jnp.bfloat16
    z, y, me = lax.axis_index("fs"), lax.axis_index("grp"), lax.axis_index("tp")
    rows, width = x_ref.shape
    share = rows // count
    wide = width // chunks
    kcols, vcols = q_hbm.shape[1], v_hbm.shape[1]
    units = g_hbm.shape[1]
    big = units - small
    xi, ci = me // 2, lax.rem(me, 2)
    core_peer = 2 * xi + 1 - ci
    line_peer = 2 * (1 - xi) + ci
    side = z // 2
    mate = z + 1 - 2 * lax.rem(z, 2)
    partner = lax.rem(z + 2, n)
    inner = lax.rem(z + side, 2) == 1
    outer = jnp.logical_not(inner)
    cross = 2 - side
    far = 3 * (1 - side)

    strip = 256
    items = []

    def add(source, target, start, total, place, step):
        first = len(items)
        for at in range(0, total, step):
            size = min(step, total - at)
            items.append((source, target, start + at, size, place + at))
        return list(range(first, len(items)))

    QKV = add(q_hbm, qkv_w, 0, kcols, 0, strip)
    QKV += add(k_hbm, qkv_w, 0, kcols, kcols, strip)
    QKV += add(v_hbm, qkv_w, 0, vcols, 2 * kcols, strip)
    OUT = add(o_hbm, out_w, 0, width, 0, width // 4)
    NARROW, EXTRA = [], []
    for at in range(0, big, strip):
        most = small if at < small else big
        size = min(strip, most - at)
        pair = add(g_hbm, gate_w, at, size, at, strip) + add(u_hbm, up_w, at, size, at, strip)
        (NARROW if at < small else EXTRA).append(pair)

    def remote(source, target, send, recv, where):
        return pltpu.make_async_remote_copy(
            src_ref=source,
            dst_ref=target,
            send_sem=send,
            recv_sem=recv,
            device_id=where,
            device_id_type=pl.DeviceIdType.MESH,
        )

    def high_of(i):
        return items[i][0].shape[0] // 2

    def rows_of(i, origin, half):
        high = high_of(i)
        return pl.ds(pl.multiple_of((2 * origin + half) * high, high), high)

    def all_rows(i, origin):
        high = items[i][0].shape[0]
        return pl.ds(pl.multiple_of(origin * high, high), high)

    def lanes(start, size):
        return pl.ds(pl.multiple_of(start, 128), size)

    def piece(i, origin, half):
        _, target, _, size, place = items[i]
        return target.at[rows_of(i, origin, half), pl.ds(place, size)]

    def own_rows(i, half):
        source, _, start, size, _ = items[i]
        high = high_of(i)
        return source.at[pl.ds(pl.multiple_of(half * high, high), high), pl.ds(start, size)]

    def spare(i, sent):
        return remote(sent, piece(i, z, 1 - y), s_grp.at[i, z], r_grp.at[i, z], {"fs": mate})

    def to_right(i, origin, source):
        return remote(
            source, piece(i, origin, y), s_right.at[i, origin], r_line.at[i, origin], {"fs": z + 1}
        )

    def to_left(i, origin, source):
        return remote(
            source, piece(i, origin, y), s_left.at[i, origin], r_line.at[i, origin], {"fs": z - 1}
        )

    def to_grp(i, origin, block):
        return remote(block, block, s_grp.at[i, origin], r_grp.at[i, origin], {"grp": 1 - y})

    def local_copy(i):
        source, target, start, size, place = items[i]
        return pltpu.make_async_copy(
            source.at[:, pl.ds(start, size)],
            target.at[all_rows(i, z), pl.ds(place, size)],
            local.at[i],
        )

    def start_own(group):
        for i in group:
            own = own_rows(i, y)
            pl.when(z + 1 < n)(lambda i=i, own=own: to_right(i, z, own).start())
            pl.when(z >= 1)(lambda i=i, own=own: to_left(i, z, own).start())
            local_copy(i).start()
        for i in group:
            pl.when(outer)(lambda i=i: spare(i, own_rows(i, 1 - y)).start())

    def sides(d):
        return (
            (z >= d, z - d, z + 1 < n, to_right, z >= 2),
            (z + d < n, z + d, z >= 1, to_left, z < n - 2),
        )

    def pass_on(group, distances):
        for d in distances:
            for i in group:
                for there, origin, more, send, shared in sides(d):

                    @pl.when(there)
                    def _():
                        block = piece(i, origin, y)
                        send(i, origin, block).wait_recv()
                        pl.when(more)(lambda: send(i, origin, block).start())
                        if d == 1:
                            pl.when(shared)(lambda: to_grp(i, origin, block).start())
                        else:
                            to_grp(i, origin, block).start()

    def complete(group):
        for i in group:
            local_copy(i).wait()
            for d in range(1, n):
                for cond, origin in ((z >= d, z - d), (z + d < n, z + d)):
                    pl.when(cond)(
                        lambda i=i, o=origin: to_grp(i, o, piece(i, o, 1 - y)).wait_recv()
                    )

    def drain(group):
        for i in group:
            own = own_rows(i, y)
            pl.when(z + 1 < n)(lambda: to_right(i, z, own).wait_send())
            pl.when(z >= 1)(lambda: to_left(i, z, own).wait_send())
            pl.when(outer)(lambda: spare(i, own_rows(i, 1 - y)).wait_send())
            for d in range(1, n):
                for there, origin, more, send, shared in sides(d):

                    @pl.when(there)
                    def _():
                        block = piece(i, origin, y)
                        pl.when(more)(lambda: send(i, origin, block).wait_send())
                        if d == 1:
                            pl.when(shared)(lambda: to_grp(i, origin, block).wait_send())
                        else:
                            to_grp(i, origin, block).wait_send()

    origins = (mate, cross, far)
    EXTRAS = [i for pair in EXTRA for i in pair]

    def cut_rows(i, half, to):
        source, _, start, size, _ = items[i]
        high = high_of(i)
        offset = start if i in EXTRAS else to * big + start
        return source.at[pl.ds(pl.multiple_of(half * high, high), high), lanes(offset, size)]

    def to_mate(i, origin, sent):
        return remote(
            sent, piece(i, origin, y), s_right.at[i, origin], r_line.at[i, origin], {"fs": mate}
        )

    def to_cross(i):
        return remote(
            cut_rows(i, y, 1 - side),
            piece(i, z, y),
            s_left.at[i, z],
            r_line.at[i, z],
            {"fs": cross},
        )

    def keep(i):
        source, target, start, size, place = items[i]
        offset = start if i in EXTRAS else side * big + start
        return pltpu.make_async_copy(
            source.at[:, lanes(offset, size)],
            target.at[all_rows(i, z), pl.ds(place, size)],
            local.at[i],
        )

    def start_near(pair, ends):
        for i in pair:
            if i not in EXTRAS:
                to_mate(i, z, cut_rows(i, y, side)).start()
                keep(i).start()
            elif ends:
                to_mate(i, z, cut_rows(i, y, side)).start()
            else:
                keep(i).start()

    def start_cross(pair):
        for i in pair:
            to_cross(i).start()

    def start_spare(pair):
        for i in pair:
            spare(i, cut_rows(i, 1 - y, side)).start()

    def pass_cut(pair, k):
        def step(i):
            origin = origins[k]
            block = piece(i, origin, y)
            to_mate(i, origin, block).wait_recv()
            if i in EXTRAS:
                if k:
                    to_grp(i, origin, block).start()
                return
            if k:
                pl.when(inner)(lambda: to_mate(i, origin, block).start())
            to_grp(i, origin, block).start()

        for i in pair:
            if i in EXTRAS:
                pl.when(inner)(lambda i=i: step(i))
            else:
                step(i)

    def complete_cut(pair):
        def step(i):
            keep(i).wait()
            for origin in origins:
                to_grp(i, origin, piece(i, origin, 1 - y)).wait_recv()

        for i in pair:
            if i in EXTRAS:
                pl.when(inner)(lambda i=i: step(i))
            else:
                step(i)

    def drain_cut(pair):
        for i in pair:
            to_cross(i).wait_send()
            if i in EXTRAS:

                @pl.when(outer)
                def _():
                    to_mate(i, z, cut_rows(i, y, side)).wait_send()
                    spare(i, cut_rows(i, 1 - y, side)).wait_send()

                @pl.when(inner)
                def _():
                    for k in (1, 2):
                        to_grp(i, origins[k], piece(i, origins[k], y)).wait_send()

            else:
                to_mate(i, z, cut_rows(i, y, side)).wait_send()
                for k in range(3):
                    block = piece(i, origins[k], y)
                    if k:
                        pl.when(inner)(
                            lambda k=k, b=block: to_mate(i, origins[k], b).wait_send()
                        )
                    to_grp(i, origins[k], block).wait_send()

    depth = d_hbm.shape[0]
    sub, rest = small - depth, big - 2 * depth

    def down_block(c, start, size):
        return down_w.at[pl.ds(pl.multiple_of(start, 16), size), pl.ds(c * wide, wide)]

    def down_src(c, start, size):
        return d_hbm.at[pl.ds(pl.multiple_of(start, 16), size), pl.ds(c * wide, wide)]

    def end_place(c, start, size):
        return down_block(c, side * sub + start, size)

    def near_place(c, start, size):
        return down_block(c, (1 - side) * depth + start, size)

    def near_src(c, start, size):
        return down_src(c, side * rest + start, size)

    def middle_place(c, whose, start, size):
        return down_block(c, small + whose * rest + start, size)

    def middle_src(c, start, size):
        return down_src(c, (1 - side) * sub + start, size)

    def halved(c, size, half, place):
        return place(c, half * (size // 2), size // 2)

    def from_mate(c, half, to_inner):
        if to_inner:
            return halved(c, depth, half, end_place)
        return halved(c, sub, half, near_place)

    def middle(c, whose, half):
        return middle_place(c, whose, half * (rest // 2), rest // 2)

    def down_to_mate(c, to_inner):
        sent = halved(c, depth, y, down_src) if to_inner else halved(c, sub, y, near_src)
        return remote(
            sent, from_mate(c, y, to_inner), s_down.at[c, 0], r_down.at[c, 0], {"fs": mate}
        )

    def down_to_cross(c):
        return remote(
            halved(c, rest, y, middle_src),
            middle(c, side, y),
            s_down.at[c, 1],
            r_down.at[c, 1],
            {"fs": cross},
        )

    def down_local(c, k):
        if k == 0:
            return pltpu.make_async_copy(
                down_src(c, 0, depth), end_place(c, 0, depth), l_down.at[c, 0]
            )
        if k == 1:
            return pltpu.make_async_copy(
                near_src(c, 0, sub), near_place(c, 0, sub), l_down.at[c, 0]
            )
        return pltpu.make_async_copy(
            middle_src(c, 0, rest), middle_place(c, side, 0, rest), l_down.at[c, 1]
        )

    def down_grp(c, k, block):
        return remote(block, block, sy_down.at[c, k], ry_down.at[c, k], {"grp": 1 - y})

    def start_down(c):
        @pl.when(outer)
        def _():
            down_to_mate(c, True).start()
            down_local(c, 0).start()

        @pl.when(inner)
        def _():
            down_to_mate(c, False).start()
            down_local(c, 1).start()

    def start_middle(c):
        down_to_cross(c).start()
        down_local(c, 2).start()

    def down_arrival(c, k, block):
        return remote(block, block, s_down.at[c, k], r_down.at[c, k], {"fs": mate})

    def pass_down(c):
        @pl.when(outer)
        def _():
            block = from_mate(c, y, False)
            down_arrival(c, 0, block).wait_recv()
            down_grp(c, 0, block).start()

        @pl.when(inner)
        def _():
            for k, block in ((0, from_mate(c, y, True)), (1, middle(c, 1 - side, y))):
                down_arrival(c, k, block).wait_recv()
                down_grp(c, k, block).start()

    def complete_down(c):
        @pl.when(outer)
        def _():
            down_local(c, 0).wait()
            down_grp(c, 0, from_mate(c, 1 - y, False)).wait_recv()

        @pl.when(inner)
        def _():
            down_local(c, 1).wait()
            down_local(c, 2).wait()
            down_grp(c, 0, from_mate(c, 1 - y, True)).wait_recv()
            down_grp(c, 1, middle(c, 1 - side, 1 - y)).wait_recv()

    def drain_down(c):
        @pl.when(outer)
        def _():
            down_to_mate(c, True).wait_send()
            down_grp(c, 0, from_mate(c, y, False)).wait_send()

        @pl.when(inner)
        def _():
            down_to_mate(c, False).wait_send()
            down_to_cross(c).wait_send()
            down_grp(c, 0, from_mate(c, y, True)).wait_send()
            down_grp(c, 1, middle(c, 1 - side, y)).wait_send()

    def sum_core1(c):
        return remote(
            part1.at[c, :, 1 - ci], core1.at[c], s_sum.at[c, 0], r_sum.at[c, 0], {"tp": core_peer}
        )

    def sum_line1(c):
        return remote(
            send1.at[c], line1.at[c], s_sum.at[c, 1], r_sum.at[c, 1], {"tp": line_peer}
        )

    def sum_core2(c):
        return remote(
            part2.at[c, :, :, 1 - ci],
            core2.at[c],
            s_sum.at[c, 2],
            r_sum.at[c, 2],
            {"tp": core_peer},
        )

    def line_first(c):
        return c % 2 == 0 and c < chunks // 2

    def sum_line2(c):
        where = {"fs": partner} if line_first(c) else {"tp": line_peer}
        return remote(send2.at[c], line2.at[c], s_sum.at[c, 3], r_sum.at[c, 3], where)

    def sum_line3(c):
        where = {"tp": line_peer} if line_first(c) else {"fs": partner}
        return remote(send3.at[c], line3.at[c], s_sum.at[c, 4], r_sum.at[c, 4], where)

    lump = share // parts

    def rows_at(which, t, p):
        start = pl.multiple_of(which * rows + t * share + p * lump, lump)
        return second.at[pl.ds(start, lump)]

    def give(p, slot, which, t, where, target=None):
        block = rows_at(which, t, p)
        return remote(
            block,
            block if target is None else target,
            s_share.at[slot, p],
            r_share.at[slot, p],
            where,
        )

    def to_partner(p):
        return give(p, 0, 0, me, {"fs": partner}, rows_at(1, me, p))

    def across(p, which):
        return give(p, 1 + which, which, me, {"tp": line_peer})

    def across_arrival(p, which):
        return give(p, 1 + which, which, line_peer, {"tp": line_peer})

    def over(p, which, mine):
        return give(p, 3 + 2 * which + (1 - mine), which, me if mine else line_peer, {"tp": core_peer})

    def over_arrival(p, which, mine):
        t = core_peer if mine else 2 * (1 - xi) + 1 - ci
        return give(p, 3 + 2 * which + (1 - mine), which, t, {"tp": core_peer})

    def fin(c, slot, t, where):
        block = result.at[c, t]
        return remote(block, block, s_fin.at[c, slot], r_fin.at[c, slot], where)

    def put(c, t):
        r = pl.ds(pl.multiple_of(t * share, share), share)
        return pltpu.make_async_copy(
            result.at[c, t], out_hbm.at[r, pl.ds(c * wide, wide)], store.at[c, t]
        )

    barrier = pltpu.get_barrier_semaphore()

    def greet(where):
        pl.semaphore_signal(
            barrier, inc=1, device_id=where, device_id_type=pl.DeviceIdType.MESH
        )

    get_x = pltpu.make_async_copy(x_hbm, x_ref, load)
    get_x.start()
    for where in ({"grp": 1 - y}, {"tp": core_peer}, {"tp": line_peer}, {"fs": partner}):
        greet(where)
    pl.when(z + 1 < n)(lambda: greet({"fs": z + 1}))
    pl.when(z >= 1)(lambda: greet({"fs": z - 1}))
    pl.semaphore_wait(barrier, 4 + jnp.minimum(z, 1) + jnp.minimum(n - 1 - z, 1))

    start_own(QKV)

    @pl.when(outer)
    def _():
        hidden[:, small:] = jnp.zeros((2 * rows, big - small), bf16)
        down_w[small:] = jnp.zeros((big - small, width), bf16)

    get_x.wait()
    tall = min(64, share)

    def norm_step(s, carry):
        r = pl.ds(pl.multiple_of(s * tall, tall), tall)
        normed[r] = norm_rows(x_ref[r], gain1_ref[...]).astype(bf16)
        return carry

    lax.fori_loop(0, rows // tall, norm_step, 0)
    lowrank[...] = lax.dot_general(
        normed[...], first_ref[...], (((1,), (1,)), ((), ())), preferred_element_type=f32
    ).astype(bf16)
    extra[...] = extra_ref[...].T

    def tiles(total, body, tile=256):
        def step(s, carry):
            body(pl.multiple_of(s * tile, tile), tile)
            return carry

        lax.fori_loop(0, total // tile, step, 0)
        if total % tile:
            body(total - total % tile, total % tile)

    pl.when(outer)(lambda: start_own(OUT))
    pass_on(QKV, (1, 2))

    @pl.when(inner)
    def _():
        start_own(OUT)

    @pl.when(outer)
    def _():
        for pair in NARROW:
            start_cross(pair)
            start_near(pair, True)

    pass_on(QKV, (3,))
    complete(QKV)

    def project(at, size):
        qkv[:, pl.ds(at, size)] = jnp.dot(
            normed[...], qkv_w[:, pl.ds(at, size)], preferred_element_type=f32
        ).astype(bf16)

    tiles(qkv_w.shape[1], project)
    pass_on(OUT, (1,))

    @pl.when(inner)
    def _():
        for pair in NARROW:
            start_cross(pair)

    for h in range(heads):
        attention_kernel(heads, qkv, lowrank, second_ref, bias_ref, extra, hgain_ref, headed, [h])
        if h == 0:
            pass_on(OUT, (2,))

            @pl.when(inner)
            def _():
                start_near(NARROW[0], False)
                for pair in EXTRA:
                    start_cross(pair)
                pass_cut(NARROW[0], 0)

    @pl.when(outer)
    def _():
        for pair in EXTRA:
            start_cross(pair)
            start_near(pair, True)
            start_spare(pair)

    pass_on(OUT, (3,))

    @pl.when(inner)
    def _():
        for pair in NARROW[1:]:
            start_near(pair, False)

    complete(OUT)

    for c in range(chunks):
        mixed = jnp.dot(
            headed[...], out_w[:, c * wide : (c + 1) * wide], preferred_element_type=f32
        ).astype(bf16)
        part1[c] = mixed.reshape(2, 2, share, wide)
        sum_core1(c).start()
    pl.when(outer)(lambda: pass_cut(NARROW[0], 0))
    for c in range(chunks):
        sum_core1(c).wait_recv()
        send1[c] = (part1[c, 1 - xi, ci].astype(f32) + core1[c, 1 - xi].astype(f32)).astype(bf16)
        sum_line1(c).start()
    pl.when(outer)(lambda: pass_cut(NARROW[0], 1))

    @pl.when(inner)
    def _():
        for pair in EXTRA:
            start_near(pair, False)
        pass_cut(NARROW[0], 1)
        for pair in NARROW[1:]:
            pass_cut(pair, 0)
    own = pl.ds(pl.multiple_of(me * share, share), share)
    for c in range(chunks):
        sum_line1(c).wait_recv()
        cols = slice(c * wide, (c + 1) * wide)
        total = part1[c, xi, ci].astype(f32) + core1[c, xi].astype(f32) + line1[c].astype(f32)
        resid[:, cols] = (x_ref[own, cols].astype(f32) + total).astype(bf16)
    for p in range(parts):
        value = resid[p * lump : (p + 1) * lump]
        start = pl.multiple_of(me * share + p * lump, lump)
        second[pl.ds(start, lump)] = norm_rows(value, gain2_ref[...]).astype(bf16)
        to_partner(p).start()
        across(p, 0).start()
        over(p, 0, 1).start()

    def gate_up(which, pairs):
        r = slice(which * rows, (which + 1) * rows)

        def run(start, size):
            def step(s, carry):
                cols = pl.ds(pl.multiple_of(start + s * 128, 128), 128)
                both = jnp.dot(
                    second[r],
                    jnp.concatenate([gate_w[:, cols], up_w[:, cols]], axis=1),
                    preferred_element_type=f32,
                )
                hidden[r, cols] = (jax.nn.silu(both[:, :128]) * both[:, 128:]).astype(bf16)
                return carry

            lax.fori_loop(0, size // 128, step, 0)

        first, last = items[pairs[0][0]], items[pairs[-1][0]]
        run(first[4], last[4] + last[3] - first[4])

    def relay_own():
        for p in range(parts):
            across_arrival(p, 0).wait_recv()
            over(p, 0, 0).start()

    def relay_partner():
        for p in range(parts):
            give(p, 0, 1, me, {"fs": partner}).wait_recv()
            across(p, 1).start()
            over(p, 1, 1).start()

    @pl.when(outer)
    def _():
        for c in range(chunks):
            start_down(c)
        pass_cut(NARROW[0], 2)
        for pair in NARROW[1:]:
            pass_cut(pair, 0)
        relay_own()
        for k in (1, 2):
            for pair in NARROW[1:]:
                pass_cut(pair, k)

    @pl.when(inner)
    def _():
        pass_cut(NARROW[0], 2)
        for pair in NARROW[1:]:
            pass_cut(pair, 1)
        relay_own()
        for pair in NARROW[1:]:
            pass_cut(pair, 2)
        for pair in EXTRA:
            for k in range(3):
                pass_cut(pair, k)
        for c in range(chunks):
            start_down(c)
            start_middle(c)

    for p in range(parts):
        over_arrival(p, 0, 1).wait_recv()
        over_arrival(p, 0, 0).wait_recv()
    complete_cut(NARROW[0])
    gate_up(0, NARROW[:1])

    def gate_up_rest():
        for pair in NARROW[1:]:
            complete_cut(pair)
        gate_up(0, NARROW[1:])

    def relay_last():
        for p in range(parts):
            across_arrival(p, 1).wait_recv()
            over(p, 1, 0).start()

    def receive_last():
        for p in range(parts):
            over_arrival(p, 1, 1).wait_recv()
            over_arrival(p, 1, 0).wait_recv()

    def pass_downs(quarter):
        for c in range(quarter * chunks // 4, (quarter + 1) * chunks // 4):
            pass_down(c)

    @pl.when(outer)
    def _():
        relay_partner()
        gate_up_rest()
        relay_last()
        pass_downs(0)
        receive_last()
        gate_up(1, NARROW)
        for quarter in range(1, 4):
            pass_downs(quarter)

    @pl.when(inner)
    def _():
        gate_up_rest()
        relay_partner()
        pass_downs(0)
        for pair in EXTRA:
            complete_cut(pair)
        gate_up(0, EXTRA)
        relay_last()
        pass_downs(1)
        receive_last()
        gate_up(1, NARROW)
        pass_downs(2)
        gate_up(1, EXTRA)
        pass_downs(3)

    def sum_a(c):
        complete_down(c)
        for which in range(2):
            out = jnp.dot(
                hidden[which * rows : (which + 1) * rows],
                down_w[:, c * wide : (c + 1) * wide],
                preferred_element_type=f32,
            ).astype(bf16)
            part2[c, which] = out.reshape(2, 2, share, wide)
        sum_core2(c).start()

    def chip(c, which, across_x):
        return part2[c, which, across_x, ci].astype(f32) + core2[c, which, across_x].astype(f32)

    def sum_b(c):
        sum_core2(c).wait_recv()
        for k in range(2):
            value = chip(c, 1, k) if line_first(c) else chip(c, k, 1 - xi)
            send2[c, k] = value.astype(bf16)
        sum_line2(c).start()

    def mine(c):
        if line_first(c):
            return chip(c, 0, xi) + line2[c, xi].astype(f32)
        return chip(c, 0, xi) + line2[c, 0].astype(f32)

    def theirs(c):
        if line_first(c):
            return chip(c, 0, 1 - xi) + line2[c, 1 - xi].astype(f32)
        return chip(c, 1, xi) + line2[c, 1].astype(f32)

    def sum_c(c):
        sum_line2(c).wait_recv()
        send3[c] = theirs(c).astype(bf16)
        sum_line3(c).start()

    def sum_d(c):
        sum_line3(c).wait_recv()
        total = mine(c) + line3[c].astype(f32)
        value = resid[:, c * wide : (c + 1) * wide].astype(f32) + total
        result[c, me] = value.astype(bf16)
        fin(c, 0, me, {"tp": line_peer}).start()
        fin(c, 1, me, {"tp": core_peer}).start()
        put(c, me).start()

    def sum_e(c):
        fin(c, 0, line_peer, {"tp": line_peer}).wait_recv()
        fin(c, 2, line_peer, {"tp": core_peer}).start()
        put(c, line_peer).start()

    corner = 2 * (1 - xi) + 1 - ci

    def sum_f(c):
        fin(c, 1, core_peer, {"tp": core_peer}).wait_recv()
        put(c, core_peer).start()
        fin(c, 2, corner, {"tp": core_peer}).wait_recv()
        put(c, corner).start()

    for c in range(chunks + 1):
        if c < chunks:
            sum_a(c)
        if c:
            sum_b(c - 1)
    for _, k, c in sum_order(chunks, line_first):
        stage = (sum_c, sum_d, sum_e)[k]
        stage(c)
    for c in range(chunks):
        sum_f(c)

    for c in range(chunks):
        for t in (me, core_peer, line_peer, corner):
            put(c, t).wait()
        fin(c, 0, me, {"tp": line_peer}).wait_send()
        fin(c, 1, me, {"tp": core_peer}).wait_send()
        fin(c, 2, line_peer, {"tp": core_peer}).wait_send()
        for copy in (sum_core1, sum_line1, sum_core2, sum_line2, sum_line3):
            copy(c).wait_send()
        drain_down(c)
    for p in range(parts):
        to_partner(p).wait_send()
        for which in range(2):
            across(p, which).wait_send()
            over(p, which, 1).wait_send()
            over(p, which, 0).wait_send()
    drain(QKV)
    drain(OUT)
    for pair in NARROW + EXTRA:
        drain_cut(pair)


def sum_order(chunks, line_first):
    x, line, events = 0, 0, []
    for c in range(chunks):
        if line_first(c):
            line += 4
            events.append((line, 0, c))
        else:
            x += 2
            events.append((x, 0, c))
    for at, _, c in sorted(events):
        if line_first(c):
            x = max(x, at) + 1
            events.append((x, 1, c))
        else:
            line = max(line, at) + 2
            events.append((line, 1, c))
    for at, k, c in sorted(events):
        if k == 1:
            x = max(x, at) + 1
            events.append((x, 2, c))
    return sorted(events)


def narrow_units(units):
    return units // 128 * 3 // 8 * 128


def fits(x, q, k, v, o, g, u, d):
    copies, n, count = (lax.axis_size(a) for a in ("grp", "fs", "tp"))
    rows, width = x.shape
    if (copies, n, count) != (2, 4, 4) or rows % (64 * count) or width % 2048:
        return False
    for p in (q, k, v, o, g, u, d):
        if p.shape[0] % 32 or p.shape[1] % 128:
            return False
    units, depth = g.shape[1], d.shape[0]
    small = narrow_units(units)
    sub, rest = small - depth, units - small - 2 * depth
    if min(sub, rest) <= 0 or sub % 32 or rest % 32:
        return False
    if small % 256:
        return False
    held = n * (q.size + k.size + v.size + o.size) + 3 * (units - small) * n * g.shape[0]
    return 2 * held + 24 * x.size <= 54 * 2**20


def fused(x, gain1, q, k, v, first, second, bias, extra, hgain, o, gain2, g, u, d):
    n, count = lax.axis_size("fs"), lax.axis_size("tp")
    rows, width = x.shape
    share = rows // count
    heads = extra.shape[1]
    chunks, parts = 8, 4
    wide = width // chunks
    bf16, f32 = jnp.bfloat16, jnp.float32
    vmem, hbm = pl.BlockSpec(memory_space=pltpu.VMEM), pl.BlockSpec(memory_space=pl.ANY)
    qkv_cols = 2 * q.shape[1] + v.shape[1]
    held = heads * hgain.shape[0]
    units = g.shape[1]
    small = narrow_units(units)
    big = units - small
    buffers = [
        ((rows, width), bf16),
        ((n * q.shape[0], qkv_cols), bf16),
        ((n * o.shape[0], width), bf16),
        ((n * g.shape[0], big), bf16),
        ((n * u.shape[0], big), bf16),
        ((big, width), bf16),
        ((rows, width), bf16),
        ((rows, first.shape[1]), bf16),
        ((rows, heads), f32),
        ((rows, qkv_cols), bf16),
        ((rows, held), bf16),
        ((chunks, 2, 2, share, wide), bf16),
        ((chunks, 2, share, wide), bf16),
        ((chunks, share, wide), bf16),
        ((chunks, share, wide), bf16),
        ((share, width), bf16),
        ((2 * rows, width), bf16),
        ((2 * rows, big), bf16),
        ((chunks, 2, 2, 2, share, wide), bf16),
        ((chunks, 2, 2, share, wide), bf16),
        ((chunks, 2, share, wide), bf16),
        ((chunks, 2, share, wide), bf16),
        ((chunks, share, wide), bf16),
        ((chunks, share, wide), bf16),
        ((chunks, count, share, wide), bf16),
    ]
    lots = sum(-(-size // 256) for size in (q.shape[1], k.shape[1], v.shape[1])) + 4
    lots += 2 * (small // 256 + -(-(big - small) // 256))
    counts = [(lots, n)] * 5 + [(lots,)] + [(chunks, 2)] * 5
    counts += [(chunks, 5)] * 2 + [(7, parts)] * 2 + [(chunks, 3)] * 2 + [(chunks, count)]
    return pl.pallas_call(
        functools.partial(fused_kernel, (n, count, heads, chunks, small, parts)),
        out_shape=jax.ShapeDtypeStruct((rows, width), bf16),
        in_specs=[vmem] * 7 + [hbm] * 8,
        out_specs=hbm,
        scratch_shapes=[pltpu.VMEM(s, t) for s, t in buffers]
        + [pltpu.SemaphoreType.DMA(s) for s in counts]
        + [pltpu.SemaphoreType.DMA],
        compiler_params=pltpu.CompilerParams(
            vmem_limit_bytes=62 * 1024 * 1024, collective_id=0, has_side_effects=True
        ),
    )(
        gain1[None, :],
        first.T,
        second,
        bias[None, :],
        extra.T,
        hgain[None, :],
        gain2[None, :],
        *(x, q, k, v, o, g, u, d),
    )


def shards(*arrays):
    if fits(*[arrays[i] for i in (0, 2, 3, 4, 10, 12, 13, 14)]):
        return fused(*arrays)
    return spread(*arrays)


def spread(
    layer_input_tokens,
    attention_norm_gain,
    query_projection,
    key_projection,
    value_projection,
    decay_first_factor,
    decay_second_factor,
    decay_logit_bias,
    extra_log_decay,
    head_output_gain,
    attention_output_projection,
    feedforward_norm_gain,
    gate_projection,
    up_projection,
    down_projection,
):
    rows = layer_input_tokens.shape[0]
    count = lax.axis_size("tp")
    me = lax.axis_index("tp")
    share = rows // count
    qkv_full = gather_shared(
        jnp.concatenate([query_projection, key_projection, value_projection], axis=1)
    )
    out_full = gather_shared(attention_output_projection)
    gate_full = gather_shared(gate_projection)
    up_full = gather_shared(up_projection)
    down_full = gather_shared(down_projection, 2)

    normed = norm_rows(layer_input_tokens, attention_norm_gain).astype(jnp.bfloat16)
    lowrank = jnp.dot(normed, decay_first_factor, preferred_element_type=jnp.float32).astype(
        jnp.bfloat16
    )
    qkv = shared_dot(normed, qkv_full)
    headed = attention(
        qkv, lowrank, decay_second_factor, decay_logit_bias, extra_log_decay, head_output_gain
    )
    turned = jnp.concatenate(
        [
            lax.dynamic_slice_in_dim(headed, lax.rem(me - j + count, count) * share, share, 0)
            for j in range(count)
        ],
        axis=0,
    )
    mixer = scatter_sum(shared_dot(turned, out_full), share)
    own = lax.dynamic_slice_in_dim(layer_input_tokens, me * share, share, 0)
    residual = (own.astype(jnp.float32) + mixer).astype(jnp.bfloat16)
    mine = norm_rows(residual, feedforward_norm_gain).astype(jnp.bfloat16)
    second = jnp.concatenate([mine] + [step_on(mine, j) for j in range(1, count)], axis=0)
    hidden = in_order(
        [
            (gated(second, g_own, u_own), gated(second, g_other, u_other))
            for (g_own, g_other), (u_own, u_other) in zip(gate_full, up_full)
        ]
    )
    channel = scatter_sum(shared_dot(hidden, down_full), share)
    finished = (residual.astype(jnp.float32) + channel).astype(jnp.bfloat16)
    return lax.all_gather(finished, "tp", axis=0, tiled=True)


def solution(mesh):
    placed = (
        P(("grp", "fs"), None),
        P(),
        P("fs", "tp"),
        P("fs", "tp"),
        P("fs", "tp"),
        P(),
        P(None, "tp"),
        P("tp"),
        P(("grp", "fs"), "tp"),
        P(),
        P(("tp", "fs"), None),
        P(),
        P("fs", "tp"),
        P("fs", "tp"),
        P(("tp", "fs"), None),
    )
    return jax.shard_map(
        shards, mesh=mesh, in_specs=placed, out_specs=P(("grp", "fs"), None), check_vma=False
    )
```
